32 devices in a mesh: ep: 8 (over z, x), tp: 4 (over y, core).
Axes of the slice: x: 2, y: 2, z: 4, core: 2. Of those that a mesh axis runs over, the one named last changes fastest.
Arguments:
- tokens: bfloat16 [768, 4096], P('ep'), may hold values from -6 to 6
- mix_gain: float32 [4096], replicated, may hold values from 0.1 to 1.9
- ffn_gain: float32 [4096], replicated, may hold values from 0.1 to 1.9
- in_proj: bfloat16 [4096, 1024], P(None, 'tp'), may hold values from -0.09375 to 0.09375
- decay_rate: float32 [64, 64], P('tp'), may hold values from 0.05 to 2
- frequency: float32 [64, 64], P('tp'), may hold values from -3 to 3
- log_step: float32 [64], P('tp'), may hold values from -3 to 0.5
- b_real: float32 [64, 64, 16], P('tp'), may hold values from -1.5 to 1.5
- b_imag: float32 [64, 64, 16], P('tp'), may hold values from -1.5 to 1.5
- c_real: float32 [64, 16, 64], P('tp'), may hold values from -0.75 to 0.75
- c_imag: float32 [64, 16, 64], P('tp'), may hold values from -0.75 to 0.75
- skip_gain: float32 [1024], P('tp'), may hold values from -5 to 5
- states: float32 [2, 768, 4096], P(None, 'ep', 'tp'), may hold values from -6 to 6
- out_proj: bfloat16 [1024, 4096], P('tp'), may hold values from -0.1875 to 0.1875
- route_ids: int32 [768, 2], P('ep'), may hold values from 0 to 7, all different within a row; in each aligned block of 96 rows (0 to 95, 96 to 191, ...) at most 48 rows name the same one
- route_logits: float32 [768, 2], P('ep'), may hold values from -5 to 5
- expert_gate: bfloat16 [8, 4096, 3072], P('ep', None, 'tp'), may hold values from -0.09375 to 0.09375
- expert_up: bfloat16 [8, 4096, 3072], P('ep', None, 'tp'), may hold values from -0.09375 to 0.09375
- expert_down: bfloat16 [8, 3072, 4096], P('ep', 'tp'), may hold values from -0.109375 to 0.109375
- dense_gate: bfloat16 [4096, 6144], P('tp', 'ep'), may hold values from -0.09375 to 0.09375
- dense_up: bfloat16 [4096, 6144], P('tp', 'ep'), may hold values from -0.09375 to 0.09375
- dense_down: bfloat16 [6144, 4096], P('ep', 'tp'), may hold values from -0.078125 to 0.078125
- branch_gate: bfloat16 [4096], replicated, may hold values from -0.09375 to 0.09375
Outputs:
- output: bfloat16 [768, 4096], P('ep', 'tp')
- new_states: float32 [2, 768, 4096], P(None, 'ep', 'tp')
The draws below stay inside these ranges and needn't reach their ends.
Inputs may be any that keep to these rules, and one draw needn't show every extreme that they name: `route_ids`: each row names 2 different experts; among the rows of one device (aligned blocks of 96 rows) no expert is named by more than 48 rows.
All inputs are finite; a program needn't handle non-finite values.
Results may differ from the reference program's by a relative error of at most 0.017.
Values may be sent and summed in bfloat16 or wider, within the bound.
A program may use at most 128 MiB of HBM per device.

```python
import math
import jax
import jax.numpy as jnp
import numpy as np
from jax import lax

D = 4096
S5W = 1024
GROUP = 16
GROUPS = 64
STATE = 64
FFE = 3072
FFD = 6144
TOPK = 2
SEQ_DEV = 96
BATCH = 768
EXPERTS = 8
CAP = 48
N_EP = 8
N_TP = 4


def steps_of(own_key, dims, cuts, least, top_value):
    loudness, own = 1.0, jax.random.fold_in(own_key, 6)
    for axis_at, blocks in cuts:
        steps = jnp.exp(jax.random.uniform(jax.random.fold_in(own, axis_at), (blocks,), jnp.float32, least / len(cuts), top_value / len(cuts)))
        loudness = loudness * jnp.repeat(steps, dims[axis_at] // blocks).reshape([-1 if axis == axis_at else 1 for axis in range(len(dims))])
    return loudness


def deal_out(key, own, number, rows, number_of, top, bound, slope):
    sequence = jax.random.permutation(key, number_of)
    crowded, ordinary = portions_of(number_of, rows * top, bound, slope, True), portions_of(number_of, rows * top, bound, slope, False)
    places = jnp.arange(number_of)

    def named(lengths, turn):
        used = int((lengths > 0).sum())
        fixed = max(1, used // 4)
        passed = fixed + (places - fixed + turn * (used - fixed)) % max(1, number_of - fixed)
        return jnp.zeros((number_of,), jnp.int32).at[sequence[jnp.where(places < fixed, places, passed)]].set(jnp.asarray(lengths, jnp.int32))

    lengths = jnp.where(number % 4 == 0, named(crowded, number // 4), named(ordinary, number - number // 4 - 1))
    mixed = jax.random.permutation(jax.random.fold_in(own, 3), number_of)
    donor, receiver = mixed[0:number_of // 2 * 2:2], mixed[1:number_of // 2 * 2:2]
    slack = jnp.minimum(lengths[donor] - 1, bound - lengths[receiver]) // 2
    slack = jnp.where((donor == sequence[0]) | (receiver == sequence[0]) | (lengths[receiver] == 0), 0, jnp.maximum(slack, 0))
    passed = jax.random.randint(jax.random.fold_in(own, 4), (number_of // 2,), 0, 1 << 20) % (slack + 1)
    lengths = lengths.at[donor].add(-passed).at[receiver].add(passed)
    labels = jnp.searchsorted(jnp.cumsum(lengths), jnp.arange(rows * top), side="right").astype(jnp.int32)
    listing = labels.reshape(top, rows).T
    listing = listing[jax.random.permutation(jax.random.fold_in(own, 1), rows)]
    turn = jax.random.randint(jax.random.fold_in(own, 2), (rows, 1), 0, top)
    return jnp.take_along_axis(listing, (jnp.arange(top)[None, :] + turn) % top, axis=1)


def portions_of(amount, total, bound, slope, full):
    weights = [(1 << 20) // math.isqrt(standing ** slope) + 1 for standing in range(1, amount + 1)]
    largest = bound if full else min(bound, max(-(-total // amount), total * weights[0] // sum(weights)))
    least = 1 if total - largest >= amount - 1 else 0
    counts, rest = [largest] + [least] * (amount - 1), total - largest - least * (amount - 1)
    while rest > 0:
        free = [i for i in range(1, amount) if counts[i] < largest] or [i for i in range(1, amount) if counts[i] < bound]
        mass, budget = sum([weights[i] for i in free]), rest
        for i in free:
            addition = min(bound - counts[i], max(1, budget * weights[i] // mass), rest)
            counts[i] = counts[i] + addition
            rest = rest - addition
    return np.array(counts)


def noise(rng, extent, width, bound, pieces=(), kind=jnp.bfloat16):
    loudness = steps_of(rng, extent, pieces, -0.22, 0.18) if pieces else 1.0
    values = jax.random.normal(rng, extent, jnp.float32) * width * loudness
    return jnp.minimum(jnp.maximum(values, -bound), bound).astype(kind)


def setup_inputs(seed: int = 0) -> dict:
    seeds = jax.random.split(jax.random.key(seed), 24)
    tokens = noise(seeds[0], (BATCH, D), 1.0, 6.0, ((0, 8),))
    mix_gain = jnp.clip(1.0 + 0.18 * jax.random.normal(seeds[1], (D,), jnp.float32), 0.1, 1.9)
    ffn_gain = jnp.clip(1.0 + 0.18 * jax.random.normal(seeds[2], (D,), jnp.float32), 0.1, 1.9)
    in_proj = noise(seeds[3], (D, S5W), D ** -0.5, 0.09375, ((1, 4),))
    decay_rate = jnp.clip(jnp.exp(math.log(2.0) - 3.6888794 * jax.random.uniform(seeds[4], (GROUPS, STATE), jnp.float32) ** steps_of(seeds[4], (GROUPS, STATE), ((0, 4),), -0.2, 0.2)), 0.05, 2.0)
    frequency = jnp.clip(jax.random.uniform(seeds[5], (GROUPS, STATE), jnp.float32, -3.0, 3.0) * steps_of(seeds[5], (GROUPS, STATE), ((0, 4),), -0.4, 0.0), -3.0, 3.0)
    log_step = jnp.clip(-3.0 + 3.5 * jax.random.uniform(seeds[6], (GROUPS,), jnp.float32) ** steps_of(seeds[6], (GROUPS,), ((0, 4),), -0.2, 0.2), -3.0, 0.5)
    b_real = noise(seeds[7], (GROUPS, STATE, GROUP), GROUP ** -0.5, 1.5, ((0, 4),), jnp.float32)
    b_imag = noise(seeds[8], (GROUPS, STATE, GROUP), GROUP ** -0.5, 1.5, ((0, 4),), jnp.float32)
    c_real = noise(seeds[9], (GROUPS, GROUP, STATE), STATE ** -0.5, 0.75, ((0, 4),), jnp.float32)
    c_imag = noise(seeds[10], (GROUPS, GROUP, STATE), STATE ** -0.5, 0.75, ((0, 4),), jnp.float32)
    skip_gain = noise(seeds[11], (S5W,), 1.0, 5.0, ((0, 4),), jnp.float32)
    states = noise(seeds[12], (2, BATCH, GROUPS * STATE), 1.0, 6.0, ((1, 8), (2, 4)), jnp.float32)
    out_proj = noise(seeds[13], (S5W, D), S5W ** -0.5, 0.1875, ((0, 4),))
    route_ids_keys = jax.random.split(jax.random.fold_in(seeds[14], 1), BATCH // SEQ_DEV)
    route_ids_turns = jax.random.permutation(jax.random.fold_in(seeds[14], 3), BATCH // SEQ_DEV)
    route_ids = jax.vmap(lambda own, number: deal_out(jax.random.fold_in(seeds[14], 2), own, number, SEQ_DEV, EXPERTS, TOPK, CAP, 2))(route_ids_keys, route_ids_turns).reshape((BATCH, TOPK))
    route_logits = noise(seeds[15], (BATCH, TOPK), 1.0, 5.0, ((0, 8),), jnp.float32)
    expert_gate = noise(seeds[16], (EXPERTS, D, FFE), D ** -0.5, 0.09375, ((0, 8), (2, 4)))
    expert_up = noise(seeds[17], (EXPERTS, D, FFE), D ** -0.5, 0.09375, ((0, 8), (2, 4)))
    expert_down = noise(seeds[18], (EXPERTS, FFE, D), FFE ** -0.5, 0.109375, ((0, 8), (1, 4)))
    dense_gate = noise(seeds[19], (D, FFD), D ** -0.5, 0.09375, ((0, 4), (1, 8)))
    dense_up = noise(seeds[20], (D, FFD), D ** -0.5, 0.09375, ((0, 4), (1, 8)))
    dense_down = noise(seeds[21], (FFD, D), FFD ** -0.5, 0.078125, ((0, 8), (1, 4)))
    branch_gate = noise(seeds[22], (D,), D ** -0.5, 0.09375)
    return dict(tokens=tokens, mix_gain=mix_gain, ffn_gain=ffn_gain, in_proj=in_proj, decay_rate=decay_rate, frequency=frequency, log_step=log_step, b_real=b_real, b_imag=b_imag, c_real=c_real, c_imag=c_imag, skip_gain=skip_gain, states=states, out_proj=out_proj, route_ids=route_ids, route_logits=route_logits, expert_gate=expert_gate, expert_up=expert_up, expert_down=expert_down, dense_gate=dense_gate, dense_up=dense_up, dense_down=dense_down, branch_gate=branch_gate)


def rms_norm(values, gain):
    flt = values.astype(jnp.float32)
    scaled = flt * lax.rsqrt(lax.optimization_barrier(jnp.mean(flt * flt, axis=-1, keepdims=True)) + 1e-06)
    return (scaled * gain.astype(jnp.float32)).astype(jnp.bfloat16)

def discretize(decay_rate, frequency, log_step, b_real, b_imag):
    step_size = jnp.exp(log_step)[:, None]
    lam_re = -decay_rate
    lam_im = frequency
    magnitude = jnp.exp(lam_re * step_size)
    abar_re = magnitude * jnp.cos(lam_im * step_size)
    abar_im = magnitude * jnp.sin(lam_im * step_size)
    denom = lam_re * lam_re + lam_im * lam_im
    fac_re = ((abar_re - 1.0) * lam_re + abar_im * lam_im) / denom
    fac_im = (abar_im * lam_re - (abar_re - 1.0) * lam_im) / denom
    bbar_re = fac_re[..., None] * b_real - fac_im[..., None] * b_imag
    bbar_im = fac_re[..., None] * b_imag + fac_im[..., None] * b_real
    return (abar_re, abar_im, bbar_re, bbar_im)

def state_step(drive, states, decay_rate, frequency, log_step, b_real, b_imag, c_real, c_imag, skip_gain):
    count = drive.shape[0]
    groups = decay_rate.shape[0]
    abar_re, abar_im, bbar_re, bbar_im = discretize(decay_rate, frequency, log_step, b_real, b_imag)
    grouped = drive.astype(jnp.float32).reshape(count, groups, GROUP)
    old_re = states[0].reshape(count, groups, STATE)
    old_im = states[1].reshape(count, groups, STATE)
    high = lax.Precision.HIGHEST
    push_re = jnp.einsum('ngh,gph->ngp', grouped, bbar_re, precision=high)
    push_im = jnp.einsum('ngh,gph->ngp', grouped, bbar_im, precision=high)
    new_re = abar_re * old_re - abar_im * old_im + push_re
    new_im = abar_re * old_im + abar_im * old_re + push_im
    readout = jnp.einsum('ngp,ghp->ngh', new_re, c_real, precision=high) - jnp.einsum('ngp,ghp->ngh', new_im, c_imag, precision=high) + skip_gain.reshape(groups, GROUP) * grouped
    reads = jax.nn.gelu(readout.reshape(count, groups * GROUP)).astype(jnp.bfloat16)
    fresh = jnp.stack([new_re.reshape(count, groups * STATE), new_im.reshape(count, groups * STATE)])
    return (reads, fresh)

def reference(tokens, mix_gain, ffn_gain, in_proj, decay_rate, frequency, log_step, b_real, b_imag, c_real, c_imag, skip_gain, states, out_proj, route_ids, route_logits, expert_gate, expert_up, expert_down, dense_gate, dense_up, dense_down, branch_gate):
    normed = rms_norm(tokens, mix_gain)
    drive = jnp.dot(normed, in_proj, preferred_element_type=jnp.float32).astype(jnp.bfloat16)
    reads, new_states = state_step(drive, states, decay_rate, frequency, log_step, b_real, b_imag, c_real, c_imag, skip_gain)
    block_width = S5W // N_TP
    mixed = jnp.zeros((BATCH, D), jnp.float32)
    for block in range(N_TP):
        piece = jnp.dot(reads[:, block * block_width:(block + 1) * block_width], out_proj[block * block_width:(block + 1) * block_width], preferred_element_type=jnp.float32).astype(jnp.bfloat16)
        mixed = mixed + piece.astype(jnp.float32)
    mixed = mixed.astype(jnp.bfloat16)
    resid = (tokens.astype(jnp.float32) + mixed.astype(jnp.float32)).astype(jnp.bfloat16)
    normed_two = rms_norm(resid, ffn_gain)
    route_weights = jax.nn.softmax(route_logits, axis=-1)
    blocked_ids = route_ids.reshape(N_EP, SEQ_DEV * TOPK)
    onehot = (blocked_ids[..., None] == jnp.arange(EXPERTS, dtype=jnp.int32)[None, None, :]).astype(jnp.int32)
    rank = jnp.cumsum(onehot, axis=1) - onehot
    slot = lax.optimization_barrier(jnp.sum(rank * onehot, axis=-1))
    block_index = jnp.arange(N_EP, dtype=jnp.int32)[:, None]
    position = blocked_ids * (N_EP * CAP) + block_index * CAP + slot
    token_index = block_index * SEQ_DEV + jnp.arange(SEQ_DEV * TOPK, dtype=jnp.int32)[None, :] // TOPK
    table = jnp.full((EXPERTS * N_EP * CAP,), BATCH, jnp.int32).at[position.reshape(-1)].set(token_index.reshape(-1))
    padded = jnp.concatenate([normed_two, jnp.zeros((1, D), jnp.bfloat16)], axis=0)
    hidden_block = FFE // N_TP

    def one_expert(inputs):
        index_row, gate_w, up_w, down_w = inputs
        rows_in = padded[index_row]
        summed = jnp.zeros((N_EP * CAP, D), jnp.float32)
        for block in range(N_TP):
            lo = block * hidden_block
            gate_val = jnp.dot(rows_in, gate_w[:, lo:lo + hidden_block], preferred_element_type=jnp.float32)
            up_val = jnp.dot(rows_in, up_w[:, lo:lo + hidden_block], preferred_element_type=jnp.float32)
            hidden = (jax.nn.silu(gate_val) * up_val).astype(jnp.bfloat16)
            piece = jnp.dot(hidden, down_w[lo:lo + hidden_block], preferred_element_type=jnp.float32)
            summed = summed + piece.astype(jnp.bfloat16).astype(jnp.float32)
        return summed.astype(jnp.bfloat16)
    expert_out = lax.map(one_expert, (table.reshape(EXPERTS, N_EP * CAP), expert_gate, expert_up, expert_down))
    picked = expert_out.reshape(EXPERTS * N_EP * CAP, D)[position.reshape(-1)]
    picked = picked.reshape(BATCH, TOPK, D).astype(jnp.float32)
    routed = lax.optimization_barrier(jnp.sum(route_weights[..., None] * picked, axis=1))
    gate_val = jnp.dot(normed_two, dense_gate, preferred_element_type=jnp.float32)
    up_val = jnp.dot(normed_two, dense_up, preferred_element_type=jnp.float32)
    dense_hidden = (jax.nn.silu(gate_val) * up_val).astype(jnp.bfloat16)
    dense_term = jnp.dot(dense_hidden, dense_down, preferred_element_type=jnp.float32)
    branch = jax.nn.sigmoid(jnp.dot(normed_two, branch_gate, preferred_element_type=jnp.float32))
    output = (resid.astype(jnp.float32) + routed + branch[:, None] * dense_term).astype(jnp.bfloat16)
    return (output, new_states)
```

```python
import functools
import jax
import jax.numpy as jnp
from jax import lax
from jax.experimental import pallas as pl
from jax.experimental.pallas import tpu as pltpu
from jax.sharding import PartitionSpec as P

GROUP = 16
STATE = 64
MESH = pl.DeviceIdType.MESH


def fast_extent(axis, size):
    if axis == "tp":
        return 2
    extent = 1
    while (2 * extent) * (2 * extent) * 2 <= size:
        extent *= 2
    return extent


class Grid:
    def __init__(self, axis, size):
        self.axis, self.size = axis, size
        self.fast = fast_extent(axis, size)
        self.slow = size // self.fast
        self.me = lax.axis_index(axis)
        self.at_fast = self.me % self.fast
        self.at_slow = self.me // self.fast

    def index(self, slow_step, fast_step):
        slow_at = (self.at_slow + slow_step + self.slow) % self.slow
        fast_at = (self.at_fast + fast_step + self.fast) % self.fast
        return slow_at * self.fast + fast_at

    def peers(self):
        return [self.index(k, 0) for k in range(1, self.slow)] + [
            self.index(0, q) for q in range(1, self.fast)
        ]

    def greet(self):
        barrier = pltpu.get_barrier_semaphore()
        peers = self.peers()
        for peer in peers:
            pl.semaphore_signal(barrier, inc=1, device_id={self.axis: peer}, device_id_type=MESH)
        pl.semaphore_wait(barrier, len(peers))

    def greet_all(self):
        barrier = pltpu.get_barrier_semaphore()
        for k in range(1, self.size):
            pl.semaphore_signal(
                barrier,
                inc=1,
                device_id={self.axis: (self.me + k) % self.size},
                device_id_type=MESH,
            )
        pl.semaphore_wait(barrier, self.size - 1)

    def copy(self, source, target, sent, landed, peer):
        return pltpu.make_async_remote_copy(
            src_ref=source,
            dst_ref=target,
            send_sem=sent,
            recv_sem=landed,
            device_id={self.axis: peer},
            device_id_type=MESH,
        )


def part_of(ref, owner, start, rows, width, cols):
    if cols:
        return ref.at[pl.ds(start, rows), pl.ds(pl.multiple_of(owner * width, 128), width)]
    return ref.at[owner, pl.ds(start, rows), :]


def gather_kernel(axis, size, pieces, cols, *refs):
    count = len(pieces)
    ins, outs = refs[:count], refs[count : 2 * count]
    slow_sent, slow_landed, fast_sent, fast_landed, own_sem = refs[2 * count :]
    grid = Grid(axis, size)
    spans = []
    for item, number in enumerate(pieces):
        rows = ins[item].shape[0] // number
        spans += [(item, j, j * rows, rows) for j in range(number)]

    def place(item, owner, start, rows):
        return part_of(outs[item], owner, start, rows, ins[item].shape[1], cols)

    grid.greet()
    pending = []
    for item, j, start, rows in spans:
        for k in range(1, grid.slow):
            copy = grid.copy(
                ins[item].at[pl.ds(start, rows), :],
                place(item, grid.me, start, rows),
                slow_sent.at[item, j, k - 1],
                slow_landed.at[item, j, k - 1],
                grid.index(k, 0),
            )
            copy.start()
            pending.append(copy)
    for item, j, start, rows in spans:
        for q in range(1, grid.fast):
            copy = grid.copy(
                ins[item].at[pl.ds(start, rows), :],
                place(item, grid.me, start, rows),
                fast_sent.at[item, j, 0, q - 1],
                fast_landed.at[item, j, 0, q - 1],
                grid.index(0, q),
            )
            copy.start()
            pending.append(copy)
    owns = []
    for item in range(count):
        own = pltpu.make_async_copy(
            ins[item], place(item, grid.me, 0, ins[item].shape[0]), own_sem.at[item]
        )
        own.start()
        owns.append(own)
    for item, j, start, rows in spans:
        for k in range(1, grid.slow):
            block = place(item, grid.index(-k, 0), start, rows)
            grid.copy(
                block,
                block,
                slow_sent.at[item, j, k - 1],
                slow_landed.at[item, j, k - 1],
                grid.index(-k, 0),
            ).wait_recv()
            for q in range(1, grid.fast):
                copy = grid.copy(
                    block,
                    block,
                    fast_sent.at[item, j, k, q - 1],
                    fast_landed.at[item, j, k, q - 1],
                    grid.index(0, q),
                )
                copy.start()
                pending.append(copy)
    for item, j, start, rows in spans:
        for k in range(grid.slow):
            for q in range(1, grid.fast):
                block = place(item, grid.index(-k, -q), start, rows)
                grid.copy(
                    block,
                    block,
                    fast_sent.at[item, j, k, q - 1],
                    fast_landed.at[item, j, k, q - 1],
                    grid.index(0, -q),
                ).wait_recv()
    for copy in pending:
        copy.wait_send()
    for own in owns:
        own.wait()


def all_gather(arrays, axis, size, pieces, cols, collective_id):
    shapes = []
    for array in arrays:
        rows, width = array.shape
        shape = (rows, size * width) if cols else (size, rows, width)
        shapes.append(jax.ShapeDtypeStruct(shape, array.dtype))
    fast = fast_extent(axis, size)
    slow = size // fast
    count, most = len(arrays), max(pieces)
    sems = [
        pltpu.SemaphoreType.DMA((count, most, slow - 1)),
        pltpu.SemaphoreType.DMA((count, most, slow - 1)),
        pltpu.SemaphoreType.DMA((count, most, slow, fast - 1)),
        pltpu.SemaphoreType.DMA((count, most, slow, fast - 1)),
        pltpu.SemaphoreType.DMA((count,)),
    ]
    return pl.pallas_call(
        functools.partial(gather_kernel, axis, size, pieces, cols),
        out_shape=shapes,
        in_specs=[pl.BlockSpec(memory_space=pltpu.VMEM)] * count,
        out_specs=[pl.BlockSpec(memory_space=pltpu.VMEM)] * count,
        scratch_shapes=sems,
        compiler_params=pltpu.CompilerParams(
            collective_id=collective_id, has_side_effects=True, vmem_limit_bytes=16 << 20
        ),
    )(*arrays)


def reduce_kernel(
    axis,
    size,
    number,
    cols,
    x_ref,
    o_ref,
    got_fast,
    mid,
    got_slow,
    total_ref,
    fast_sent,
    fast_landed,
    slow_sent,
    slow_landed,
):
    grid = Grid(axis, size)
    rows, width = o_ref.shape
    step = rows // number
    grid.greet()
    pending = []
    for k in range(1, grid.slow + 1):
        for j in range(number):
            for q in range(1, grid.fast):
                copy = grid.copy(
                    part_of(x_ref, grid.index(k, q), j * step, step, width, cols),
                    got_fast.at[q - 1, k - 1, pl.ds(j * step, step), :],
                    fast_sent.at[q - 1, k - 1, j],
                    fast_landed.at[q - 1, k - 1, j],
                    grid.index(0, q),
                )
                copy.start()
                pending.append(copy)
    for k in range(1, grid.slow + 1):
        for j in range(number):
            span = pl.ds(j * step, step)
            total = part_of(x_ref, grid.index(k, 0), j * step, step, width, cols)[...].astype(
                jnp.float32
            )
            for q in range(1, grid.fast):
                block = got_fast.at[q - 1, k - 1, span, :]
                grid.copy(
                    block,
                    block,
                    fast_sent.at[q - 1, k - 1, j],
                    fast_landed.at[q - 1, k - 1, j],
                    grid.index(0, -q),
                ).wait_recv()
                total = total + block[...].astype(jnp.float32)
            if k == grid.slow:
                total_ref[span, :] = total
            else:
                mid[k - 1, span, :] = total.astype(mid.dtype)
                copy = grid.copy(
                    mid.at[k - 1, span, :],
                    got_slow.at[k - 1, span, :],
                    slow_sent.at[k - 1, j],
                    slow_landed.at[k - 1, j],
                    grid.index(k, 0),
                )
                copy.start()
                pending.append(copy)
    for j in range(number):
        span = pl.ds(j * step, step)
        total = total_ref[span, :]
        for k in range(1, grid.slow):
            block = got_slow.at[k - 1, span, :]
            grid.copy(
                block,
                block,
                slow_sent.at[k - 1, j],
                slow_landed.at[k - 1, j],
                grid.index(-k, 0),
            ).wait_recv()
            total = total + block[...].astype(jnp.float32)
        o_ref[span, :] = total.astype(o_ref.dtype)
    for copy in pending:
        copy.wait_send()


def reduce_scatter(array, axis, size, number, cols, collective_id):
    if cols:
        rows, width = array.shape[0], array.shape[1] // size
    else:
        rows, width = array.shape[1:]
    fast = fast_extent(axis, size)
    slow = size // fast
    return pl.pallas_call(
        functools.partial(reduce_kernel, axis, size, number, cols),
        out_shape=jax.ShapeDtypeStruct((rows, width), array.dtype),
        in_specs=[pl.BlockSpec(memory_space=pltpu.VMEM)],
        out_specs=pl.BlockSpec(memory_space=pltpu.VMEM),
        scratch_shapes=[
            pltpu.VMEM((fast - 1, slow, rows, width), array.dtype),
            pltpu.VMEM((slow - 1, rows, width), array.dtype),
            pltpu.VMEM((slow - 1, rows, width), array.dtype),
            pltpu.VMEM((rows, width), jnp.float32),
            pltpu.SemaphoreType.DMA((fast - 1, slow, number)),
            pltpu.SemaphoreType.DMA((fast - 1, slow, number)),
            pltpu.SemaphoreType.DMA((slow - 1, number)),
            pltpu.SemaphoreType.DMA((slow - 1, number)),
        ],
        compiler_params=pltpu.CompilerParams(
            collective_id=collective_id, has_side_effects=True, vmem_limit_bytes=24 << 20
        ),
    )(array)

class Gather:
    def __init__(self, grid, source, target, number, cols, sems):
        self.grid, self.source, self.target, self.cols = grid, source, target, cols
        self.slow_sent, self.slow_landed, self.fast_sent, self.fast_landed, self.own_sem = sems
        self.rows, self.width = source.shape
        self.step = self.rows // number
        self.number = number
        self.pending = []

    def place(self, owner, j):
        return part_of(self.target, owner, j * self.step, self.step, self.width, self.cols)

    def slow_copy(self, source, target, j, k, peer):
        return self.grid.copy(
            source, target, self.slow_sent.at[j, k - 1], self.slow_landed.at[j, k - 1], peer
        )

    def fast_copy(self, source, target, j, k, q, peer):
        return self.grid.copy(
            source, target, self.fast_sent.at[j, k, q - 1], self.fast_landed.at[j, k, q - 1], peer
        )

    def launch(self, copy):
        copy.start()
        self.pending.append(copy)

    def start(self):
        grid = self.grid
        for j in range(self.number):
            piece = self.source.at[pl.ds(j * self.step, self.step), :]
            spot = self.place(grid.me, j)
            for k in range(1, grid.slow):
                self.launch(self.slow_copy(piece, spot, j, k, grid.index(k, 0)))
        for j in range(self.number):
            piece = self.source.at[pl.ds(j * self.step, self.step), :]
            spot = self.place(grid.me, j)
            for q in range(1, grid.fast):
                self.launch(self.fast_copy(piece, spot, j, 0, q, grid.index(0, q)))
        self.own = pltpu.make_async_copy(
            self.source,
            part_of(self.target, grid.me, 0, self.rows, self.width, self.cols),
            self.own_sem,
        )
        self.own.start()

    def relay(self):
        grid = self.grid
        for j in range(self.number):
            for k in range(1, grid.slow):
                spot = self.place(grid.index(-k, 0), j)
                self.slow_copy(spot, spot, j, k, grid.index(-k, 0)).wait_recv()
                for q in range(1, grid.fast):
                    self.launch(self.fast_copy(spot, spot, j, k, q, grid.index(0, q)))

    def arrive(self):
        grid = self.grid
        for j in range(self.number):
            for k in range(grid.slow):
                for q in range(1, grid.fast):
                    spot = self.place(grid.index(-k, -q), j)
                    self.fast_copy(spot, spot, j, k, q, grid.index(0, -q)).wait_recv()
        self.own.wait()

    def finish(self):
        for copy in self.pending:
            copy.wait_send()


def gather_sems(grid_fast, grid_slow, number):
    return [
        pltpu.SemaphoreType.DMA((number, grid_slow - 1)),
        pltpu.SemaphoreType.DMA((number, grid_slow - 1)),
        pltpu.SemaphoreType.DMA((number, grid_slow, grid_fast - 1)),
        pltpu.SemaphoreType.DMA((number, grid_slow, grid_fast - 1)),
        pltpu.SemaphoreType.DMA,
    ]


class Reduce:
    def __init__(self, grid, source, number, cols, scratch):
        self.grid, self.source, self.cols, self.number = grid, source, cols, number
        self.got_fast, self.mid, self.got_slow, self.total = scratch[:4]
        self.fast_sent, self.fast_landed, self.slow_sent, self.slow_landed = scratch[4:]
        rows, self.width = self.total.shape
        self.step = rows // number
        self.pending = []

    def part(self, dest, j):
        return part_of(self.source, dest, j * self.step, self.step, self.width, self.cols)

    def span(self, j):
        return pl.ds(j * self.step, self.step)

    def fast_copy(self, source, k, j, q, peer):
        return self.grid.copy(
            source,
            self.got_fast.at[q - 1, k - 1, self.span(j), :],
            self.fast_sent.at[q - 1, k - 1, j],
            self.fast_landed.at[q - 1, k - 1, j],
            peer,
        )

    def slow_copy(self, k, j, peer):
        return self.grid.copy(
            self.mid.at[k - 1, self.span(j), :],
            self.got_slow.at[k - 1, self.span(j), :],
            self.slow_sent.at[k - 1, j],
            self.slow_landed.at[k - 1, j],
            peer,
        )

    def push_part(self, k, q):
        grid = self.grid
        for j in range(self.number):
            copy = self.fast_copy(self.part(grid.index(k, q), j), k, j, q, grid.index(0, q))
            copy.start()
            self.pending.append(copy)

    def push(self):
        for k in range(1, self.grid.slow + 1):
            for q in range(1, self.grid.fast):
                self.push_part(k, q)

    def relay(self):
        grid = self.grid
        for k in range(1, grid.slow + 1):
            for j in range(self.number):
                value = self.part(grid.index(k, 0), j)[...].astype(jnp.float32)
                for q in range(1, grid.fast):
                    block = self.got_fast.at[q - 1, k - 1, self.span(j), :]
                    self.fast_copy(block, k, j, q, grid.index(0, -q)).wait_recv()
                    value = value + block[...].astype(jnp.float32)
                if k == grid.slow:
                    self.total[self.span(j), :] = value
                else:
                    self.mid[k - 1, self.span(j), :] = value.astype(self.mid.dtype)
                    copy = self.slow_copy(k, j, grid.index(k, 0))
                    copy.start()
                    self.pending.append(copy)

    def collect(self, emit):
        grid = self.grid
        for j in range(self.number):
            value = self.total[self.span(j), :]
            for k in range(1, grid.slow):
                self.slow_copy(k, j, grid.index(-k, 0)).wait_recv()
                value = value + self.got_slow[k - 1, self.span(j), :].astype(jnp.float32)
            emit(self.span(j), value)

    def finish(self):
        for copy in self.pending:
            copy.wait_send()


def reduce_scratch(fast, slow, rows, width, number):
    return [
        pltpu.VMEM((fast - 1, slow, rows, width), jnp.bfloat16),
        pltpu.VMEM((slow - 1, rows, width), jnp.bfloat16),
        pltpu.VMEM((slow - 1, rows, width), jnp.bfloat16),
        pltpu.VMEM((rows, width), jnp.float32),
        pltpu.SemaphoreType.DMA((fast - 1, slow, number)),
        pltpu.SemaphoreType.DMA((fast - 1, slow, number)),
        pltpu.SemaphoreType.DMA((slow - 1, number)),
        pltpu.SemaphoreType.DMA((slow - 1, number)),
    ]


def tile_of(extent):
    for tile in (256, 128):
        if extent % tile == 0:
            return tile
    return extent


def branches_kernel(
    axis,
    size,
    rows_ref,
    cols_ref,
    dense_gate,
    dense_up,
    gate_hbm,
    up_hbm,
    down_hbm,
    dense_out,
    expert_out,
    full,
    gate,
    up,
    down,
    both,
    own_hidden,
    hidden,
    part,
    weight_sems,
    *rest,
):
    grid = Grid(axis, size)
    rows_gather = Gather(grid, rows_ref, full, ROW_PIECES, True, rest[:5])
    hidden_gather = Gather(grid, own_hidden, dense_out, 2, False, rest[5:10])
    dense_sum = Reduce(grid, both, 4, False, rest[10:18])
    expert_sum = Reduce(grid, part, 4, True, rest[18:26])
    loads = []
    for item, (source, target) in enumerate(((gate_hbm, gate), (up_hbm, up), (down_hbm, down))):
        load = pltpu.make_async_copy(source, target, weight_sems.at[item])
        load.start()
        loads.append(load)
    grid.greet()
    rows_gather.start()
    share, double = both.shape[1:]
    width = double // 2

    @pl.loop(0, size)
    def _(dest):
        start = pl.multiple_of(dest * share, 16)
        block = cols_ref[pl.ds(start, share), :]
        both[dest, :, :width] = jnp.dot(
            block, dense_gate[...], preferred_element_type=jnp.float32
        ).astype(jnp.bfloat16)
        both[dest, :, width:] = jnp.dot(
            block, dense_up[...], preferred_element_type=jnp.float32
        ).astype(jnp.bfloat16)

    dense_sum.push()
    dense_sum.relay()
    rows_gather.relay()
    rows_gather.arrive()
    loads[0].wait()
    loads[1].wait()
    inner = hidden.shape[1]
    tile = tile_of(inner)

    @pl.loop(0, inner // tile)
    def _(step):
        span = pl.ds(pl.multiple_of(step * tile, 128), tile)
        gate_val = jnp.dot(full[...], gate[:, span], preferred_element_type=jnp.float32)
        up_val = jnp.dot(full[...], up[:, span], preferred_element_type=jnp.float32)
        hidden[:, span] = (jax.nn.silu(gate_val) * up_val).astype(jnp.bfloat16)

    def emit_hidden(span, value):
        own_hidden[span, :] = (jax.nn.silu(value[:, :width]) * value[:, width:]).astype(
            jnp.bfloat16
        )

    dense_sum.collect(emit_hidden)
    loads[2].wait()
    hidden_gather.start()
    wide = 2 * tile_of(part.shape[1])

    @pl.loop(0, part.shape[1] // wide)
    def _(step):
        span = pl.ds(pl.multiple_of(step * wide, 128), wide)
        part[:, span] = jnp.dot(
            hidden[...], down[:, span], preferred_element_type=jnp.float32
        ).astype(jnp.bfloat16)

    expert_sum.push()
    expert_sum.relay()
    hidden_gather.relay()
    hidden_gather.arrive()

    def emit_expert(span, value):
        expert_out[span, :] = value.astype(expert_out.dtype)

    expert_sum.collect(emit_expert)
    for phase in (rows_gather, hidden_gather, dense_sum, expert_sum):
        phase.finish()


ROW_PIECES = 4


def branches(rows, every_cols, dense_gate, dense_up, gate, up, down, axis, size, collective_id):
    room, width = rows.shape
    total, hidden_width = every_cols.shape[0], dense_gate.shape[1]
    share, inner = total // size, gate.shape[1]
    fast = fast_extent(axis, size)
    slow = size // fast
    whole = pl.BlockSpec(memory_space=pltpu.VMEM)
    far = pl.BlockSpec(memory_space=pl.ANY)
    bf16 = jnp.bfloat16
    return pl.pallas_call(
        functools.partial(branches_kernel, axis, size),
        out_shape=(
            jax.ShapeDtypeStruct((size, share, hidden_width), bf16),
            jax.ShapeDtypeStruct((room, width), bf16),
        ),
        in_specs=[whole] * 4 + [far] * 3,
        out_specs=(whole, whole),
        scratch_shapes=[
            pltpu.VMEM((room, size * width), bf16),
            pltpu.VMEM(gate.shape, bf16),
            pltpu.VMEM(up.shape, bf16),
            pltpu.VMEM(down.shape, bf16),
            pltpu.VMEM((size, share, 2 * hidden_width), bf16),
            pltpu.VMEM((share, hidden_width), bf16),
            pltpu.VMEM((room, inner), bf16),
            pltpu.VMEM((room, size * width), bf16),
            pltpu.SemaphoreType.DMA((3,)),
        ]
        + gather_sems(fast, slow, ROW_PIECES)
        + gather_sems(fast, slow, 2)
        + reduce_scratch(fast, slow, share, 2 * hidden_width, 4)
        + reduce_scratch(fast, slow, room, width, 4),
        compiler_params=pltpu.CompilerParams(
            collective_id=collective_id, has_side_effects=True, vmem_limit_bytes=54 << 20
        ),
    )(rows, every_cols, dense_gate, dense_up, gate, up, down)


def mixer_kernel(
    tokens,
    mix_gain,
    in_proj_hbm,
    decay_rate,
    frequency,
    log_step,
    b_real,
    b_imag,
    c_real,
    c_imag,
    skip_gain,
    states_hbm,
    reads,
    fresh_hbm,
    in_proj,
    old,
    fresh,
    normed,
    sems,
):
    load_proj = pltpu.make_async_copy(in_proj_hbm, in_proj, sems.at[0])
    load_old = pltpu.make_async_copy(states_hbm, old, sems.at[1])
    load_proj.start()
    load_old.start()
    count, width = tokens.shape
    groups, entries = decay_rate.shape
    channels = skip_gain.shape[1]
    wide = groups * entries
    f32, bf16 = jnp.float32, jnp.bfloat16

    def iota(shape, dim):
        return lax.broadcasted_iota(jnp.int32, shape, dim)

    eye = iota((groups, groups), 0) == iota((groups, groups), 1)
    step_size = jnp.exp(jnp.sum(jnp.where(eye, log_step[...], 0.0), axis=1, keepdims=True))
    lam_re, lam_im = -decay_rate[...], frequency[...]
    magnitude = jnp.exp(lam_re * step_size)
    abar_re = magnitude * jnp.cos(lam_im * step_size)
    abar_im = magnitude * jnp.sin(lam_im * step_size)
    denom = lam_re * lam_re + lam_im * lam_im
    fac_re = ((abar_re - 1.0) * lam_re + abar_im * lam_im) / denom
    fac_im = (abar_im * lam_re - (abar_re - 1.0) * lam_im) / denom
    packed = jnp.concatenate([abar_re, abar_im, fac_re, fac_im], axis=0)
    repeat = (iota((entries, wide), 1) % entries == iota((entries, wide), 0)).astype(f32)
    spread = jnp.dot(packed, repeat, precision=lax.Precision.HIGHEST, preferred_element_type=f32)
    owner = iota((groups, wide), 1) // entries == iota((groups, wide), 0)

    def row_of(item):
        part = spread[item * groups : (item + 1) * groups]
        return jnp.sum(jnp.where(owner, part, 0.0), axis=0, keepdims=True)

    abar_re, abar_im, fac_re, fac_im = (row_of(item) for item in range(4))
    inside = iota((wide, channels), 0) // entries == iota((wide, channels), 1) // GROUP
    place_in = (iota((GROUP, channels), 1) % GROUP == iota((GROUP, channels), 0)).astype(bf16)
    place_out = (iota((entries, wide), 1) % entries == iota((entries, wide), 0)).astype(bf16)
    inside_out = iota((channels, wide), 0) // GROUP == iota((channels, wide), 1) // entries

    def in_matrix(ref):
        flat = ref[...].reshape(wide, GROUP).astype(bf16)
        full = jnp.dot(flat, place_in, preferred_element_type=f32)
        return jnp.where(inside, full, 0.0).astype(bf16)

    def out_matrix(ref):
        flat = ref[...].reshape(channels, entries).astype(bf16)
        full = jnp.dot(flat, place_out, preferred_element_type=f32)
        return jnp.where(inside_out, full, 0.0).astype(bf16)

    def by_rows(left, right):
        return lax.dot_general(
            left, right, (((1,), (1,)), ((), ())), preferred_element_type=f32
        )

    step = 16
    for start in range(0, count, step):
        flt = tokens[start : start + step, :].astype(f32)
        scale = lax.rsqrt(jnp.mean(flt * flt, axis=-1, keepdims=True) + 1e-06)
        normed[start : start + step, :] = (flt * scale * mix_gain[...]).astype(bf16)
    load_proj.wait()
    drive = jnp.dot(normed[...], in_proj[...], preferred_element_type=f32).astype(bf16)
    push_a = by_rows(drive, in_matrix(b_real))
    push_b = by_rows(drive, in_matrix(b_imag))
    load_old.wait()
    old_re, old_im = old[0], old[1]
    new_re = abar_re * old_re - abar_im * old_im + fac_re * push_a - fac_im * push_b
    fresh[0] = new_re
    new_im = abar_re * old_im + abar_im * old_re + fac_re * push_b + fac_im * push_a
    fresh[1] = new_im
    store = pltpu.make_async_copy(fresh, fresh_hbm, sems.at[2])
    store.start()
    readout = (
        by_rows(new_re.astype(bf16), out_matrix(c_real))
        - by_rows(new_im.astype(bf16), out_matrix(c_imag))
        + skip_gain[...] * drive.astype(f32)
    )
    reads[...] = jax.nn.gelu(readout).astype(bf16)
    store.wait()


def mixer(tokens, mix_gain, in_proj, params, skip_gain, states):
    count = tokens.shape[0]
    channels = in_proj.shape[1]
    whole = pl.BlockSpec(memory_space=pltpu.VMEM)
    far = pl.BlockSpec(memory_space=pl.ANY)
    return pl.pallas_call(
        mixer_kernel,
        out_shape=(
            jax.ShapeDtypeStruct((count, channels), jnp.bfloat16),
            jax.ShapeDtypeStruct(states.shape, jnp.float32),
        ),
        in_specs=[whole, whole, far] + [whole] * 8 + [far],
        out_specs=(whole, far),
        scratch_shapes=[
            pltpu.VMEM(in_proj.shape, jnp.bfloat16),
            pltpu.VMEM(states.shape, jnp.float32),
            pltpu.VMEM(states.shape, jnp.float32),
            pltpu.VMEM(tokens.shape, jnp.bfloat16),
            pltpu.SemaphoreType.DMA((3,)),
        ],
        compiler_params=pltpu.CompilerParams(vmem_limit_bytes=40 << 20),
    )(tokens, mix_gain, in_proj, *params, skip_gain, states)


def exit_kernel(
    size,
    reads,
    out_proj,
    tokens,
    ffn_gain,
    branch_gate,
    route_ids,
    route_logits,
    own_cols,
    resid_cols,
    side,
    partial,
    stat,
    stat_got,
    stat_sent,
    stat_landed,
    *scratch,
):
    f32, bf16 = jnp.float32, jnp.bfloat16
    grid = Grid("tp", size)
    mix = Reduce(grid, partial, MIX_PIECES, True, scratch)
    count, width = resid_cols.shape
    grid.greet_all()

    def block(dest):
        span = pl.ds(pl.multiple_of(dest * width, 128), width)
        partial[:, span] = jnp.dot(
            reads[...], out_proj[:, span], preferred_element_type=f32
        ).astype(bf16)

    for k in range(1, grid.slow + 1):
        for q in range(1, grid.fast):
            block(grid.index(k, q))
            mix.push_part(k, q)
    for k in range(1, grid.slow + 1):
        block(grid.index(k, 0))
    logits = route_logits[...]
    top = logits.shape[1]
    raised = jnp.exp(logits - jnp.max(logits, axis=1, keepdims=True))
    weights = raised / jnp.sum(raised, axis=1, keepdims=True)
    ids = route_ids[...].astype(f32)
    mix.relay()
    mine = pl.ds(pl.multiple_of(grid.me * width, 128), width)
    gain = ffn_gain[:, mine]
    gate = gain * branch_gate[:, mine]
    lanes = lax.broadcasted_iota(jnp.int32, (count, 128), 1)
    ssq_parts, dot_parts = [], []

    def emit(span, value):
        mixed = value.astype(bf16).astype(f32)
        resid = (tokens[span, mine].astype(f32) + mixed).astype(bf16)
        resid_cols[span, :] = resid
        flt = resid.astype(f32)
        ssq_parts.append(jnp.sum(flt * flt, axis=1, keepdims=True))
        dot_parts.append(jnp.sum(flt * gate, axis=1, keepdims=True))

    mix.collect(emit)
    ssq, dots = jnp.concatenate(ssq_parts, axis=0), jnp.concatenate(dot_parts, axis=0)
    table = jnp.where(lanes == 0, ssq, jnp.where(lanes == 1, dots, 0.0))
    for item in range(top):
        table = jnp.where(lanes == 2 + item, ids[:, item : item + 1], table)
        table = jnp.where(lanes == 2 + top + item, weights[:, item : item + 1], table)
    if count < 128:
        table = jnp.concatenate([table, jnp.zeros((128 - count, 128), f32)], axis=0)
    turned = table.T
    stat[...] = turned[:8]
    copies = []
    for k in range(1, size):
        copy = grid.copy(
            stat,
            stat_got.at[k - 1],
            stat_sent.at[k - 1],
            stat_landed.at[k - 1],
            (grid.me + k) % size,
        )
        copy.start()
        copies.append(copy)
    total = turned[:8]
    for copy in copies:
        copy.wait_recv()
    for k in range(1, size):
        total = total + stat_got[k - 1]
    scale = lax.rsqrt(total[0:1] / (width * size) + 1e-06)
    branch = jax.nn.sigmoid(total[1:2] * scale)
    rows = lax.broadcasted_iota(jnp.int32, (8, 128), 0)
    shifted = jnp.concatenate([turned[2 : 2 + 2 * top], jnp.zeros((8 - 2 * top, 128), f32)], axis=0)
    side[...] = jnp.where(rows == 2 * top, branch, shifted)
    column = jnp.broadcast_to(scale, (128, 128)).T[:count, 0:1]
    own_cols[...] = (resid_cols[...].astype(f32) * column * gain).astype(bf16)
    for copy in copies:
        copy.wait_send()
    mix.finish()


MIX_PIECES = 2


def mixer_exit(reads, out_proj, tokens, ffn_gain, branch_gate, route_ids, route_logits, size):
    count, width = tokens.shape
    part = width // size
    fast = fast_extent("tp", size)
    bf16 = jnp.bfloat16
    whole = pl.BlockSpec(memory_space=pltpu.VMEM)
    return pl.pallas_call(
        functools.partial(exit_kernel, size),
        out_shape=(
            jax.ShapeDtypeStruct((count, part), bf16),
            jax.ShapeDtypeStruct((count, part), bf16),
            jax.ShapeDtypeStruct((8, 128), jnp.float32),
        ),
        in_specs=[whole] * 7,
        out_specs=(whole,) * 3,
        scratch_shapes=[
            pltpu.VMEM((count, width), bf16),
            pltpu.VMEM((8, 128), jnp.float32),
            pltpu.VMEM((size - 1, 8, 128), jnp.float32),
            pltpu.SemaphoreType.DMA((size - 1,)),
            pltpu.SemaphoreType.DMA((size - 1,)),
        ]
        + reduce_scratch(fast, size // fast, count, part, MIX_PIECES),
        compiler_params=pltpu.CompilerParams(
            collective_id=0, has_side_effects=True, vmem_limit_bytes=24 << 20
        ),
    )(reads, out_proj, tokens, ffn_gain, branch_gate, route_ids, route_logits)


def shards(
    tokens,
    mix_gain,
    ffn_gain,
    in_proj,
    decay_rate,
    frequency,
    log_step,
    b_real,
    b_imag,
    c_real,
    c_imag,
    skip_gain,
    states,
    out_proj,
    route_ids,
    route_logits,
    expert_gate,
    expert_up,
    expert_down,
    dense_gate,
    dense_up,
    dense_down,
    branch_gate,
):
    seq_count, width = tokens.shape
    tp_count = lax.axis_size("tp")
    ep_count = lax.axis_size("ep")
    part_width = width // tp_count
    params = (
        decay_rate,
        frequency,
        log_step.reshape(1, -1),
        b_real,
        b_imag,
        c_real,
        c_imag,
    )
    reads, new_states = mixer(
        tokens, mix_gain.reshape(1, -1), in_proj, params, skip_gain.reshape(1, -1), states
    )
    own_cols, resid_cols, side = mixer_exit(
        reads,
        out_proj,
        tokens,
        ffn_gain.reshape(1, -1),
        branch_gate.astype(jnp.float32).reshape(1, -1),
        route_ids,
        route_logits,
        tp_count,
    )
    top_count = route_ids.shape[1]
    every_cols, every_side = all_gather([own_cols, side], "ep", ep_count, [2, 1], False, 2)
    total_count = ep_count * seq_count
    every_cols = every_cols.reshape(total_count, part_width)
    every_side = every_side[:, :, :seq_count].transpose(1, 0, 2).reshape(-1, total_count)
    every_ids = every_side[:top_count].T
    every_weights = every_side[top_count : 2 * top_count].T
    every_branch = every_side[2 * top_count]
    mine = every_ids == lax.axis_index("ep").astype(jnp.float32)
    taken = jnp.any(mine, axis=1)
    own_weight = jnp.sum(jnp.where(mine, every_weights, 0.0), axis=1)
    order = jnp.cumsum(taken.astype(jnp.int32)) - 1
    room = ep_count * max(2, 2 * seq_count * top_count // ep_count)
    slots = jnp.arange(room, dtype=jnp.int32)
    select = (order[None, :] == slots[:, None]) & taken[None, :]
    row_weight = jnp.sum(jnp.where(select, own_weight[None, :], 0.0), axis=1)
    select = select.astype(jnp.bfloat16)
    expert_in = jnp.dot(select, every_cols, preferred_element_type=jnp.float32).astype(jnp.bfloat16)
    dense_hidden, expert_cols = branches(
        expert_in,
        every_cols,
        dense_gate,
        dense_up,
        expert_gate[0],
        expert_up[0],
        expert_down[0],
        "tp",
        tp_count,
        3,
    )
    dense_hidden = dense_hidden.reshape(total_count, dense_gate.shape[1])
    weighted = (expert_cols.astype(jnp.float32) * row_weight[:, None]).astype(jnp.bfloat16)
    routed_part = lax.dot_general(
        select, weighted, (((0,), (0,)), ((), ())), preferred_element_type=jnp.float32
    )
    dense_part = jnp.dot(dense_hidden, dense_down, preferred_element_type=jnp.float32)
    share = (routed_part + every_branch[:, None] * dense_part).astype(jnp.bfloat16)
    share = share.reshape(ep_count, seq_count, part_width)
    gathered = reduce_scatter(share, "ep", ep_count, 2, False, 4)
    output = (resid_cols.astype(jnp.float32) + gathered.astype(jnp.float32)).astype(jnp.bfloat16)
    return (output, new_states)


def solution(mesh):
    return jax.shard_map(
        shards,
        mesh=mesh,
        in_specs=(
            P("ep", None),
            P(),
            P(),
            P(None, "tp"),
            P("tp", None),
            P("tp", None),
            P("tp"),
            P("tp", None, None),
            P("tp", None, None),
            P("tp", None, None),
            P("tp", None, None),
            P("tp"),
            P(None, "ep", "tp"),
            P("tp", None),
            P("ep", None),
            P("ep", None),
            P("ep", None, "tp"),
            P("ep", None, "tp"),
            P("ep", "tp", None),
            P("tp", "ep"),
            P("tp", "ep"),
            P("ep", "tp"),
            P(),
        ),
        out_specs=(P("ep", "tp"), P(None, "ep", "tp")),
        check_vma=False,
    )
```

```python
import functools
import jax
import jax.numpy as jnp
from jax import lax
from jax.experimental import pallas as pl
from jax.experimental.pallas import tpu as pltpu
from jax.sharding import PartitionSpec as P

GROUP = 16
STATE = 64
MESH = pl.DeviceIdType.MESH


def fast_extent(axis, size):
    if axis == "tp":
        return 2
    extent = 1
    while (2 * extent) * (2 * extent) * 2 <= size:
        extent *= 2
    return extent


class Grid:
    def __init__(self, axis, size):
        self.axis, self.size = axis, size
        self.fast = fast_extent(axis, size)
        self.slow = size // self.fast
        self.me = lax.axis_index(axis)
        self.at_fast = self.me % self.fast
        self.at_slow = self.me // self.fast

    def index(self, slow_step, fast_step):
        slow_at = (self.at_slow + slow_step + self.slow) % self.slow
        fast_at = (self.at_fast + fast_step + self.fast) % self.fast
        return slow_at * self.fast + fast_at

    def peers(self):
        return [self.index(k, 0) for k in range(1, self.slow)] + [
            self.index(0, q) for q in range(1, self.fast)
        ]

    def greet(self):
        barrier = pltpu.get_barrier_semaphore()
        peers = self.peers()
        for peer in peers:
            pl.semaphore_signal(barrier, inc=1, device_id={self.axis: peer}, device_id_type=MESH)
        pl.semaphore_wait(barrier, len(peers))

    def greet_all(self):
        barrier = pltpu.get_barrier_semaphore()
        for k in range(1, self.size):
            pl.semaphore_signal(
                barrier,
                inc=1,
                device_id={self.axis: (self.me + k) % self.size},
                device_id_type=MESH,
            )
        pl.semaphore_wait(barrier, self.size - 1)

    def copy(self, source, target, sent, landed, peer):
        return pltpu.make_async_remote_copy(
            src_ref=source,
            dst_ref=target,
            send_sem=sent,
            recv_sem=landed,
            device_id={self.axis: peer},
            device_id_type=MESH,
        )


def part_of(ref, owner, start, rows, width, cols):
    if cols:
        return ref.at[pl.ds(start, rows), pl.ds(pl.multiple_of(owner * width, 128), width)]
    return ref.at[owner, pl.ds(start, rows), :]


class Gather:
    def __init__(self, grid, source, target, number, cols, sems, shape=None):
        self.grid, self.source, self.target, self.cols = grid, source, target, cols
        self.slow_sent, self.slow_landed, self.fast_sent, self.fast_landed, self.own_sem = sems
        self.rows, self.width = shape or source.shape
        self.step = self.rows // number
        self.number = number
        self.pending = []

    def piece(self, j):
        if self.source is None:
            return self.place(self.grid.me, j)
        return self.source.at[pl.ds(j * self.step, self.step), :]

    def place(self, owner, j):
        return part_of(self.target, owner, j * self.step, self.step, self.width, self.cols)

    def slow_copy(self, source, target, j, k, peer):
        return self.grid.copy(
            source, target, self.slow_sent.at[j, k - 1], self.slow_landed.at[j, k - 1], peer
        )

    def fast_copy(self, source, target, j, k, q, peer):
        return self.grid.copy(
            source, target, self.fast_sent.at[j, k, q - 1], self.fast_landed.at[j, k, q - 1], peer
        )

    def launch(self, copy):
        copy.start()
        self.pending.append(copy)

    def start_piece(self, j):
        grid = self.grid
        piece, spot = self.piece(j), self.place(grid.me, j)
        for k in range(1, grid.slow):
            self.launch(self.slow_copy(piece, spot, j, k, grid.index(k, 0)))
        for q in range(1, grid.fast):
            self.launch(self.fast_copy(piece, spot, j, 0, q, grid.index(0, q)))

    def start(self):
        for j in range(self.number):
            self.start_piece(j)
        if self.source is not None:
            self.own = pltpu.make_async_copy(
                self.source,
                part_of(self.target, self.grid.me, 0, self.rows, self.width, self.cols),
                self.own_sem,
            )
            self.own.start()

    def relay(self):
        grid = self.grid
        for j in range(self.number):
            for k in range(1, grid.slow):
                spot = self.place(grid.index(-k, 0), j)
                self.slow_copy(spot, spot, j, k, grid.index(-k, 0)).wait_recv()
                for q in range(1, grid.fast):
                    self.launch(self.fast_copy(spot, spot, j, k, q, grid.index(0, q)))

    def arrive(self):
        grid = self.grid
        for j in range(self.number):
            for k in range(grid.slow):
                for q in range(1, grid.fast):
                    spot = self.place(grid.index(-k, -q), j)
                    self.fast_copy(spot, spot, j, k, q, grid.index(0, -q)).wait_recv()
        if self.source is not None:
            self.own.wait()

    def finish(self):
        for copy in self.pending:
            copy.wait_send()


def gather_sems(grid_fast, grid_slow, number):
    return [
        pltpu.SemaphoreType.DMA((number, grid_slow - 1)),
        pltpu.SemaphoreType.DMA((number, grid_slow - 1)),
        pltpu.SemaphoreType.DMA((number, grid_slow, grid_fast - 1)),
        pltpu.SemaphoreType.DMA((number, grid_slow, grid_fast - 1)),
        pltpu.SemaphoreType.DMA,
    ]


class Reduce:
    def __init__(self, grid, source, number, cols, scratch):
        self.grid, self.source, self.cols, self.number = grid, source, cols, number
        self.got_fast, self.mid, self.got_slow, self.total = scratch[:4]
        self.fast_sent, self.fast_landed, self.slow_sent, self.slow_landed = scratch[4:]
        rows, self.width = self.total.shape
        self.step = rows // number
        self.pending = []

    def part(self, dest, j):
        return part_of(self.source, dest, j * self.step, self.step, self.width, self.cols)

    def span(self, j):
        return pl.ds(j * self.step, self.step)

    def fast_copy(self, source, k, j, q, peer):
        return self.grid.copy(
            source,
            self.got_fast.at[q - 1, k - 1, self.span(j), :],
            self.fast_sent.at[q - 1, k - 1, j],
            self.fast_landed.at[q - 1, k - 1, j],
            peer,
        )

    def slow_copy(self, k, j, peer):
        return self.grid.copy(
            self.mid.at[k - 1, self.span(j), :],
            self.got_slow.at[k - 1, self.span(j), :],
            self.slow_sent.at[k - 1, j],
            self.slow_landed.at[k - 1, j],
            peer,
        )

    def push_part(self, k, q):
        grid = self.grid
        for j in range(self.number):
            copy = self.fast_copy(self.part(grid.index(k, q), j), k, j, q, grid.index(0, q))
            copy.start()
            self.pending.append(copy)

    def push(self):
        for k in range(1, self.grid.slow + 1):
            for q in range(1, self.grid.fast):
                self.push_part(k, q)

    def relay(self):
        grid = self.grid
        for k in range(1, grid.slow + 1):
            for j in range(self.number):
                value = self.part(grid.index(k, 0), j)[...].astype(jnp.float32)
                for q in range(1, grid.fast):
                    block = self.got_fast.at[q - 1, k - 1, self.span(j), :]
                    self.fast_copy(block, k, j, q, grid.index(0, -q)).wait_recv()
                    value = value + block[...].astype(jnp.float32)
                if k == grid.slow:
                    self.total[self.span(j), :] = value
                else:
                    self.mid[k - 1, self.span(j), :] = value.astype(self.mid.dtype)
                    copy = self.slow_copy(k, j, grid.index(k, 0))
                    copy.start()
                    self.pending.append(copy)

    def collect_piece(self, j):
        value = self.total[self.span(j), :]
        for k in range(1, self.grid.slow):
            self.slow_copy(k, j, self.grid.index(-k, 0)).wait_recv()
            value = value + self.got_slow[k - 1, self.span(j), :].astype(jnp.float32)
        return value

    def collect(self, emit):
        for j in range(self.number):
            emit(self.span(j), self.collect_piece(j))

    def finish(self):
        for copy in self.pending:
            copy.wait_send()


def reduce_scratch(fast, slow, rows, width, number):
    return [
        pltpu.VMEM((fast - 1, slow, rows, width), jnp.bfloat16),
        pltpu.VMEM((slow - 1, rows, width), jnp.bfloat16),
        pltpu.VMEM((slow - 1, rows, width), jnp.bfloat16),
        pltpu.VMEM((rows, width), jnp.float32),
        pltpu.SemaphoreType.DMA((fast - 1, slow, number)),
        pltpu.SemaphoreType.DMA((fast - 1, slow, number)),
        pltpu.SemaphoreType.DMA((slow - 1, number)),
        pltpu.SemaphoreType.DMA((slow - 1, number)),
    ]


def tile_of(extent):
    for tile in (256, 128):
        if extent % tile == 0:
            return tile
    return extent


def mixer_kernel(
    *refs,
):
    far, reads, fresh_hbm = refs[:12], refs[12], refs[13]
    near, fresh, normed, sems = refs[14:26], refs[26], refs[27], refs[28]
    loads = []
    for item, (source, target) in enumerate(zip(far, near)):
        load = pltpu.make_async_copy(source, target, sems.at[item])
        load.start()
        loads.append(load)
    tokens, mix_gain, in_proj, decay_rate, frequency, log_step = near[:6]
    b_real, b_imag, c_real, c_imag, skip_gain, old = near[6:]
    count, width = tokens.shape
    groups, entries = decay_rate.shape
    channels = skip_gain.shape[1]
    wide = groups * entries
    f32, bf16 = jnp.float32, jnp.bfloat16

    def iota(shape, dim):
        return lax.broadcasted_iota(jnp.int32, shape, dim)

    for item in range(3, 6):
        loads[item].wait()
    eye = iota((groups, groups), 0) == iota((groups, groups), 1)
    step_size = jnp.exp(jnp.sum(jnp.where(eye, log_step[...], 0.0), axis=1, keepdims=True))
    lam_re, lam_im = -decay_rate[...], frequency[...]
    magnitude = jnp.exp(lam_re * step_size)
    abar_re = magnitude * jnp.cos(lam_im * step_size)
    abar_im = magnitude * jnp.sin(lam_im * step_size)
    denom = lam_re * lam_re + lam_im * lam_im
    fac_re = ((abar_re - 1.0) * lam_re + abar_im * lam_im) / denom
    fac_im = (abar_im * lam_re - (abar_re - 1.0) * lam_im) / denom
    packed = jnp.concatenate([abar_re, abar_im, fac_re, fac_im], axis=0)
    repeat = (iota((entries, wide), 1) % entries == iota((entries, wide), 0)).astype(f32)
    spread = jnp.dot(packed, repeat, precision=lax.Precision.HIGHEST, preferred_element_type=f32)
    owner = iota((groups, wide), 1) // entries == iota((groups, wide), 0)

    def row_of(item):
        part = spread[item * groups : (item + 1) * groups]
        return jnp.sum(jnp.where(owner, part, 0.0), axis=0, keepdims=True)

    abar_re, abar_im, fac_re, fac_im = (row_of(item) for item in range(4))
    repeat = repeat.astype(bf16)
    inside = iota((channels, wide), 0) // GROUP == iota((channels, wide), 1) // entries

    def matrix(ref):
        flat = ref[...].reshape(channels, entries).astype(bf16)
        full = jnp.dot(flat, repeat, preferred_element_type=f32)
        return jnp.where(inside, full, 0.0).astype(bf16)

    def by_rows(left, right):
        return lax.dot_general(
            left, right, (((1,), (1,)), ((), ())), preferred_element_type=f32
        )

    loads[0].wait()
    loads[1].wait()
    step = 16
    for start in range(0, count, step):
        flt = tokens[start : start + step, :].astype(f32)
        scale = lax.rsqrt(jnp.mean(flt * flt, axis=-1, keepdims=True) + 1e-06)
        normed[start : start + step, :] = (flt * scale * mix_gain[...]).astype(bf16)
    loads[2].wait()
    drive = jnp.dot(normed[...], in_proj[...], preferred_element_type=f32).astype(bf16)
    for load in loads[6:]:
        load.wait()
    push_a = jnp.dot(drive, matrix(b_real), preferred_element_type=f32)
    push_b = jnp.dot(drive, matrix(b_imag), preferred_element_type=f32)
    old_re, old_im = old[0], old[1]
    new_re = abar_re * old_re - abar_im * old_im + fac_re * push_a - fac_im * push_b
    fresh[0] = new_re
    new_im = abar_re * old_im + abar_im * old_re + fac_re * push_b + fac_im * push_a
    fresh[1] = new_im
    store = pltpu.make_async_copy(fresh, fresh_hbm, sems.at[12])
    store.start()
    readout = (
        by_rows(new_re.astype(bf16), matrix(c_real))
        - by_rows(new_im.astype(bf16), matrix(c_imag))
        + skip_gain[...] * drive.astype(f32)
    )
    reads[...] = jax.nn.gelu(readout).astype(bf16)
    store.wait()


def mixer(*arrays):
    tokens, in_proj, states = arrays[0], arrays[2], arrays[-1]
    far = pl.BlockSpec(memory_space=pl.ANY)
    return pl.pallas_call(
        mixer_kernel,
        out_shape=(
            jax.ShapeDtypeStruct((tokens.shape[0], in_proj.shape[1]), jnp.bfloat16),
            jax.ShapeDtypeStruct(states.shape, jnp.float32),
        ),
        in_specs=[far] * len(arrays),
        out_specs=(pl.BlockSpec(memory_space=pltpu.VMEM), far),
        scratch_shapes=[pltpu.VMEM(array.shape, array.dtype) for array in arrays]
        + [
            pltpu.VMEM(states.shape, jnp.float32),
            pltpu.VMEM(tokens.shape, jnp.bfloat16),
            pltpu.SemaphoreType.DMA((13,)),
        ],
        compiler_params=pltpu.CompilerParams(vmem_limit_bytes=62 << 20),
    )(*arrays)


def exit_kernel(
    size,
    reads,
    out_proj_hbm,
    tokens_hbm,
    ffn_gain,
    branch_gate,
    route_ids,
    route_logits,
    own_cols,
    resid_cols,
    side,
    out_proj,
    tokens,
    load_sems,
    partial,
    stat,
    stat_got,
    stat_sent,
    stat_landed,
    *scratch,
):
    f32, bf16 = jnp.float32, jnp.bfloat16
    grid = Grid("tp", size)
    mix = Reduce(grid, partial, MIX_PIECES, True, scratch)
    count, width = resid_cols.shape
    mine = pl.ds(pl.multiple_of(grid.me * width, 128), width)
    loads = [
        pltpu.make_async_copy(out_proj_hbm, out_proj, load_sems.at[0]),
        pltpu.make_async_copy(tokens_hbm.at[:, mine], tokens, load_sems.at[1]),
    ]
    for load in loads:
        load.start()
    grid.greet_all()
    for load in loads:
        load.wait()

    def block(dest):
        span = pl.ds(pl.multiple_of(dest * width, 128), width)
        partial[:, span] = jnp.dot(
            reads[...], out_proj[:, span], preferred_element_type=f32
        ).astype(bf16)

    for k in range(1, grid.slow + 1):
        for q in range(1, grid.fast):
            block(grid.index(k, q))
            mix.push_part(k, q)
    for k in range(1, grid.slow + 1):
        block(grid.index(k, 0))
    logits = route_logits[...]
    top = logits.shape[0]
    raised = jnp.exp(logits - jnp.max(logits, axis=0, keepdims=True))
    weights = raised / jnp.sum(raised, axis=0, keepdims=True)
    side[...] = jnp.zeros((8, 128), f32)
    side[0:top, 0:count] = route_ids[...].astype(f32)
    side[top : 2 * top, 0:count] = weights
    mix.relay()
    gain = ffn_gain[:, mine]
    gate = gain * branch_gate[:, mine]
    lanes = lax.broadcasted_iota(jnp.int32, (count, 128), 1)
    ssq_parts, dot_parts = [], []

    def emit(span, value):
        mixed = value.astype(bf16).astype(f32)
        resid = (tokens[span, :].astype(f32) + mixed).astype(bf16)
        resid_cols[span, :] = resid
        flt = resid.astype(f32)
        ssq_parts.append(jnp.sum(flt * flt, axis=1, keepdims=True))
        dot_parts.append(jnp.sum(flt * gate, axis=1, keepdims=True))

    mix.collect(emit)
    ssq, dots = jnp.concatenate(ssq_parts, axis=0), jnp.concatenate(dot_parts, axis=0)
    table = jnp.where(lanes == 0, ssq, jnp.where(lanes == 1, dots, 0.0))
    if count < 128:
        table = jnp.concatenate([table, jnp.zeros((128 - count, 128), f32)], axis=0)
    turned = table.T
    stat[...] = turned[:8]
    copies = []
    for k in range(1, size):
        copy = grid.copy(
            stat,
            stat_got.at[k - 1],
            stat_sent.at[k - 1],
            stat_landed.at[k - 1],
            (grid.me + k) % size,
        )
        copy.start()
        copies.append(copy)
    total = turned[:8]
    for copy in copies:
        copy.wait_recv()
    for k in range(1, size):
        total = total + stat_got[k - 1]
    scale = lax.rsqrt(total[0:1] / (width * size) + 1e-06)
    branch = jax.nn.sigmoid(total[1:2] * scale)
    side[2 * top : 2 * top + 1, :] = branch
    column = jnp.broadcast_to(scale, (128, 128)).T[:count, 0:1]
    own_cols[...] = (resid_cols[...].astype(f32) * column * gain).astype(bf16)
    for copy in copies:
        copy.wait_send()
    mix.finish()


MIX_PIECES = 2


def mixer_exit(reads, out_proj, tokens, ffn_gain, branch_gate, route_ids, route_logits, size):
    count, width = tokens.shape
    part = width // size
    fast = fast_extent("tp", size)
    bf16 = jnp.bfloat16
    whole = pl.BlockSpec(memory_space=pltpu.VMEM)
    far = pl.BlockSpec(memory_space=pl.ANY)
    return pl.pallas_call(
        functools.partial(exit_kernel, size),
        out_shape=(
            jax.ShapeDtypeStruct((count, part), bf16),
            jax.ShapeDtypeStruct((count, part), bf16),
            jax.ShapeDtypeStruct((8, 128), jnp.float32),
        ),
        in_specs=[whole, far, far] + [whole] * 4,
        out_specs=(whole,) * 3,
        scratch_shapes=[
            pltpu.VMEM(out_proj.shape, bf16),
            pltpu.VMEM((count, part), bf16),
            pltpu.SemaphoreType.DMA((2,)),
            pltpu.VMEM((count, width), bf16),
            pltpu.VMEM((8, 128), jnp.float32),
            pltpu.VMEM((size - 1, 8, 128), jnp.float32),
            pltpu.SemaphoreType.DMA((size - 1,)),
            pltpu.SemaphoreType.DMA((size - 1,)),
        ]
        + reduce_scratch(fast, size // fast, count, part, MIX_PIECES),
        compiler_params=pltpu.CompilerParams(
            collective_id=0, has_side_effects=True, vmem_limit_bytes=58 << 20
        ),
    )(reads, out_proj, tokens, ffn_gain, branch_gate, route_ids, route_logits)


class Chain:
    def __init__(self, size):
        self.size = size
        self.x_size = fast_extent("ep", size)
        self.z_size = size // self.x_size
        self.me = lax.axis_index("ep")
        self.x = self.me % self.x_size
        self.z = self.me // self.x_size
        self.pending = []

    def at(self, j):
        left, right = self.z, self.z_size - 1 - self.z
        both = jnp.minimum(left, right)
        if j == 0:
            return self.z
        near = (j + 1) // 2
        paired = self.z - near if j % 2 else self.z + near
        single = jnp.where(left > right, self.z - (j - both), self.z + (j - both))
        return jnp.where(j <= 2 * both, paired, single)

    def index(self, z, x_step):
        return z * self.x_size + (self.x + x_step + self.x_size) % self.x_size

    def copy(self, source, target, sent, landed, peer):
        return pltpu.make_async_remote_copy(
            src_ref=source,
            dst_ref=target,
            send_sem=sent,
            recv_sem=landed,
            device_id={"ep": peer},
            device_id_type=MESH,
        )

    def launch(self, copy, cond=None):
        if cond is None:
            copy.start()
        else:
            pl.when(cond)(copy.start)
        self.pending.append((copy, cond))

    def finish(self):
        for copy, cond in self.pending:
            if cond is None:
                copy.wait_send()
            else:
                pl.when(cond)(copy.wait_send)


def layer_kernel(ep_size, tp_size, top, cap, names, *refs):
    own_cols, resid_cols, side = refs[:3]
    weights_hbm, out, refs = refs[3:9], refs[9], refs[10:]
    r = dict(zip(names, refs))
    extra = list(refs[len(names) :])
    f32, bf16 = jnp.float32, jnp.bfloat16
    chain, grid = Chain(ep_size), Grid("tp", tp_size)
    z_size, x_size, z, x = chain.z_size, chain.x_size, chain.z, chain.x
    rounds = ep_size // tp_size
    pieces = min(tp_size, 4)
    count, width = own_cols.shape

    def take(number):
        taken = extra[:number]
        del extra[:number]
        return taken

    dense_sums, hidden_gathers, row_gathers, expert_sums = [], [], [], []
    both, every_hidden, own_hidden, full, part = [], [], [], [], []
    for g in range(rounds):
        stores = take(5)
        for target, store in zip((both, every_hidden, own_hidden, full, part), stores):
            target.append(store)
        dense_sums.append(Reduce(grid, both[g], 1, False, take(8)))
        hidden_gathers.append(Gather(grid, own_hidden[g], every_hidden[g], 1, False, take(5)))
        row_gathers.append(
            Gather(grid, None, full[g], pieces, True, take(5), (tp_size * cap, width))
        )
        expert_sums.append(Reduce(grid, part[g], pieces, True, take(8)))

    near = [r[name] for name in WEIGHTS]
    loads = []
    for item, (source, target) in enumerate(zip(weights_hbm, near)):
        load = pltpu.make_async_copy(source, target, r["load_sems"].at[item])
        load.start()
        loads.append(load)
    dense_gate, dense_up, gate, up, down, dense_down = near
    barrier = pltpu.get_barrier_semaphore()
    for k in range(1, ep_size):
        pl.semaphore_signal(
            barrier, inc=1, device_id={"ep": (chain.me + k) % ep_size}, device_id_type=MESH
        )
    for k in range(1, tp_size):
        pl.semaphore_signal(
            barrier, inc=1, device_id={"tp": (grid.me + k) % tp_size}, device_id_type=MESH
        )
    pl.semaphore_wait(barrier, ep_size + tp_size - 2)

    cols, sides = r["cols"], r["sides"]

    def chunk(j, q=0):
        return chain.index(chain.at(j), -q)

    def send_chunk(j):
        spot = cols.at[chunk(j)]
        source = own_cols if j == 0 else spot
        at = chain.at(j)
        for turn, step, cond in (
            (0, 1, (at <= z) & (z < z_size - 1)),
            (1, -1, (at >= z) & (z > 0)),
        ):
            copy = chain.copy(
                source,
                spot,
                r["z_sent"].at[turn, j],
                r["z_landed"].at[at],
                jnp.where(cond, z + step, z) * x_size + x,
            )
            chain.launch(copy, cond)
        for q in range(1, x_size):
            copy = chain.copy(
                source,
                spot,
                r["x_sent"].at[q - 1, j],
                r["x_landed"].at[q - 1, j],
                chain.index(z, q),
            )
            chain.launch(copy)

    def wait_chunk(j, q):
        spot = cols.at[chunk(j, q)]
        if q:
            landed = r["x_landed"].at[q - 1, j]
        else:
            landed = r["z_landed"].at[chain.at(j)]
        chain.copy(spot, spot, r["x_sent"].at[0, 0], landed, chain.index(z, 1)).wait_recv()

    send_chunk(0)
    for k in range(1, ep_size):
        copy = chain.copy(
            side,
            sides.at[chain.me],
            r["side_sent"].at[k - 1],
            r["side_landed"].at[k - 1],
            (chain.me + k) % ep_size,
        )
        chain.launch(copy)

    mine = pl.ds(pl.multiple_of(grid.me * width, 128), width)
    hidden_width = dense_gate.shape[1]
    expert = chain.me.astype(f32)
    lane_ok = (lax.broadcasted_iota(jnp.int32, (1, 128), 1) < count).astype(f32)
    slots = lax.broadcasted_iota(jnp.int32, (128, 128), 0).astype(f32)
    before = (
        lax.broadcasted_iota(jnp.int32, (128, 128), 0)
        < lax.broadcasted_iota(jnp.int32, (128, 128), 1)
    ).astype(bf16)

    def process(j, q):
        i = j * x_size + q
        g, at = i // tp_size, i % tp_size
        if i == 0:
            block, info = own_cols[...], side[...]
        else:
            source = chunk(j, q)
            away = (chain.me - source + ep_size) % ep_size
            spot = sides.at[source]
            chain.copy(
                spot, spot, r["side_sent"].at[0], r["side_landed"].at[away - 1], source
            ).wait_recv()
            block, info = cols[source], sides[source]
        taken, weight = jnp.zeros((1, 128), f32), jnp.zeros((1, 128), f32)
        for item in range(top):
            hit = jnp.where(info[item : item + 1] == expert, lane_ok, 0.0)
            taken = taken + hit
            weight = weight + hit * info[top + item : top + item + 1]
        rank = jnp.dot(
            jnp.broadcast_to(taken, (8, 128)).astype(bf16), before, preferred_element_type=f32
        )[0:1]
        table = jnp.where(slots == rank, taken, 0.0)
        rows = jnp.dot(
            table[:cap, :count].astype(bf16), block, preferred_element_type=f32
        ).astype(bf16)
        full[g][at * cap : (at + 1) * cap, mine] = rows
        share = tp_size // pieces
        if at % share == share - 1:
            row_gathers[g].start_piece(at // share)
        r["turned"][i] = jnp.where(
            slots == 127.0, info[2 * top : 2 * top + 1], table * weight
        ).T
        if i == 0:
            loads[0].wait()
            loads[1].wait()
        both[g][at, :, :hidden_width] = jnp.dot(
            block, dense_gate[...], preferred_element_type=f32
        ).astype(bf16)
        both[g][at, :, hidden_width:] = jnp.dot(
            block, dense_up[...], preferred_element_type=f32
        ).astype(bf16)
        if at == tp_size - 1:
            dense_sums[g].push()
        if at == 0 and g > 0:
            dense_sums[g - 1].relay()

    inner = gate.shape[1]
    tile = tile_of(inner)
    hidden = r["hidden"]

    def expert_hidden(g):
        row_gathers[g].relay()
        row_gathers[g].arrive()
        rows = full[g]

        @pl.loop(0, inner // tile)
        def _(step):
            span = pl.ds(pl.multiple_of(step * tile, 128), tile)
            gate_val = jnp.dot(rows[...], gate[:, span], preferred_element_type=f32)
            up_val = jnp.dot(rows[...], up[:, span], preferred_element_type=f32)
            hidden[g, :, span] = (jax.nn.silu(gate_val) * up_val).astype(bf16)

    wide = tile_of(width)

    def expert_part(g):
        target = part[g]

        @pl.loop(0, tp_size * width // wide)
        def _(step):
            span = pl.ds(pl.multiple_of(step * wide, 128), wide)
            target[:, span] = jnp.dot(
                hidden[g], down[:, span], preferred_element_type=f32
            ).astype(bf16)

    def dense_hidden(g):
        def emit(span, value):
            own_hidden[g][span, :] = (
                jax.nn.silu(value[:, :hidden_width]) * value[:, hidden_width:]
            ).astype(bf16)

        dense_sums[g].collect(emit)
        hidden_gathers[g].start()

    for j in range(z_size):
        if j:
            wait_chunk(j, 0)
            send_chunk(j)
            for q in range(1, x_size):
                wait_chunk(j - 1, q)
                process(j - 1, q)
        process(j, 0)
    loads[2].wait()
    loads[3].wait()
    last = rounds - 1
    for g in range(last):
        expert_hidden(g)
    for q in range(1, x_size):
        wait_chunk(z_size - 1, q)
        process(z_size - 1, q)
    dense_sums[last].relay()
    for g in range(last):
        dense_hidden(g)
    loads[4].wait()
    for g in range(last):
        expert_part(g)
    expert_hidden(last)
    dense_hidden(last)
    expert_part(last)
    for g in reversed(range(rounds)):
        expert_sums[g].push()
        expert_sums[g].relay()
    for g in range(rounds):
        hidden_gathers[g].relay()
    for g in range(rounds):
        hidden_gathers[g].arrive()
    loads[5].wait()

    collected, own_share = set(), r["own_share"]

    def share_of(j, q):
        i = j * x_size + q
        g, at = i // tp_size, i % tp_size
        chunks = tp_size // pieces
        piece = at // chunks
        if (g, piece) not in collected:
            collected.add((g, piece))
            rows = chunks * cap
            r["expert_out"][g, piece * rows : (piece + 1) * rows, :] = (
                expert_sums[g].collect_piece(piece).astype(bf16)
            )
        turned = r["turned"][i]
        routed = jnp.dot(
            turned[:count, :cap].astype(bf16),
            r["expert_out"][g, at * cap : (at + 1) * cap, :],
            preferred_element_type=f32,
        )
        dense = jnp.dot(every_hidden[g][at], dense_down[...], preferred_element_type=f32)
        return routed + turned[:count, 127:128] * dense

    def send_share(j):
        for q in range(1, x_size):
            i = j * x_size + q
            r["x_share"][i] = share_of(j, q).astype(bf16)
            copy = chain.copy(
                r["x_share"].at[i],
                r["x_got"].at[j, q - 1],
                r["xs_sent"].at[i],
                r["xs_landed"].at[j, q - 1],
                chain.index(z, -q),
            )
            chain.launch(copy)
        own_share[j] = share_of(j, 0)

    def finish_share(j):
        for q in range(1, x_size):
            spot = r["x_got"].at[j, q - 1]
            chain.copy(
                spot, spot, r["xs_sent"].at[0], r["xs_landed"].at[j, q - 1], chain.index(z, q)
            ).wait_recv()
            own_share[j] = own_share[j] + r["x_got"][j, q - 1].astype(f32)
        at = chain.at(j)
        for turn, cond in (
            (0, (at <= z) & (z < z_size - 1)),
            (1, (at >= z) & (z > 0)),
        ):

            @pl.when(cond)
            def _():
                spot = r["z_got"].at[turn, at]
                chain.copy(
                    spot,
                    spot,
                    r["zs_sent"].at[0],
                    r["zs_landed"].at[turn, at],
                    chain.index(z, 1),
                ).wait_recv()
                own_share[j] = own_share[j] + r["z_got"][turn, at].astype(f32)

        if j == 0:
            total = own_share[0].astype(bf16).astype(f32)
            out[...] = (resid_cols[...].astype(f32) + total).astype(bf16)
        else:
            r["z_share"][j] = own_share[j].astype(bf16)
            turn = jnp.where(at < z, 0, 1)
            copy = chain.copy(
                r["z_share"].at[j],
                r["z_got"].at[turn, at],
                r["zs_sent"].at[j],
                r["zs_landed"].at[turn, at],
                jnp.where(at < z, z - 1, z + 1) * x_size + x,
            )
            chain.launch(copy)

    for j in reversed(range(z_size)):
        send_share(j)
        if j + 1 < z_size:
            finish_share(j + 1)
    finish_share(0)
    chain.finish()
    for phase in dense_sums + hidden_gathers + row_gathers + expert_sums:
        phase.finish()


WEIGHTS = ("dense_gate", "dense_up", "gate", "up", "down", "dense_down")


def layer(own_cols, resid_cols, side, weights, top, ep_size, tp_size):
    count, width = own_cols.shape
    bf16, f32 = jnp.bfloat16, jnp.float32
    vmem, dma = pltpu.VMEM, pltpu.SemaphoreType.DMA
    x_size = fast_extent("ep", ep_size)
    z_size = ep_size // x_size
    cap = max(2, 2 * count * top // ep_size)
    cap = -(-cap // 16) * 16
    hidden_width, inner = weights[0].shape[1], weights[2].shape[1]
    rounds, rows = ep_size // tp_size, tp_size * cap
    pieces = min(tp_size, 4)
    fast = fast_extent("tp", tp_size)
    slow = tp_size // fast
    named = {name: vmem(array.shape, bf16) for name, array in zip(WEIGHTS, weights)}
    named.update(
        load_sems=dma((len(weights),)),
        cols=vmem((ep_size, count, width), bf16),
        sides=vmem((ep_size, 8, 128), f32),
        turned=vmem((ep_size, 128, 128), f32),
        hidden=vmem((rounds, rows, inner), bf16),
        expert_out=vmem((rounds, rows, width), bf16),
        own_share=vmem((z_size, count, width), f32),
        x_share=vmem((ep_size, count, width), bf16),
        x_got=vmem((z_size, x_size - 1, count, width), bf16),
        z_share=vmem((z_size, count, width), bf16),
        z_got=vmem((2, z_size, count, width), bf16),
        z_sent=dma((2, z_size)),
        z_landed=dma((z_size,)),
        x_sent=dma((x_size - 1, z_size)),
        x_landed=dma((x_size - 1, z_size)),
        side_sent=dma((ep_size - 1,)),
        side_landed=dma((ep_size - 1,)),
        xs_sent=dma((ep_size,)),
        xs_landed=dma((z_size, x_size - 1)),
        zs_sent=dma((z_size,)),
        zs_landed=dma((2, z_size)),
    )
    extra = []
    for _ in range(rounds):
        extra += [
            vmem((tp_size, count, 2 * hidden_width), bf16),
            vmem((tp_size, count, hidden_width), bf16),
            vmem((count, hidden_width), bf16),
            vmem((rows, tp_size * width), bf16),
            vmem((rows, tp_size * width), bf16),
        ]
        extra += reduce_scratch(fast, slow, count, 2 * hidden_width, 1)
        extra += gather_sems(fast, slow, 1) + gather_sems(fast, slow, pieces)
        extra += reduce_scratch(fast, slow, rows, width, pieces)
    whole = pl.BlockSpec(memory_space=pltpu.VMEM)
    far = pl.BlockSpec(memory_space=pl.ANY)
    return pl.pallas_call(
        functools.partial(layer_kernel, ep_size, tp_size, top, cap, tuple(named)),
        out_shape=jax.ShapeDtypeStruct((count, width), bf16),
        in_specs=[whole] * 3 + [far] * len(weights),
        out_specs=whole,
        scratch_shapes=list(named.values()) + extra,
        compiler_params=pltpu.CompilerParams(
            collective_id=1, has_side_effects=True, vmem_limit_bytes=62 << 20
        ),
    )(own_cols, resid_cols, side, *weights)


def shards(
    tokens,
    mix_gain,
    ffn_gain,
    in_proj,
    decay_rate,
    frequency,
    log_step,
    b_real,
    b_imag,
    c_real,
    c_imag,
    skip_gain,
    states,
    out_proj,
    route_ids,
    route_logits,
    expert_gate,
    expert_up,
    expert_down,
    dense_gate,
    dense_up,
    dense_down,
    branch_gate,
):
    tp_count = lax.axis_size("tp")
    ep_count = lax.axis_size("ep")
    reads, new_states = mixer(
        tokens,
        mix_gain.reshape(1, -1),
        in_proj,
        decay_rate,
        frequency,
        log_step.reshape(1, -1),
        jnp.swapaxes(b_real, 1, 2),
        jnp.swapaxes(b_imag, 1, 2),
        c_real,
        c_imag,
        skip_gain.reshape(1, -1),
        states,
    )
    own_cols, resid_cols, side = mixer_exit(
        reads,
        out_proj,
        tokens,
        ffn_gain.reshape(1, -1),
        branch_gate.astype(jnp.float32).reshape(1, -1),
        route_ids.T,
        route_logits.T,
        tp_count,
    )
    weights = (dense_gate, dense_up, expert_gate[0], expert_up[0], expert_down[0], dense_down)
    output = layer(own_cols, resid_cols, side, weights, route_ids.shape[1], ep_count, tp_count)
    return (output, new_states)


def solution(mesh):
    return jax.shard_map(
        shards,
        mesh=mesh,
        in_specs=(
            P("ep", None),
            P(),
            P(),
            P(None, "tp"),
            P("tp", None),
            P("tp", None),
            P("tp"),
            P("tp", None, None),
            P("tp", None, None),
            P("tp", None, None),
            P("tp", None, None),
            P("tp"),
            P(None, "ep", "tp"),
            P("tp", None),
            P("ep", None),
            P("ep", None),
            P("ep", None, "tp"),
            P("ep", None, "tp"),
            P("ep", "tp", None),
            P("tp", "ep"),
            P("tp", "ep"),
            P("ep", "tp"),
            P(),
        ),
        out_specs=(P("ep", "tp"), P(None, "ep", "tp")),
        check_vma=False,
    )
```

```python
import functools
import jax
import jax.numpy as jnp
from jax import lax
from jax.experimental import pallas as pl
from jax.experimental.pallas import tpu as pltpu
from jax.sharding import PartitionSpec as P

GROUP = 16
STATE = 64
MESH = pl.DeviceIdType.MESH


def fast_extent(axis, size):
    if axis == "tp":
        return 2
    extent = 1
    while (2 * extent) * (2 * extent) * 2 <= size:
        extent *= 2
    return extent


class Grid:
    def __init__(self, axis, size):
        self.axis, self.size = axis, size
        self.fast = fast_extent(axis, size)
        self.slow = size // self.fast
        self.me = lax.axis_index(axis)
        self.at_fast = self.me % self.fast
        self.at_slow = self.me // self.fast

    def index(self, slow_step, fast_step):
        slow_at = (self.at_slow + slow_step + self.slow) % self.slow
        fast_at = (self.at_fast + fast_step + self.fast) % self.fast
        return slow_at * self.fast + fast_at

    def peers(self):
        return [self.index(k, 0) for k in range(1, self.slow)] + [
            self.index(0, q) for q in range(1, self.fast)
        ]

    def copy(self, source, target, sent, landed, peer):
        return pltpu.make_async_remote_copy(
            src_ref=source,
            dst_ref=target,
            send_sem=sent,
            recv_sem=landed,
            device_id={self.axis: peer},
            device_id_type=MESH,
        )


def part_of(ref, owner, start, rows, width, cols):
    if cols:
        return ref.at[pl.ds(start, rows), pl.ds(pl.multiple_of(owner * width, 128), width)]
    return ref.at[owner, pl.ds(start, rows), :]


class Gather:
    def __init__(self, grid, source, target, number, cols, sems, shape=None):
        self.grid, self.source, self.target, self.cols = grid, source, target, cols
        self.slow_sent, self.slow_landed, self.fast_sent, self.fast_landed, self.own_sem = sems
        self.rows, self.width = shape or source.shape
        self.step = self.rows // number
        self.number = number
        self.pending = []

    def piece(self, j):
        if self.source is None:
            return self.place(self.grid.me, j)
        return self.source.at[pl.ds(j * self.step, self.step), :]

    def place(self, owner, j):
        return part_of(self.target, owner, j * self.step, self.step, self.width, self.cols)

    def slow_copy(self, source, target, j, k, peer):
        return self.grid.copy(
            source, target, self.slow_sent.at[j, k - 1], self.slow_landed.at[j, k - 1], peer
        )

    def fast_copy(self, source, target, j, k, q, peer):
        return self.grid.copy(
            source, target, self.fast_sent.at[j, k, q - 1], self.fast_landed.at[j, k, q - 1], peer
        )

    def launch(self, copy):
        copy.start()
        self.pending.append(copy)

    def start_piece(self, j):
        grid = self.grid
        piece, spot = self.piece(j), self.place(grid.me, j)
        for k in range(1, grid.slow):
            self.launch(self.slow_copy(piece, spot, j, k, grid.index(k, 0)))
        for q in range(1, grid.fast):
            self.launch(self.fast_copy(piece, spot, j, 0, q, grid.index(0, q)))

    def start(self):
        for j in range(self.number):
            self.start_piece(j)
        if self.source is not None:
            self.own = pltpu.make_async_copy(
                self.source,
                part_of(self.target, self.grid.me, 0, self.rows, self.width, self.cols),
                self.own_sem,
            )
            self.own.start()

    def relay(self):
        grid = self.grid
        for j in range(self.number):
            for k in range(1, grid.slow):
                spot = self.place(grid.index(-k, 0), j)
                self.slow_copy(spot, spot, j, k, grid.index(-k, 0)).wait_recv()
                for q in range(1, grid.fast):
                    self.launch(self.fast_copy(spot, spot, j, k, q, grid.index(0, q)))

    def arrive(self):
        grid = self.grid
        for j in range(self.number):
            for k in range(grid.slow):
                for q in range(1, grid.fast):
                    spot = self.place(grid.index(-k, -q), j)
                    self.fast_copy(spot, spot, j, k, q, grid.index(0, -q)).wait_recv()
        if self.source is not None:
            self.own.wait()

    def finish(self):
        for copy in self.pending:
            copy.wait_send()


def gather_sems(grid_fast, grid_slow, number):
    return [
        pltpu.SemaphoreType.DMA((number, grid_slow - 1)),
        pltpu.SemaphoreType.DMA((number, grid_slow - 1)),
        pltpu.SemaphoreType.DMA((number, grid_slow, grid_fast - 1)),
        pltpu.SemaphoreType.DMA((number, grid_slow, grid_fast - 1)),
        pltpu.SemaphoreType.DMA,
    ]


class Reduce:
    def __init__(self, grid, source, number, cols, scratch):
        self.grid, self.source, self.cols, self.number = grid, source, cols, number
        self.got_fast, self.mid, self.got_slow, self.total = scratch[:4]
        self.fast_sent, self.fast_landed, self.slow_sent, self.slow_landed = scratch[4:]
        rows, self.width = self.total.shape
        self.step = rows // number
        self.pending = []

    def part(self, dest, j):
        return part_of(self.source, dest, j * self.step, self.step, self.width, self.cols)

    def span(self, j):
        return pl.ds(j * self.step, self.step)

    def fast_copy(self, source, k, j, q, peer):
        return self.grid.copy(
            source,
            self.got_fast.at[q - 1, k - 1, self.span(j), :],
            self.fast_sent.at[q - 1, k - 1, j],
            self.fast_landed.at[q - 1, k - 1, j],
            peer,
        )

    def slow_copy(self, k, j, peer):
        return self.grid.copy(
            self.mid.at[k - 1, self.span(j), :],
            self.got_slow.at[k - 1, self.span(j), :],
            self.slow_sent.at[k - 1, j],
            self.slow_landed.at[k - 1, j],
            peer,
        )

    def push_part(self, k, q):
        grid = self.grid
        for j in reversed(range(self.number)):
            copy = self.fast_copy(self.part(grid.index(k, q), j), k, j, q, grid.index(0, q))
            copy.start()
            self.pending.append(copy)

    def push(self):
        for k in range(1, self.grid.slow + 1):
            for q in range(1, self.grid.fast):
                self.push_part(k, q)

    def relay(self, pieces=None):
        grid = self.grid
        for k in range(1, grid.slow + 1):
            for j in reversed(range(self.number) if pieces is None else pieces):
                value = self.part(grid.index(k, 0), j)[...].astype(jnp.float32)
                for q in range(1, grid.fast):
                    block = self.got_fast.at[q - 1, k - 1, self.span(j), :]
                    self.fast_copy(block, k, j, q, grid.index(0, -q)).wait_recv()
                    value = value + block[...].astype(jnp.float32)
                if k == grid.slow:
                    self.total[self.span(j), :] = value
                else:
                    self.mid[k - 1, self.span(j), :] = value.astype(self.mid.dtype)
                    copy = self.slow_copy(k, j, grid.index(k, 0))
                    copy.start()
                    self.pending.append(copy)

    def collect_piece(self, j):
        value = self.total[self.span(j), :]
        for k in range(1, self.grid.slow):
            self.slow_copy(k, j, self.grid.index(-k, 0)).wait_recv()
            value = value + self.got_slow[k - 1, self.span(j), :].astype(jnp.float32)
        return value

    def collect(self, emit):
        for j in range(self.number):
            emit(self.span(j), self.collect_piece(j))

    def finish(self):
        for copy in self.pending:
            copy.wait_send()


def reduce_scratch(fast, slow, rows, width, number):
    return [
        pltpu.VMEM((fast - 1, slow, rows, width), jnp.bfloat16),
        pltpu.VMEM((slow - 1, rows, width), jnp.bfloat16),
        pltpu.VMEM((slow - 1, rows, width), jnp.bfloat16),
        pltpu.VMEM((rows, width), jnp.float32),
        pltpu.SemaphoreType.DMA((fast - 1, slow, number)),
        pltpu.SemaphoreType.DMA((fast - 1, slow, number)),
        pltpu.SemaphoreType.DMA((slow - 1, number)),
        pltpu.SemaphoreType.DMA((slow - 1, number)),
    ]


def tile_of(extent):
    for tile in (256, 128):
        if extent % tile == 0:
            return tile
    return extent


def mixer_kernel(
    *refs,
):
    far, partial, fresh_hbm = refs[:13], refs[13], refs[14]
    near, fresh, normed, sems = refs[15:28], refs[28], refs[29], refs[30]
    loads = []
    for item, (source, target) in enumerate(zip(far, near)):
        load = pltpu.make_async_copy(source, target, sems.at[item])
        load.start()
        loads.append(load)
    tokens, mix_gain, in_proj, decay_rate, frequency, log_step = near[:6]
    b_real, b_imag, c_real, c_imag, skip_gain, old, out_proj = near[6:]
    count, width = tokens.shape
    groups, entries = decay_rate.shape
    channels = skip_gain.shape[1]
    wide = groups * entries
    f32, bf16 = jnp.float32, jnp.bfloat16

    def iota(shape, dim):
        return lax.broadcasted_iota(jnp.int32, shape, dim)

    for item in range(3, 6):
        loads[item].wait()
    eye = iota((groups, groups), 0) == iota((groups, groups), 1)
    step_size = jnp.exp(jnp.sum(jnp.where(eye, log_step[...], 0.0), axis=1, keepdims=True))
    lam_re, lam_im = -decay_rate[...], frequency[...]
    magnitude = jnp.exp(lam_re * step_size)
    abar_re = magnitude * jnp.cos(lam_im * step_size)
    abar_im = magnitude * jnp.sin(lam_im * step_size)
    denom = lam_re * lam_re + lam_im * lam_im
    fac_re = ((abar_re - 1.0) * lam_re + abar_im * lam_im) / denom
    fac_im = (abar_im * lam_re - (abar_re - 1.0) * lam_im) / denom
    packed = jnp.concatenate([abar_re, abar_im, fac_re, fac_im], axis=0)
    repeat = (iota((entries, wide), 1) % entries == iota((entries, wide), 0)).astype(f32)
    spread = jnp.dot(packed, repeat, precision=lax.Precision.HIGHEST, preferred_element_type=f32)
    owner = iota((groups, wide), 1) // entries == iota((groups, wide), 0)

    def row_of(item):
        part = spread[item * groups : (item + 1) * groups]
        return jnp.sum(jnp.where(owner, part, 0.0), axis=0, keepdims=True)

    abar_re, abar_im, fac_re, fac_im = (row_of(item) for item in range(4))
    repeat = repeat.astype(bf16)
    inside = iota((channels, wide), 0) // GROUP == iota((channels, wide), 1) // entries

    def matrix(ref):
        flat = ref[...].reshape(channels, entries).astype(bf16)
        full = jnp.dot(flat, repeat, preferred_element_type=f32)
        return jnp.where(inside, full, 0.0).astype(bf16)

    def by_rows(left, right):
        return lax.dot_general(
            left, right, (((1,), (1,)), ((), ())), preferred_element_type=f32
        )

    loads[0].wait()
    loads[1].wait()
    step = 16
    for start in range(0, count, step):
        flt = tokens[start : start + step, :].astype(f32)
        scale = lax.rsqrt(jnp.mean(flt * flt, axis=-1, keepdims=True) + 1e-06)
        normed[start : start + step, :] = (flt * scale * mix_gain[...]).astype(bf16)
    loads[2].wait()
    drive = jnp.dot(normed[...], in_proj[...], preferred_element_type=f32).astype(bf16)
    for load in loads[6:12]:
        load.wait()
    push_a = jnp.dot(drive, matrix(b_real), preferred_element_type=f32)
    push_b = jnp.dot(drive, matrix(b_imag), preferred_element_type=f32)
    old_re, old_im = old[0], old[1]
    new_re = abar_re * old_re - abar_im * old_im + fac_re * push_a - fac_im * push_b
    fresh[0] = new_re
    new_im = abar_re * old_im + abar_im * old_re + fac_re * push_b + fac_im * push_a
    fresh[1] = new_im
    store = pltpu.make_async_copy(fresh, fresh_hbm, sems.at[13])
    store.start()
    readout = (
        by_rows(new_re.astype(bf16), matrix(c_real))
        - by_rows(new_im.astype(bf16), matrix(c_imag))
        + skip_gain[...] * drive.astype(f32)
    )
    reads = jax.nn.gelu(readout).astype(bf16)
    loads[12].wait()
    span = min(1024, partial.shape[1])
    for start in range(0, partial.shape[1], span):
        partial[:, start : start + span] = jnp.dot(
            reads, out_proj[:, start : start + span], preferred_element_type=f32
        ).astype(bf16)
    store.wait()


def mixer(*arrays):
    tokens, states = arrays[0], arrays[-2]
    far = pl.BlockSpec(memory_space=pl.ANY)
    return pl.pallas_call(
        mixer_kernel,
        out_shape=(
            jax.ShapeDtypeStruct(tokens.shape, jnp.bfloat16),
            jax.ShapeDtypeStruct(states.shape, jnp.float32),
        ),
        in_specs=[far] * len(arrays),
        out_specs=(pl.BlockSpec(memory_space=pltpu.VMEM), far),
        scratch_shapes=[pltpu.VMEM(array.shape, array.dtype) for array in arrays]
        + [
            pltpu.VMEM(states.shape, jnp.float32),
            pltpu.VMEM(tokens.shape, jnp.bfloat16),
            pltpu.SemaphoreType.DMA((14,)),
        ],
        compiler_params=pltpu.CompilerParams(vmem_limit_bytes=62 << 20),
    )(*arrays)


class Chain:
    def __init__(self, size):
        self.size = size
        self.x_size = fast_extent("ep", size)
        self.z_size = size // self.x_size
        self.me = lax.axis_index("ep")
        self.x = self.me % self.x_size
        self.z = self.me // self.x_size
        self.pending = []

    def at(self, j):
        left, right = self.z, self.z_size - 1 - self.z
        both = jnp.minimum(left, right)
        if j == 0:
            return self.z
        near = (j + 1) // 2
        paired = self.z - near if j % 2 else self.z + near
        single = jnp.where(left > right, self.z - (j - both), self.z + (j - both))
        return jnp.where(j <= 2 * both, paired, single)

    def traced_at(self, j):
        left, right = self.z, self.z_size - 1 - self.z
        both = jnp.minimum(left, right)
        near = (j + 1) // 2
        paired = jnp.where(j % 2 == 1, self.z - near, self.z + near)
        single = jnp.where(left > right, self.z - (j - both), self.z + (j - both))
        return jnp.where(j <= 2 * both, paired, single)

    def index(self, z, x_step):
        return z * self.x_size + (self.x + x_step + self.x_size) % self.x_size

    def copy(self, source, target, sent, landed, peer):
        return pltpu.make_async_remote_copy(
            src_ref=source,
            dst_ref=target,
            send_sem=sent,
            recv_sem=landed,
            device_id={"ep": peer},
            device_id_type=MESH,
        )

    def launch(self, copy, cond=None):
        if cond is None:
            copy.start()
        else:
            pl.when(cond)(copy.start)
        self.pending.append((copy, cond))

    def finish(self):
        for copy, cond in self.pending:
            if cond is None:
                copy.wait_send()
            else:
                pl.when(cond)(copy.wait_send)


def layer_kernel(ep_size, tp_size, top, cap, names, *refs):
    partial, ffn_gain, route_ids, route_logits = refs[:4]
    weights_hbm, branch_hbm, tokens_hbm = refs[4:10], refs[10], refs[11]
    out, resid_cols, refs = refs[12], refs[13], refs[14:]
    r = dict(zip(names, refs))
    extra = list(refs[len(names) :])
    own_cols, side, late = r["own_cols"], r["side"], r["late"]
    f32, bf16 = jnp.float32, jnp.bfloat16
    chain, grid = Chain(ep_size), Grid("tp", tp_size)
    z_size, x_size, z, x = chain.z_size, chain.x_size, chain.z, chain.x
    rounds = ep_size // tp_size
    pieces = min(tp_size, 4)
    count, width = own_cols.shape

    def take(number):
        taken = extra[:number]
        del extra[:number]
        return taken

    dense_sums, hidden_gathers, row_gathers, expert_sums = [], [], [], []
    both, every_hidden, own_hidden, full, part = [], [], [], [], []
    for g in range(rounds):
        stores = take(5)
        for target, store in zip((both, every_hidden, own_hidden, full, part), stores):
            target.append(store)
        dense_sums.append(Reduce(grid, both[g], 1, False, take(8)))
        hidden_gathers.append(Gather(grid, own_hidden[g], every_hidden[g], 1, False, take(5)))
        row_gathers.append(
            Gather(grid, None, full[g], pieces, True, take(5), (tp_size * cap, width))
        )
        expert_sums.append(Reduce(grid, part[g], pieces, True, take(8)))

    mix = Reduce(grid, partial, PIECES, True, take(8))
    mine = pl.ds(pl.multiple_of(grid.me * width, 128), width)
    near = [r[name] for name in WEIGHTS]
    loads = []
    transfers = list(zip(weights_hbm, near))
    transfers.insert(0, (tokens_hbm.at[:, mine], r["tokens"]))
    transfers.insert(1, (branch_hbm.at[mine], r["branch"]))
    for item, (source, target) in enumerate(transfers):
        load = pltpu.make_async_copy(source, target, r["load_sems"].at[item])
        load.start()
        loads.append(load)
    first_loads, loads = loads[:2], loads[2:]
    dense_gate, dense_up, gate, up, down, dense_down = near
    barrier = pltpu.get_barrier_semaphore()
    for k in range(1, x_size):
        pl.semaphore_signal(
            barrier, inc=1, device_id={"ep": chain.index(z, k)}, device_id_type=MESH
        )
    ends = (z > 0, z - 1), (z < z_size - 1, z + 1)
    for cond, at in ends:

        @pl.when(cond)
        def _():
            pl.semaphore_signal(
                barrier, inc=1, device_id={"ep": at * x_size + x}, device_id_type=MESH
            )
    for k in range(1, tp_size):
        pl.semaphore_signal(
            barrier, inc=1, device_id={"tp": (grid.me + k) % tp_size}, device_id_type=MESH
        )
    beside = (z + z_size - 1) // z_size + (2 * z_size - 2 - z) // z_size
    pl.semaphore_wait(barrier, x_size + tp_size - 2 + beside)
    mix.push()
    logits = route_logits[...]
    raised = jnp.exp(logits - jnp.max(logits, axis=0, keepdims=True))
    side[...] = jnp.zeros((8, 128), f32)
    late[...] = jnp.zeros((8, 128), f32)
    side[0:top, 0:count] = route_ids[...].astype(f32)
    side[top : 2 * top, 0:count] = raised / jnp.sum(raised, axis=0, keepdims=True)
    for load in first_loads:
        load.wait()
    mix.relay()

    cols, sides, lates = r["cols"], r["sides"], r["lates"]

    def chunk(j, q=0):
        return chain.index(chain.at(j), -q)

    step = count // PIECES

    def spot_of(source, p):
        if p >= PIECES:
            return (sides, lates)[p - PIECES].at[source]
        return cols.at[source, pl.ds(p * step, step), :]

    def chunk_of(j, q):
        return chain.index(chain.traced_at(j), -q)

    def send_chunk(j, p, cond=None, record=True, along=True, across=True):
        at = chain.at(j)
        spot = spot_of(chunk(j), p)
        if j:
            source = spot
        else:
            source = (side, late)[p - PIECES] if p >= PIECES else own_cols.at[pl.ds(p * step, step), :]
        copies = []
        for turn, move, go in (
            (0, 1, (at <= z) & (z < z_size - 1)),
            (1, -1, (at >= z) & (z > 0)),
        ) if along else ():
            copy = chain.copy(
                source,
                spot,
                r["z_sent"].at[turn, j, p],
                r["z_landed"].at[at, p],
                jnp.where(go, z + move, z) * x_size + x,
            )
            copies.append((copy, go))
        for q in range(1, x_size) if across else ():
            copy = chain.copy(
                source,
                spot,
                r["x_sent"].at[q - 1, j, p],
                r["x_landed"].at[q - 1, j, p],
                chain.index(z, q),
            )
            copies.append((copy, None))
        for copy, go in copies:
            if go is None:
                copy.start() if cond is None else pl.when(cond)(copy.start)
            else:
                pl.when(go if cond is None else go & cond)(copy.start)
            if record:
                chain.pending.append((copy, go))

    def wait_piece(j, q, p):
        spot = spot_of(chunk(j, q), p)
        if q:
            landed = r["x_landed"].at[q - 1, j, p]
        else:
            landed = r["z_landed"].at[chain.at(j), p]
        chain.copy(spot, spot, r["x_sent"].at[0, 0, 0], landed, chain.index(z, 1)).wait_recv()

    def wait_chunk(j, q):
        for p in PARTS:
            wait_piece(j, q, p)

    gain = ffn_gain[:, mine]
    gate_row = gain * r["branch"][...].astype(f32).reshape(1, width)
    lanes = lax.broadcasted_iota(jnp.int32, (count, 128), 1)
    tables = []
    send_chunk(0, PIECES)
    for p in reversed(range(PIECES)):
        span = mix.span(p)
        mixed = mix.collect_piece(p).astype(bf16).astype(f32)
        resid = (r["tokens"][span, :].astype(f32) + mixed).astype(bf16)
        resid_cols[span, :] = resid
        flt = resid.astype(f32)
        own_cols[span, :] = (flt * gain).astype(bf16)
        send_chunk(0, p)
        ssq = jnp.sum(flt * flt, axis=1, keepdims=True)
        dots = jnp.sum(flt * gate_row, axis=1, keepdims=True)
        tables.insert(0, jnp.where(lanes[:step] == 0, ssq, jnp.where(lanes[:step] == 1, dots, 0.0)))
    if count < 128:
        tables.append(jnp.zeros((128 - count, 128), f32))
    stat = jnp.concatenate(tables, axis=0).T[:8]
    r["stat"][...] = stat
    copies = []
    for k in range(1, tp_size):
        copy = grid.copy(
            r["stat"],
            r["stat_got"].at[k - 1],
            r["stat_sent"].at[k - 1],
            r["stat_landed"].at[k - 1],
            (grid.me + k) % tp_size,
        )
        copy.start()
        copies.append(copy)

    def finish_stat(stat=stat):
        for k, copy in enumerate(copies):
            copy.wait_recv()
            stat = stat + r["stat_got"][k]
        scale = lax.rsqrt(stat[0:1] / (width * tp_size) + 1e-06)
        late[0:1, :] = jax.nn.sigmoid(stat[1:2] * scale)
        late[1:2, :] = scale
        lates[chain.me] = late[...]
        send_chunk(0, PIECES + 1)
    hidden_width = dense_gate.shape[1]
    expert = chain.me.astype(f32)
    lane_ok = (lax.broadcasted_iota(jnp.int32, (1, 128), 1) < count).astype(f32)
    slots = lax.broadcasted_iota(jnp.int32, (128, 128), 0).astype(f32)
    before = (
        lax.broadcasted_iota(jnp.int32, (128, 128), 0)
        < lax.broadcasted_iota(jnp.int32, (128, 128), 1)
    ).astype(bf16)

    def process(j, q):
        i = j * x_size + q
        g, at = i // tp_size, i % tp_size
        if i == 0:
            block, info = own_cols[...], side[...]
        else:
            source = chunk(j, q)
            block, info = cols[source], sides[source]
        taken, weight = jnp.zeros((1, 128), f32), jnp.zeros((1, 128), f32)
        for item in range(top):
            hit = jnp.where(info[item : item + 1] == expert, lane_ok, 0.0)
            taken = taken + hit
            weight = weight + hit * info[top + item : top + item + 1]
        rank = jnp.dot(
            jnp.broadcast_to(taken, (8, 128)).astype(bf16), before, preferred_element_type=f32
        )[0:1]
        table = jnp.where(slots == rank, taken, 0.0)
        rows = jnp.dot(
            table[:cap, :count].astype(bf16), block, preferred_element_type=f32
        )
        full[g][at * cap : (at + 1) * cap, mine] = rows.astype(bf16)
        share = tp_size // pieces
        if at % share == share - 1:
            row_gathers[g].start_piece(at // share)
        r["table"][i] = table
        r["turned"][i] = (table * weight).T
        if i == 0:
            loads[0].wait()
            loads[1].wait()
        both[g][at, :, :hidden_width] = jnp.dot(
            block, dense_gate[...], preferred_element_type=f32
        ).astype(bf16)
        both[g][at, :, hidden_width:] = jnp.dot(
            block, dense_up[...], preferred_element_type=f32
        ).astype(bf16)
        if at == tp_size - 1:
            dense_sums[g].push()
        if at == 0 and g > 0:
            dense_sums[g - 1].relay()

    inner = gate.shape[1]
    tile = tile_of(inner)
    hidden = r["hidden"]

    def expert_hidden(g):
        row_gathers[g].relay()
        for at in range(tp_size):
            i = g * tp_size + at
            row = lates[chunk(i // x_size, i % x_size), 1:2, :]
            scales = jnp.sum(r["table"][i] * row, axis=1, keepdims=True)
            r["row_scale"][g, at * cap : (at + 1) * cap, :] = jnp.broadcast_to(
                scales[:cap], (cap, 128)
            )
        row_gathers[g].arrive()
        rows = full[g]

        @pl.loop(0, inner // tile)
        def _(step):
            span = pl.ds(pl.multiple_of(step * tile, 128), tile)
            scale = r["row_scale"][g, :, 0:1]
            gate_val = jnp.dot(rows[...], gate[:, span], preferred_element_type=f32) * scale
            up_val = jnp.dot(rows[...], up[:, span], preferred_element_type=f32) * scale
            hidden[g, :, span] = (jax.nn.silu(gate_val) * up_val).astype(bf16)

    wide = min(WIDE, width)

    def expert_part(g):
        target = part[g]

        @pl.loop(0, tp_size * width // wide)
        def _(step):
            span = pl.ds(pl.multiple_of(step * wide, 128), wide)
            target[:, span] = jnp.dot(
                hidden[g], down[:, span], preferred_element_type=f32
            ).astype(bf16)

    def dense_hidden(g):
        i = g * tp_size + grid.me
        source = chunk_of(i // x_size, i % x_size)
        turned = jnp.concatenate([lates[source], jnp.zeros((120, 128), f32)], axis=0).T[:count]
        branch, scale = turned[:, 0:1], turned[:, 1:2]

        def emit(span, value):
            value = value * scale
            own_hidden[g][span, :] = (
                branch * jax.nn.silu(value[:, :hidden_width]) * value[:, hidden_width:]
            ).astype(bf16)

        dense_sums[g].collect(emit)
        hidden_gathers[g].start()

    fewer = jnp.minimum(z, z_size - 1 - z)

    def pass_on(j, p, cond=None, record=True, **kinds):
        def wait():
            wait_piece(j, 0, p)

        wait() if cond is None else pl.when(cond)(wait)
        send_chunk(j, p, cond, record, **kinds)

    last = rounds - 1
    end = z_size - 1
    process(0, 0)
    finish_stat()
    for j in range(1, end):
        if j % 2:
            two = j + 1 < end
            paired = j + 1 <= 2 * fewer
            for p in PARTS:
                pass_on(j, p)
                if two:
                    pass_on(j + 1, p, paired, across=False)
            if two:
                for p in PARTS:
                    send_chunk(j + 1, p, paired, along=False)
        else:
            for p in PARTS:
                pass_on(j, p, j > 2 * fewer, False)
        for q in range(1, x_size):
            wait_chunk(j - 1, q)
            process(j - 1, q)
        process(j, 0)
    for p in PARTS:
        pass_on(end, p, fewer > 0)
    for q in range(1, x_size):
        wait_chunk(end - 1, q)
        process(end - 1, q)
    for load in loads[2:5]:
        load.wait()
    for g in range(last):
        expert_hidden(g)
    for p in PARTS:
        pass_on(end, p, fewer == 0, False)
    process(end, 0)
    for g in range(last):
        dense_hidden(g)
        expert_part(g)
        expert_sums[g].push()
    for q in range(1, x_size):
        wait_chunk(end, q)
        process(end, q)
    dense_sums[last].relay()
    expert_sums[0].relay(range(pieces // 2))
    expert_hidden(last)
    expert_part(last)
    expert_sums[last].push()
    dense_hidden(last)
    for g in reversed(range(1, rounds)):
        expert_sums[g].relay()
    expert_sums[0].relay(range(pieces // 2, pieces))
    for g in range(rounds):
        hidden_gathers[g].relay()
    for g in range(rounds):
        hidden_gathers[g].arrive()
    loads[5].wait()

    collected, own_share = set(), r["own_share"]

    def share_of(j, q):
        i = j * x_size + q
        g, at = i // tp_size, i % tp_size
        chunks = tp_size // pieces
        piece = at // chunks
        if (g, piece) not in collected:
            collected.add((g, piece))
            rows = chunks * cap
            r["expert_out"][g, piece * rows : (piece + 1) * rows, :] = (
                expert_sums[g].collect_piece(piece).astype(bf16)
            )
        turned = r["turned"][i]
        routed = jnp.dot(
            turned[:count, :cap].astype(bf16),
            r["expert_out"][g, at * cap : (at + 1) * cap, :],
            preferred_element_type=f32,
        )
        dense = jnp.dot(every_hidden[g][at], dense_down[...], preferred_element_type=f32)
        return routed + dense

    def send_share(j):
        own_share[j] = share_of(j, 0)

    def send_twins(j):
        for q in range(1, x_size):
            i = j * x_size + q
            r["x_share"][i] = share_of(j, q).astype(bf16)
            for p in range(PIECES):
                span = pl.ds(p * step, step)
                copy = chain.copy(
                    r["x_share"].at[i, span, :],
                    r["x_got"].at[j, q - 1, span, :],
                    r["xs_sent"].at[i, p],
                    r["xs_landed"].at[j, q - 1, p],
                    chain.index(z, -q),
                )
                chain.launch(copy)

    def finish_share(j):
        at = chain.at(j)
        for p in range(PIECES):
            finish_piece(j, at, pl.ds(p * step, step), p)

    def finish_piece(j, at, span, p):
        for q in range(1, x_size):
            spot = r["x_got"].at[j, q - 1, span, :]
            chain.copy(
                spot,
                spot,
                r["xs_sent"].at[0, 0],
                r["xs_landed"].at[j, q - 1, p],
                chain.index(z, q),
            ).wait_recv()
            own_share[j, span, :] = own_share[j, span, :] + r["x_got"][j, q - 1, span, :].astype(f32)
        for turn, cond in (
            (0, (at <= z) & (z < z_size - 1)),
            (1, (at >= z) & (z > 0)),
        ):

            @pl.when(cond)
            def _():
                spot = r["z_got"].at[turn, at, span, :]
                chain.copy(
                    spot,
                    spot,
                    r["zs_sent"].at[0, 0],
                    r["zs_landed"].at[turn, at, p],
                    chain.index(z, 1),
                ).wait_recv()
                own_share[j, span, :] = own_share[j, span, :] + r["z_got"][
                    turn, at, span, :
                ].astype(f32)

        if j == 0:
            out[span, :] = own_share[0, span, :].astype(bf16)
        else:
            r["z_share"][j, span, :] = own_share[j, span, :].astype(bf16)
            turn = jnp.where(at < z, 0, 1)
            copy = chain.copy(
                r["z_share"].at[j, span, :],
                r["z_got"].at[turn, at, span, :],
                r["zs_sent"].at[j, p],
                r["zs_landed"].at[turn, at, p],
                jnp.where(at < z, z - 1, z + 1) * x_size + x,
            )
            chain.launch(copy)

    for j in reversed(range(z_size)):
        send_twins(j)
        if j + 1 < z_size:
            finish_share(j + 1)
        send_share(j)
    finish_share(0)
    chain.finish()
    for copy in copies:
        copy.wait_send()
    for phase in [mix] + dense_sums + hidden_gathers + row_gathers + expert_sums:
        phase.finish()


PIECES = 2
PARTS = (2, 1, 0, 3)
WIDE = 512
WEIGHTS = ("dense_gate", "dense_up", "gate", "up", "down", "dense_down")


def layer(partial, ffn_gain, route_ids, route_logits, weights, branch_gate, tokens, ep_size, tp_size):
    count, width = tokens.shape[0], tokens.shape[1] // tp_size
    top = route_ids.shape[0]
    bf16, f32 = jnp.bfloat16, jnp.float32
    vmem, dma = pltpu.VMEM, pltpu.SemaphoreType.DMA
    x_size = fast_extent("ep", ep_size)
    z_size = ep_size // x_size
    cap = max(2, 2 * count * top // ep_size)
    cap = -(-cap // 16) * 16
    hidden_width, inner = weights[0].shape[1], weights[2].shape[1]
    rounds, rows = ep_size // tp_size, tp_size * cap
    pieces = min(tp_size, 4)
    fast = fast_extent("tp", tp_size)
    slow = tp_size // fast
    named = {name: vmem(array.shape, bf16) for name, array in zip(WEIGHTS, weights)}
    named.update(
        load_sems=dma((len(weights) + 2,)),
        tokens=vmem((count, width), bf16),
        branch=vmem((width,), bf16),
        own_cols=vmem((count, width), bf16),
        side=vmem((8, 128), f32),
        late=vmem((8, 128), f32),
        stat=vmem((8, 128), f32),
        stat_got=vmem((tp_size - 1, 8, 128), f32),
        stat_sent=dma((tp_size - 1,)),
        stat_landed=dma((tp_size - 1,)),
        cols=vmem((ep_size, count, width), bf16),
        sides=vmem((ep_size, 8, 128), f32),
        lates=vmem((ep_size, 8, 128), f32),
        table=vmem((ep_size, 128, 128), f32),
        row_scale=vmem((rounds, rows, 128), f32),
        turned=vmem((ep_size, 128, 128), f32),
        hidden=vmem((rounds, rows, inner), bf16),
        expert_out=vmem((rounds, rows, width), bf16),
        own_share=vmem((z_size, count, width), f32),
        x_share=vmem((ep_size, count, width), bf16),
        x_got=vmem((z_size, x_size - 1, count, width), bf16),
        z_share=vmem((z_size, count, width), bf16),
        z_got=vmem((2, z_size, count, width), bf16),
        z_sent=dma((2, z_size, PIECES + 2)),
        z_landed=dma((z_size, PIECES + 2)),
        x_sent=dma((x_size - 1, z_size, PIECES + 2)),
        x_landed=dma((x_size - 1, z_size, PIECES + 2)),
        xs_sent=dma((ep_size, PIECES)),
        xs_landed=dma((z_size, x_size - 1, PIECES)),
        zs_sent=dma((z_size, PIECES)),
        zs_landed=dma((2, z_size, PIECES)),
    )
    extra = []
    for _ in range(rounds):
        extra += [
            vmem((tp_size, count, 2 * hidden_width), bf16),
            vmem((tp_size, count, hidden_width), bf16),
            vmem((count, hidden_width), bf16),
            vmem((rows, tp_size * width), bf16),
            vmem((rows, tp_size * width), bf16),
        ]
        extra += reduce_scratch(fast, slow, count, 2 * hidden_width, 1)
        extra += gather_sems(fast, slow, 1) + gather_sems(fast, slow, pieces)
        extra += reduce_scratch(fast, slow, rows, width, pieces)
    extra += reduce_scratch(fast, slow, count, width, PIECES)
    whole = pl.BlockSpec(memory_space=pltpu.VMEM)
    far = pl.BlockSpec(memory_space=pl.ANY)
    return pl.pallas_call(
        functools.partial(layer_kernel, ep_size, tp_size, top, cap, tuple(named)),
        out_shape=(jax.ShapeDtypeStruct((count, width), bf16),) * 2,
        in_specs=[whole] * 4 + [far] * (len(weights) + 2),
        out_specs=(whole, whole),
        scratch_shapes=list(named.values()) + extra,
        compiler_params=pltpu.CompilerParams(
            collective_id=0, has_side_effects=True, vmem_limit_bytes=62 << 20
        ),
    )(partial, ffn_gain, route_ids, route_logits, *weights, branch_gate, tokens)


def shards(
    tokens,
    mix_gain,
    ffn_gain,
    in_proj,
    decay_rate,
    frequency,
    log_step,
    b_real,
    b_imag,
    c_real,
    c_imag,
    skip_gain,
    states,
    out_proj,
    route_ids,
    route_logits,
    expert_gate,
    expert_up,
    expert_down,
    dense_gate,
    dense_up,
    dense_down,
    branch_gate,
):
    tp_count = lax.axis_size("tp")
    ep_count = lax.axis_size("ep")
    partial, new_states = mixer(
        tokens,
        mix_gain.reshape(1, -1),
        in_proj,
        decay_rate,
        frequency,
        log_step.reshape(1, -1),
        jnp.swapaxes(b_real, 1, 2),
        jnp.swapaxes(b_imag, 1, 2),
        c_real,
        c_imag,
        skip_gain.reshape(1, -1),
        states,
        out_proj,
    )
    weights = (
        dense_gate,
        dense_up,
        expert_gate[0],
        expert_up[0],
        expert_down[0],
        dense_down,
    )
    gathered, resid_cols = layer(
        partial,
        ffn_gain.reshape(1, -1),
        route_ids.T,
        route_logits.T,
        weights,
        branch_gate,
        tokens,
        ep_count,
        tp_count,
    )
    output = (resid_cols.astype(jnp.float32) + gathered.astype(jnp.float32)).astype(jnp.bfloat16)
    return (output, new_states)


def solution(mesh):
    return jax.shard_map(
        shards,
        mesh=mesh,
        in_specs=(
            P("ep", None),
            P(),
            P(),
            P(None, "tp"),
            P("tp", None),
            P("tp", None),
            P("tp"),
            P("tp", None, None),
            P("tp", None, None),
            P("tp", None, None),
            P("tp", None, None),
            P("tp"),
            P(None, "ep", "tp"),
            P("tp", None),
            P("ep", None),
            P("ep", None),
            P("ep", None, "tp"),
            P("ep", None, "tp"),
            P("ep", "tp", None),
            P("tp", "ep"),
            P("tp", "ep"),
            P("ep", "tp"),
            P(),
        ),
        out_specs=(P("ep", "tp"), P(None, "ep", "tp")),
        check_vma=False,
    )
```

```python
import functools
import jax
import jax.numpy as jnp
from jax import lax
from jax.experimental import pallas as pl
from jax.experimental.pallas import tpu as pltpu
from jax.sharding import PartitionSpec as P

GROUP = 16
STATE = 64
MESH = pl.DeviceIdType.MESH


def fast_extent(axis, size):
    if axis == "tp":
        return 2
    extent = 1
    while (2 * extent) * (2 * extent) * 2 <= size:
        extent *= 2
    return extent


class Grid:
    def __init__(self, axis, size):
        self.axis, self.size = axis, size
        self.fast = fast_extent(axis, size)
        self.slow = size // self.fast
        self.me = lax.axis_index(axis)
        self.at_fast = self.me % self.fast
        self.at_slow = self.me // self.fast

    def index(self, slow_step, fast_step):
        slow_at = (self.at_slow + slow_step + self.slow) % self.slow
        fast_at = (self.at_fast + fast_step + self.fast) % self.fast
        return slow_at * self.fast + fast_at

    def peers(self):
        return [self.index(k, 0) for k in range(1, self.slow)] + [
            self.index(0, q) for q in range(1, self.fast)
        ]

    def copy(self, source, target, sent, landed, peer):
        return pltpu.make_async_remote_copy(
            src_ref=source,
            dst_ref=target,
            send_sem=sent,
            recv_sem=landed,
            device_id={self.axis: peer},
            device_id_type=MESH,
        )


def part_of(ref, owner, start, rows, width, cols):
    if cols:
        return ref.at[pl.ds(start, rows), pl.ds(pl.multiple_of(owner * width, 128), width)]
    return ref.at[owner, pl.ds(start, rows), :]


class Gather:
    def __init__(self, grid, source, target, number, cols, sems, shape=None):
        self.grid, self.source, self.target, self.cols = grid, source, target, cols
        self.slow_sent, self.slow_landed, self.fast_sent, self.fast_landed, self.own_sem = sems
        self.rows, self.width = shape or source.shape
        self.step = self.rows // number
        self.number = number
        self.pending = []

    def piece(self, j):
        if self.source is None:
            return self.place(self.grid.me, j)
        return self.source.at[pl.ds(j * self.step, self.step), :]

    def place(self, owner, j):
        return part_of(self.target, owner, j * self.step, self.step, self.width, self.cols)

    def slow_copy(self, source, target, j, k, peer):
        return self.grid.copy(
            source, target, self.slow_sent.at[j, k - 1], self.slow_landed.at[j, k - 1], peer
        )

    def fast_copy(self, source, target, j, k, q, peer):
        return self.grid.copy(
            source, target, self.fast_sent.at[j, k, q - 1], self.fast_landed.at[j, k, q - 1], peer
        )

    def launch(self, copy):
        copy.start()
        self.pending.append(copy)

    def start_piece(self, j):
        grid = self.grid
        piece, spot = self.piece(j), self.place(grid.me, j)
        for k in range(1, grid.slow):
            self.launch(self.slow_copy(piece, spot, j, k, grid.index(k, 0)))
        for q in range(1, grid.fast):
            self.launch(self.fast_copy(piece, spot, j, 0, q, grid.index(0, q)))

    def start(self):
        for j in range(self.number):
            self.start_piece(j)
        if self.source is not None:
            self.own = pltpu.make_async_copy(
                self.source,
                part_of(self.target, self.grid.me, 0, self.rows, self.width, self.cols),
                self.own_sem,
            )
            self.own.start()

    def relay(self):
        grid = self.grid
        for j in range(self.number):
            for k in range(1, grid.slow):
                spot = self.place(grid.index(-k, 0), j)
                self.slow_copy(spot, spot, j, k, grid.index(-k, 0)).wait_recv()
                for q in range(1, grid.fast):
                    self.launch(self.fast_copy(spot, spot, j, k, q, grid.index(0, q)))

    def arrive(self):
        grid = self.grid
        for j in range(self.number):
            for k in range(grid.slow):
                for q in range(1, grid.fast):
                    spot = self.place(grid.index(-k, -q), j)
                    self.fast_copy(spot, spot, j, k, q, grid.index(0, -q)).wait_recv()
        if self.source is not None:
            self.own.wait()

    def finish(self):
        for copy in self.pending:
            copy.wait_send()


def gather_sems(grid_fast, grid_slow, number):
    return [
        pltpu.SemaphoreType.DMA((number, grid_slow - 1)),
        pltpu.SemaphoreType.DMA((number, grid_slow - 1)),
        pltpu.SemaphoreType.DMA((number, grid_slow, grid_fast - 1)),
        pltpu.SemaphoreType.DMA((number, grid_slow, grid_fast - 1)),
        pltpu.SemaphoreType.DMA,
    ]


class Reduce:
    def __init__(self, grid, source, number, cols, scratch):
        self.grid, self.source, self.cols, self.number = grid, source, cols, number
        self.got_fast, self.mid, self.got_slow, self.total = scratch[:4]
        self.fast_sent, self.fast_landed, self.slow_sent, self.slow_landed = scratch[4:]
        rows, self.width = self.total.shape
        self.step = rows // number
        self.pending = []

    def part(self, dest, j):
        return part_of(self.source, dest, j * self.step, self.step, self.width, self.cols)

    def span(self, j):
        return pl.ds(j * self.step, self.step)

    def fast_copy(self, source, k, j, q, peer):
        return self.grid.copy(
            source,
            self.got_fast.at[q - 1, k - 1, self.span(j), :],
            self.fast_sent.at[q - 1, k - 1, j],
            self.fast_landed.at[q - 1, k - 1, j],
            peer,
        )

    def slow_copy(self, k, j, peer):
        return self.grid.copy(
            self.mid.at[k - 1, self.span(j), :],
            self.got_slow.at[k - 1, self.span(j), :],
            self.slow_sent.at[k - 1, j],
            self.slow_landed.at[k - 1, j],
            peer,
        )

    def push_part(self, k, q):
        grid = self.grid
        for j in reversed(range(self.number)):
            copy = self.fast_copy(self.part(grid.index(k, q), j), k, j, q, grid.index(0, q))
            copy.start()
            self.pending.append(copy)

    def push(self):
        for k in range(1, self.grid.slow + 1):
            for q in range(1, self.grid.fast):
                self.push_part(k, q)

    def relay(self, pieces=None):
        grid = self.grid
        for k in range(1, grid.slow + 1):
            for j in reversed(range(self.number) if pieces is None else pieces):
                value = self.part(grid.index(k, 0), j)[...].astype(jnp.float32)
                for q in range(1, grid.fast):
                    block = self.got_fast.at[q - 1, k - 1, self.span(j), :]
                    self.fast_copy(block, k, j, q, grid.index(0, -q)).wait_recv()
                    value = value + block[...].astype(jnp.float32)
                if k == grid.slow:
                    self.total[self.span(j), :] = value
                else:
                    self.mid[k - 1, self.span(j), :] = value.astype(self.mid.dtype)
                    copy = self.slow_copy(k, j, grid.index(k, 0))
                    copy.start()
                    self.pending.append(copy)

    def collect_piece(self, j):
        value = self.total[self.span(j), :]
        for k in range(1, self.grid.slow):
            self.slow_copy(k, j, self.grid.index(-k, 0)).wait_recv()
            value = value + self.got_slow[k - 1, self.span(j), :].astype(jnp.float32)
        return value

    def collect(self, emit):
        for j in range(self.number):
            emit(self.span(j), self.collect_piece(j))

    def finish(self):
        for copy in self.pending:
            copy.wait_send()


def reduce_scratch(fast, slow, rows, width, number):
    return [
        pltpu.VMEM((fast - 1, slow, rows, width), jnp.bfloat16),
        pltpu.VMEM((slow - 1, rows, width), jnp.bfloat16),
        pltpu.VMEM((slow - 1, rows, width), jnp.bfloat16),
        pltpu.VMEM((rows, width), jnp.float32),
        pltpu.SemaphoreType.DMA((fast - 1, slow, number)),
        pltpu.SemaphoreType.DMA((fast - 1, slow, number)),
        pltpu.SemaphoreType.DMA((slow - 1, number)),
        pltpu.SemaphoreType.DMA((slow - 1, number)),
    ]


def tile_of(extent):
    for tile in (256, 128):
        if extent % tile == 0:
            return tile
    return extent


def mixer_kernel(
    *refs,
):
    far, partial, fresh_hbm = refs[:13], refs[13], refs[14]
    near, fresh, normed, sems = refs[15:28], refs[28], refs[29], refs[30]
    loads = []
    for item, (source, target) in enumerate(zip(far, near)):
        load = pltpu.make_async_copy(source, target, sems.at[item])
        load.start()
        loads.append(load)
    tokens, mix_gain, in_proj, decay_rate, frequency, log_step = near[:6]
    b_real, b_imag, c_real, c_imag, skip_gain, old, out_proj = near[6:]
    count, width = tokens.shape
    groups, entries = decay_rate.shape
    channels = skip_gain.shape[1]
    wide = groups * entries
    f32, bf16 = jnp.float32, jnp.bfloat16

    def iota(shape, dim):
        return lax.broadcasted_iota(jnp.int32, shape, dim)

    for item in range(3, 6):
        loads[item].wait()
    eye = iota((groups, groups), 0) == iota((groups, groups), 1)
    step_size = jnp.exp(jnp.sum(jnp.where(eye, log_step[...], 0.0), axis=1, keepdims=True))
    lam_re, lam_im = -decay_rate[...], frequency[...]
    magnitude = jnp.exp(lam_re * step_size)
    abar_re = magnitude * jnp.cos(lam_im * step_size)
    abar_im = magnitude * jnp.sin(lam_im * step_size)
    denom = lam_re * lam_re + lam_im * lam_im
    fac_re = ((abar_re - 1.0) * lam_re + abar_im * lam_im) / denom
    fac_im = (abar_im * lam_re - (abar_re - 1.0) * lam_im) / denom
    packed = jnp.concatenate([abar_re, abar_im, fac_re, fac_im], axis=0)
    repeat = (iota((entries, wide), 1) % entries == iota((entries, wide), 0)).astype(f32)
    spread = jnp.dot(packed, repeat, precision=lax.Precision.HIGHEST, preferred_element_type=f32)
    owner = iota((groups, wide), 1) // entries == iota((groups, wide), 0)

    def row_of(item):
        part = spread[item * groups : (item + 1) * groups]
        return jnp.sum(jnp.where(owner, part, 0.0), axis=0, keepdims=True)

    abar_re, abar_im, fac_re, fac_im = (row_of(item) for item in range(4))
    repeat = repeat.astype(bf16)
    inside = iota((channels, wide), 0) // GROUP == iota((channels, wide), 1) // entries

    def matrix(ref):
        flat = ref[...].reshape(channels, entries).astype(bf16)
        full = jnp.dot(flat, repeat, preferred_element_type=f32)
        return jnp.where(inside, full, 0.0).astype(bf16)

    def by_rows(left, right):
        return lax.dot_general(
            left, right, (((1,), (1,)), ((), ())), preferred_element_type=f32
        )

    loads[0].wait()
    loads[1].wait()
    step = 16
    for start in range(0, count, step):
        flt = tokens[start : start + step, :].astype(f32)
        scale = lax.rsqrt(jnp.mean(flt * flt, axis=-1, keepdims=True) + 1e-06)
        normed[start : start + step, :] = (flt * scale * mix_gain[...]).astype(bf16)
    loads[2].wait()
    drive = jnp.dot(normed[...], in_proj[...], preferred_element_type=f32).astype(bf16)
    for load in loads[6:12]:
        load.wait()
    push_a = jnp.dot(drive, matrix(b_real), preferred_element_type=f32)
    push_b = jnp.dot(drive, matrix(b_imag), preferred_element_type=f32)
    old_re, old_im = old[0], old[1]
    new_re = abar_re * old_re - abar_im * old_im + fac_re * push_a - fac_im * push_b
    fresh[0] = new_re
    new_im = abar_re * old_im + abar_im * old_re + fac_re * push_b + fac_im * push_a
    fresh[1] = new_im
    store = pltpu.make_async_copy(fresh, fresh_hbm, sems.at[13])
    store.start()
    readout = (
        by_rows(new_re.astype(bf16), matrix(c_real))
        - by_rows(new_im.astype(bf16), matrix(c_imag))
        + skip_gain[...] * drive.astype(f32)
    )
    reads = jax.nn.gelu(readout).astype(bf16)
    loads[12].wait()
    span = min(1024, partial.shape[1])
    for start in range(0, partial.shape[1], span):
        partial[:, start : start + span] = jnp.dot(
            reads, out_proj[:, start : start + span], preferred_element_type=f32
        ).astype(bf16)
    store.wait()


def mixer(*arrays):
    tokens, states = arrays[0], arrays[-2]
    far = pl.BlockSpec(memory_space=pl.ANY)
    return pl.pallas_call(
        mixer_kernel,
        out_shape=(
            jax.ShapeDtypeStruct(tokens.shape, jnp.bfloat16),
            jax.ShapeDtypeStruct(states.shape, jnp.float32),
        ),
        in_specs=[far] * len(arrays),
        out_specs=(pl.BlockSpec(memory_space=pltpu.VMEM), far),
        scratch_shapes=[pltpu.VMEM(array.shape, array.dtype) for array in arrays]
        + [
            pltpu.VMEM(states.shape, jnp.float32),
            pltpu.VMEM(tokens.shape, jnp.bfloat16),
            pltpu.SemaphoreType.DMA((14,)),
        ],
        compiler_params=pltpu.CompilerParams(vmem_limit_bytes=62 << 20),
    )(*arrays)


class Chain:
    def __init__(self, size):
        self.size = size
        self.x_size = fast_extent("ep", size)
        self.z_size = size // self.x_size
        self.me = lax.axis_index("ep")
        self.x = self.me % self.x_size
        self.z = self.me // self.x_size
        self.pending = []

    def at(self, j):
        left, right = self.z, self.z_size - 1 - self.z
        both = jnp.minimum(left, right)
        if j == 0:
            return self.z
        near = (j + 1) // 2
        paired = self.z - near if j % 2 else self.z + near
        single = jnp.where(left > right, self.z - (j - both), self.z + (j - both))
        return jnp.where(j <= 2 * both, paired, single)

    def traced_at(self, j):
        left, right = self.z, self.z_size - 1 - self.z
        both = jnp.minimum(left, right)
        near = (j + 1) // 2
        paired = jnp.where(j % 2 == 1, self.z - near, self.z + near)
        single = jnp.where(left > right, self.z - (j - both), self.z + (j - both))
        return jnp.where(j <= 2 * both, paired, single)

    def index(self, z, x_step):
        return z * self.x_size + (self.x + x_step + self.x_size) % self.x_size

    def copy(self, source, target, sent, landed, peer):
        return pltpu.make_async_remote_copy(
            src_ref=source,
            dst_ref=target,
            send_sem=sent,
            recv_sem=landed,
            device_id={"ep": peer},
            device_id_type=MESH,
        )

    def launch(self, copy, cond=None):
        if cond is None:
            copy.start()
        else:
            pl.when(cond)(copy.start)
        self.pending.append((copy, cond))

    def finish(self):
        for copy, cond in self.pending:
            if cond is None:
                copy.wait_send()
            else:
                pl.when(cond)(copy.wait_send)
        self.pending = []


def layer_kernel(ep_size, tp_size, top, cap, names, *refs):
    partial, ffn_gain, route_ids, route_logits = refs[:4]
    weights_hbm, branch_hbm, tokens_hbm = refs[4:10], refs[10], refs[11]
    out, refs = refs[12], refs[13:]
    r = dict(zip(names, refs))
    extra = list(refs[len(names) :])
    own_cols, resid_cols = r["own_cols"], r["resid_cols"]
    side, late = r["side"], r["late"]
    f32, bf16 = jnp.float32, jnp.bfloat16
    chain, grid = Chain(ep_size), Grid("tp", tp_size)
    z_size, x_size, z, x = chain.z_size, chain.x_size, chain.z, chain.x
    rounds = ep_size // tp_size
    pieces = min(tp_size, 4)
    count, width = own_cols.shape

    def take(number):
        taken = extra[:number]
        del extra[:number]
        return taken

    dense_sums, hidden_gathers, row_gathers, expert_sums = [], [], [], []
    both, every_hidden, own_hidden, full, part = [], [], [], [], []
    for g in range(rounds):
        stores = take(5)
        for target, store in zip((both, every_hidden, own_hidden, full, part), stores):
            target.append(store)
        dense_sums.append(Reduce(grid, both[g], 1, False, take(8)))
        hidden_gathers.append(Gather(grid, own_hidden[g], every_hidden[g], 1, False, take(5)))
        row_gathers.append(
            Gather(grid, None, full[g], pieces, True, take(5), (tp_size * cap, width))
        )
        expert_sums.append(Reduce(grid, part[g], pieces, True, take(8)))

    mix = Reduce(grid, partial, PIECES, True, take(8))
    mine = pl.ds(pl.multiple_of(grid.me * width, 128), width)
    near = [r[name] for name in WEIGHTS]
    loads = []
    transfers = list(zip(weights_hbm, near))
    transfers.insert(0, (tokens_hbm.at[:, mine], r["tokens"]))
    transfers.insert(1, (branch_hbm.at[mine], r["branch"]))
    for item, (source, target) in enumerate(transfers):
        load = pltpu.make_async_copy(source, target, r["load_sems"].at[item])
        load.start()
        loads.append(load)
    first_loads, loads = loads[:2], loads[2:]
    dense_gate, dense_up, gate, up, down, dense_down = near
    barrier = pltpu.get_barrier_semaphore()
    for k in range(1, x_size):
        pl.semaphore_signal(
            barrier, inc=1, device_id={"ep": chain.index(z, k)}, device_id_type=MESH
        )
    ends = (z > 0, z - 1), (z < z_size - 1, z + 1)
    for cond, at in ends:

        @pl.when(cond)
        def _():
            pl.semaphore_signal(
                barrier, inc=1, device_id={"ep": at * x_size + x}, device_id_type=MESH
            )
    for k in range(1, tp_size):
        pl.semaphore_signal(
            barrier, inc=1, device_id={"tp": (grid.me + k) % tp_size}, device_id_type=MESH
        )
    beside = (z + z_size - 1) // z_size + (2 * z_size - 2 - z) // z_size
    pl.semaphore_wait(barrier, x_size + tp_size - 2 + beside)
    mix.push()
    logits = route_logits[...]
    raised = jnp.exp(logits - jnp.max(logits, axis=0, keepdims=True))
    side[...] = jnp.zeros((8, 128), f32)
    late[...] = jnp.zeros((8, 128), f32)
    side[0:top, 0:count] = route_ids[...].astype(f32)
    side[top : 2 * top, 0:count] = raised / jnp.sum(raised, axis=0, keepdims=True)
    for load in first_loads:
        load.wait()
    mix.relay()

    cols, sides, lates = r["cols"], r["sides"], r["lates"]

    def chunk(j, q=0):
        return chain.index(chain.at(j), -q)

    step = count // PIECES

    def spot_of(source, p):
        if p >= PIECES:
            return (sides, lates)[p - PIECES].at[source]
        return cols.at[source, pl.ds(p * step, step), :]

    def chunk_of(j, q):
        return chain.index(chain.traced_at(j), -q)

    def send_chunk(j, p, cond=None, record=True, along=True, across=True):
        at = chain.at(j)
        spot = spot_of(chunk(j), p)
        if j:
            source = spot
        else:
            source = (side, late)[p - PIECES] if p >= PIECES else own_cols.at[pl.ds(p * step, step), :]
        copies = []
        for turn, move, go in (
            (0, 1, (at <= z) & (z < z_size - 1)),
            (1, -1, (at >= z) & (z > 0)),
        ) if along else ():
            copy = chain.copy(
                source,
                spot,
                r["z_sent"].at[turn, j, p],
                r["z_landed"].at[at, p],
                jnp.where(go, z + move, z) * x_size + x,
            )
            copies.append((copy, go))
        for q in range(1, x_size) if across else ():
            copy = chain.copy(
                source,
                spot,
                r["x_sent"].at[q - 1, j, p],
                r["x_landed"].at[q - 1, j, p],
                chain.index(z, q),
            )
            copies.append((copy, None))
        for copy, go in copies:
            if go is None:
                copy.start() if cond is None else pl.when(cond)(copy.start)
            else:
                pl.when(go if cond is None else go & cond)(copy.start)
            if record:
                chain.pending.append((copy, go))

    def wait_piece(j, q, p):
        spot = spot_of(chunk(j, q), p)
        if q:
            landed = r["x_landed"].at[q - 1, j, p]
        else:
            landed = r["z_landed"].at[chain.at(j), p]
        chain.copy(spot, spot, r["x_sent"].at[0, 0, 0], landed, chain.index(z, 1)).wait_recv()

    def wait_chunk(j, q):
        for p in PARTS:
            wait_piece(j, q, p)

    gain = ffn_gain[:, mine]
    gate_row = gain * r["branch"][...].astype(f32).reshape(1, width)
    lanes = lax.broadcasted_iota(jnp.int32, (count, 128), 1)
    tables = []
    send_chunk(0, PIECES)
    for p in reversed(range(PIECES)):
        span = mix.span(p)
        mixed = mix.collect_piece(p).astype(bf16).astype(f32)
        resid = (r["tokens"][span, :].astype(f32) + mixed).astype(bf16)
        resid_cols[span, :] = resid
        flt = resid.astype(f32)
        own_cols[span, :] = (flt * gain).astype(bf16)
        send_chunk(0, p)
        ssq = jnp.sum(flt * flt, axis=1, keepdims=True)
        dots = jnp.sum(flt * gate_row, axis=1, keepdims=True)
        tables.insert(0, jnp.where(lanes[:step] == 0, ssq, jnp.where(lanes[:step] == 1, dots, 0.0)))
    if count < 128:
        tables.append(jnp.zeros((128 - count, 128), f32))
    stat = jnp.concatenate(tables, axis=0).T[:8]
    r["stat"][...] = stat
    copies = []
    for k in range(1, tp_size):
        copy = grid.copy(
            r["stat"],
            r["stat_got"].at[k - 1],
            r["stat_sent"].at[k - 1],
            r["stat_landed"].at[k - 1],
            (grid.me + k) % tp_size,
        )
        copy.start()
        copies.append(copy)

    def finish_stat(stat=stat):
        for k, copy in enumerate(copies):
            copy.wait_recv()
            stat = stat + r["stat_got"][k]
        scale = lax.rsqrt(stat[0:1] / (width * tp_size) + 1e-06)
        late[0:1, :] = jax.nn.sigmoid(stat[1:2] * scale)
        late[1:2, :] = scale
        lates[chain.me] = late[...]
        send_chunk(0, PIECES + 1)
    hidden_width = dense_gate.shape[1]
    expert = chain.me.astype(f32)
    lane_ok = (lax.broadcasted_iota(jnp.int32, (1, 128), 1) < count).astype(f32)
    slots = lax.broadcasted_iota(jnp.int32, (128, 128), 0).astype(f32)
    before = (
        lax.broadcasted_iota(jnp.int32, (128, 128), 0)
        < lax.broadcasted_iota(jnp.int32, (128, 128), 1)
    ).astype(bf16)

    def process(j, q):
        i = j * x_size + q
        g, at = i // tp_size, i % tp_size
        if i == 0:
            block, info = own_cols[...], side[...]
        else:
            source = chunk(j, q)
            block, info = cols[source], sides[source]
        taken, weight = jnp.zeros((1, 128), f32), jnp.zeros((1, 128), f32)
        for item in range(top):
            hit = jnp.where(info[item : item + 1] == expert, lane_ok, 0.0)
            taken = taken + hit
            weight = weight + hit * info[top + item : top + item + 1]
        rank = jnp.dot(
            jnp.broadcast_to(taken, (8, 128)).astype(bf16), before, preferred_element_type=f32
        )[0:1]
        table = jnp.where(slots == rank, taken, 0.0)
        rows = jnp.dot(
            table[:cap, :count].astype(bf16), block, preferred_element_type=f32
        )
        full[g][at * cap : (at + 1) * cap, mine] = rows.astype(bf16)
        share = tp_size // pieces
        if at % share == share - 1:
            row_gathers[g].start_piece(at // share)
        r["table"][i] = table
        r["turned"][i] = (table * weight).T
        if i == 0:
            loads[0].wait()
            loads[1].wait()
        both[g][at, :, :hidden_width] = jnp.dot(
            block, dense_gate[...], preferred_element_type=f32
        ).astype(bf16)
        both[g][at, :, hidden_width:] = jnp.dot(
            block, dense_up[...], preferred_element_type=f32
        ).astype(bf16)
        if at == tp_size - 1:
            dense_sums[g].push()
        if at == 0 and g > 0:
            dense_sums[g - 1].relay()

    inner = gate.shape[1]
    tile = tile_of(inner)
    hidden = r["hidden"]

    def expert_hidden(g):
        row_gathers[g].relay()
        for at in range(tp_size):
            i = g * tp_size + at
            row = lates[chunk(i // x_size, i % x_size), 1:2, :]
            scales = jnp.sum(r["table"][i] * row, axis=1, keepdims=True)
            r["row_scale"][g, at * cap : (at + 1) * cap, :] = jnp.broadcast_to(
                scales[:cap], (cap, 128)
            )
        row_gathers[g].arrive()
        rows = full[g]

        @pl.loop(0, inner // tile)
        def _(step):
            span = pl.ds(pl.multiple_of(step * tile, 128), tile)
            scale = r["row_scale"][g, :, 0:1]
            gate_val = jnp.dot(rows[...], gate[:, span], preferred_element_type=f32) * scale
            up_val = jnp.dot(rows[...], up[:, span], preferred_element_type=f32) * scale
            hidden[g, :, span] = (jax.nn.silu(gate_val) * up_val).astype(bf16)

    wide = min(WIDE, width)

    def expert_part(g):
        target = part[g]

        @pl.loop(0, tp_size * width // wide)
        def _(step):
            span = pl.ds(pl.multiple_of(step * wide, 128), wide)
            target[:, span] = jnp.dot(
                hidden[g], down[:, span], preferred_element_type=f32
            ).astype(bf16)

    def dense_hidden(g):
        i = g * tp_size + grid.me
        source = chunk_of(i // x_size, i % x_size)
        turned = jnp.concatenate([lates[source], jnp.zeros((120, 128), f32)], axis=0).T[:count]
        branch, scale = turned[:, 0:1], turned[:, 1:2]

        def emit(span, value):
            value = value * scale
            own_hidden[g][span, :] = (
                branch * jax.nn.silu(value[:, :hidden_width]) * value[:, hidden_width:]
            ).astype(bf16)

        dense_sums[g].collect(emit)
        hidden_gathers[g].start()

    fewer = jnp.minimum(z, z_size - 1 - z)

    def pass_on(j, p, cond=None, record=True, **kinds):
        def wait():
            wait_piece(j, 0, p)

        wait() if cond is None else pl.when(cond)(wait)
        send_chunk(j, p, cond, record, **kinds)

    last = rounds - 1
    end = z_size - 1
    process(0, 0)
    finish_stat()
    for j in range(1, end):
        if j % 2:
            two = j + 1 < end
            paired = j + 1 <= 2 * fewer
            for p in PARTS:
                pass_on(j, p)
                if two:
                    pass_on(j + 1, p, paired, across=False)
            if two:
                for p in PARTS:
                    send_chunk(j + 1, p, paired, along=False)
        else:
            for p in PARTS:
                pass_on(j, p, j > 2 * fewer, False)
        if j == end - 1:
            for p in PARTS:
                pass_on(end, p, fewer > 0)
        for q in range(1, x_size):
            wait_chunk(j - 1, q)
            process(j - 1, q)
        process(j, 0)
    for q in range(1, x_size):
        wait_chunk(end - 1, q)
        process(end - 1, q)
    for p in PARTS:
        pass_on(end, p, fewer == 0, False)
    for load in loads[2:5]:
        load.wait()
    for g in range(last):
        expert_hidden(g)
    process(end, 0)
    for q in range(1, x_size):
        wait_chunk(end, q)
        process(end, q)
    dense_sums[last].relay()
    for g in range(last):
        dense_hidden(g)
        expert_part(g)
        expert_sums[g].push()
    expert_hidden(last)
    expert_part(last)
    expert_sums[last].push()
    dense_hidden(last)
    expert_sums[last].relay()
    for g in reversed(range(last)):
        expert_sums[g].relay()
    for copy in copies:
        copy.wait_send()
    for phase in [mix] + row_gathers + dense_sums:
        phase.finish()
    chain.finish()
    loads[5].wait()

    collected, own_share = set(), r["own_share"]

    def share_of(j, q):
        i = j * x_size + q
        g, at = i // tp_size, i % tp_size
        chunks = tp_size // pieces
        piece = at // chunks
        if g not in collected:
            collected.add(g)
            hidden_gathers[g].relay()
            hidden_gathers[g].arrive()
        if (g, piece) not in collected:
            collected.add((g, piece))
            rows = chunks * cap
            r["expert_out"][g, piece * rows : (piece + 1) * rows, :] = (
                expert_sums[g].collect_piece(piece).astype(bf16)
            )
        turned = r["turned"][i]
        routed = jnp.dot(
            turned[:count, :cap].astype(bf16),
            r["expert_out"][g, at * cap : (at + 1) * cap, :],
            preferred_element_type=f32,
        )
        dense = jnp.dot(every_hidden[g][at], dense_down[...], preferred_element_type=f32)
        return routed + dense

    def send_share(j):
        own_share[j] = share_of(j, 0)

    def send_twins(j):
        for q in range(1, x_size):
            i = j * x_size + q
            r["x_share"][i] = share_of(j, q).astype(bf16)
            for p in range(PIECES):
                span = pl.ds(p * step, step)
                copy = chain.copy(
                    r["x_share"].at[i, span, :],
                    r["x_got"].at[j, q - 1, span, :],
                    r["xs_sent"].at[i, p],
                    r["xs_landed"].at[j, q - 1, p],
                    chain.index(z, -q),
                )
                chain.launch(copy)

    def finish_share(j):
        at = chain.at(j)
        for p in range(PIECES):
            finish_piece(j, at, pl.ds(p * step, step), p)

    def finish_piece(j, at, span, p):
        for q in range(1, x_size):
            spot = r["x_got"].at[j, q - 1, span, :]
            chain.copy(
                spot,
                spot,
                r["xs_sent"].at[0, 0],
                r["xs_landed"].at[j, q - 1, p],
                chain.index(z, q),
            ).wait_recv()
            own_share[j, span, :] = own_share[j, span, :] + r["x_got"][j, q - 1, span, :].astype(f32)
        for turn, cond in (
            (0, (at <= z) & (z < z_size - 1)),
            (1, (at >= z) & (z > 0)),
        ):

            @pl.when(cond)
            def _():
                spot = r["z_got"].at[turn, at, span, :]
                chain.copy(
                    spot,
                    spot,
                    r["zs_sent"].at[0, 0],
                    r["zs_landed"].at[turn, at, p],
                    chain.index(z, 1),
                ).wait_recv()
                own_share[j, span, :] = own_share[j, span, :] + r["z_got"][
                    turn, at, span, :
                ].astype(f32)

        if j == 0:
            total = own_share[0, span, :].astype(bf16).astype(f32)
            out[span, :] = (resid_cols[span, :].astype(f32) + total).astype(bf16)
        else:
            r["z_share"][j, span, :] = own_share[j, span, :].astype(bf16)
            share_copy(j, p).start()

    def share_copy(j, p):
        at, span = chain.at(j), pl.ds(p * step, step)
        turn = jnp.where(at < z, 0, 1)
        return chain.copy(
            r["z_share"].at[j, span, :],
            r["z_got"].at[turn, at, span, :],
            r["zs_sent"].at[j, p],
            r["zs_landed"].at[turn, at, p],
            jnp.where(at < z, z - 1, z + 1) * x_size + x,
        )

    def finish_if(cond, j):
        if 0 < j < z_size:
            pl.when(cond)(functools.partial(finish_share, j))

    for j in reversed(range(z_size)):
        send_twins(j)
        finish_if(fewer == 0, j + 1)
        finish_if(fewer > 0, j + 2)
        send_share(j)
    finish_if(fewer > 0, 1)
    finish_share(0)
    for j in range(1, z_size):
        for p in range(PIECES):
            share_copy(j, p).wait_send()
    chain.finish()
    for phase in hidden_gathers + expert_sums:
        phase.finish()


PIECES = 2
PARTS = (2, 1, 0, 3)
WIDE = 512
WEIGHTS = ("dense_gate", "dense_up", "gate", "up", "down", "dense_down")


def layer(partial, ffn_gain, route_ids, route_logits, weights, branch_gate, tokens, ep_size, tp_size):
    count, width = tokens.shape[0], tokens.shape[1] // tp_size
    top = route_ids.shape[0]
    bf16, f32 = jnp.bfloat16, jnp.float32
    vmem, dma = pltpu.VMEM, pltpu.SemaphoreType.DMA
    x_size = fast_extent("ep", ep_size)
    z_size = ep_size // x_size
    cap = max(2, 2 * count * top // ep_size)
    cap = -(-cap // 16) * 16
    hidden_width, inner = weights[0].shape[1], weights[2].shape[1]
    rounds, rows = ep_size // tp_size, tp_size * cap
    pieces = min(tp_size, 4)
    fast = fast_extent("tp", tp_size)
    slow = tp_size // fast
    named = {name: vmem(array.shape, bf16) for name, array in zip(WEIGHTS, weights)}
    named.update(
        load_sems=dma((len(weights) + 2,)),
        tokens=vmem((count, width), bf16),
        branch=vmem((width,), bf16),
        own_cols=vmem((count, width), bf16),
        resid_cols=vmem((count, width), bf16),
        side=vmem((8, 128), f32),
        late=vmem((8, 128), f32),
        stat=vmem((8, 128), f32),
        stat_got=vmem((tp_size - 1, 8, 128), f32),
        stat_sent=dma((tp_size - 1,)),
        stat_landed=dma((tp_size - 1,)),
        cols=vmem((ep_size, count, width), bf16),
        sides=vmem((ep_size, 8, 128), f32),
        lates=vmem((ep_size, 8, 128), f32),
        table=vmem((ep_size, 128, 128), f32),
        row_scale=vmem((rounds, rows, 128), f32),
        turned=vmem((ep_size, 128, 128), f32),
        hidden=vmem((rounds, rows, inner), bf16),
        expert_out=vmem((rounds, rows, width), bf16),
        own_share=vmem((z_size, count, width), f32),
        x_share=vmem((ep_size, count, width), bf16),
        x_got=vmem((z_size, x_size - 1, count, width), bf16),
        z_share=vmem((z_size, count, width), bf16),
        z_got=vmem((2, z_size, count, width), bf16),
        z_sent=dma((2, z_size, PIECES + 2)),
        z_landed=dma((z_size, PIECES + 2)),
        x_sent=dma((x_size - 1, z_size, PIECES + 2)),
        x_landed=dma((x_size - 1, z_size, PIECES + 2)),
        xs_sent=dma((ep_size, PIECES)),
        xs_landed=dma((z_size, x_size - 1, PIECES)),
        zs_sent=dma((z_size, PIECES)),
        zs_landed=dma((2, z_size, PIECES)),
    )
    extra = []
    for _ in range(rounds):
        extra += [
            vmem((tp_size, count, 2 * hidden_width), bf16),
            vmem((tp_size, count, hidden_width), bf16),
            vmem((count, hidden_width), bf16),
            vmem((rows, tp_size * width), bf16),
            vmem((rows, tp_size * width), bf16),
        ]
        extra += reduce_scratch(fast, slow, count, 2 * hidden_width, 1)
        extra += gather_sems(fast, slow, 1) + gather_sems(fast, slow, pieces)
        extra += reduce_scratch(fast, slow, rows, width, pieces)
    extra += reduce_scratch(fast, slow, count, width, PIECES)
    whole = pl.BlockSpec(memory_space=pltpu.VMEM)
    far = pl.BlockSpec(memory_space=pl.ANY)
    return pl.pallas_call(
        functools.partial(layer_kernel, ep_size, tp_size, top, cap, tuple(named)),
        out_shape=jax.ShapeDtypeStruct((count, width), bf16),
        in_specs=[whole] * 4 + [far] * (len(weights) + 2),
        out_specs=whole,
        scratch_shapes=list(named.values()) + extra,
        compiler_params=pltpu.CompilerParams(
            collective_id=0, has_side_effects=True, vmem_limit_bytes=62 << 20
        ),
    )(partial, ffn_gain, route_ids, route_logits, *weights, branch_gate, tokens)


def shards(
    tokens,
    mix_gain,
    ffn_gain,
    in_proj,
    decay_rate,
    frequency,
    log_step,
    b_real,
    b_imag,
    c_real,
    c_imag,
    skip_gain,
    states,
    out_proj,
    route_ids,
    route_logits,
    expert_gate,
    expert_up,
    expert_down,
    dense_gate,
    dense_up,
    dense_down,
    branch_gate,
):
    tp_count = lax.axis_size("tp")
    ep_count = lax.axis_size("ep")
    partial, new_states = mixer(
        tokens,
        mix_gain.reshape(1, -1),
        in_proj,
        decay_rate,
        frequency,
        log_step.reshape(1, -1),
        jnp.swapaxes(b_real, 1, 2),
        jnp.swapaxes(b_imag, 1, 2),
        c_real,
        c_imag,
        skip_gain.reshape(1, -1),
        states,
        out_proj,
    )
    weights = (
        dense_gate,
        dense_up,
        expert_gate[0],
        expert_up[0],
        expert_down[0],
        dense_down,
    )
    output = layer(
        partial,
        ffn_gain.reshape(1, -1),
        route_ids.T,
        route_logits.T,
        weights,
        branch_gate,
        tokens,
        ep_count,
        tp_count,
    )
    return (output, new_states)


def solution(mesh):
    return jax.shard_map(
        shards,
        mesh=mesh,
        in_specs=(
            P("ep", None),
            P(),
            P(),
            P(None, "tp"),
            P("tp", None),
            P("tp", None),
            P("tp"),
            P("tp", None, None),
            P("tp", None, None),
            P("tp", None, None),
            P("tp", None, None),
            P("tp"),
            P(None, "ep", "tp"),
            P("tp", None),
            P("ep", None),
            P("ep", None),
            P("ep", None, "tp"),
            P("ep", None, "tp"),
            P("ep", "tp", None),
            P("tp", "ep"),
            P("tp", "ep"),
            P("ep", "tp"),
            P(),
        ),
        out_specs=(P("ep", "tp"), P(None, "ep", "tp")),
        check_vma=False,
    )
```

```python
import functools
import jax
import jax.numpy as jnp
from jax import lax
from jax.experimental import pallas as pl
from jax.experimental.pallas import tpu as pltpu
from jax.sharding import PartitionSpec as P

GROUP = 16
STATE = 64
MESH = pl.DeviceIdType.MESH


def fast_extent(axis, size):
    if axis == "tp":
        return 2
    extent = 1
    while (2 * extent) * (2 * extent) * 2 <= size:
        extent *= 2
    return extent


class Grid:
    def __init__(self, axis, size):
        self.axis, self.size = axis, size
        self.fast = fast_extent(axis, size)
        self.slow = size // self.fast
        self.me = lax.axis_index(axis)
        self.at_fast = self.me % self.fast
        self.at_slow = self.me // self.fast

    def index(self, slow_step, fast_step):
        slow_at = (self.at_slow + slow_step + self.slow) % self.slow
        fast_at = (self.at_fast + fast_step + self.fast) % self.fast
        return slow_at * self.fast + fast_at

    def peers(self):
        return [self.index(k, 0) for k in range(1, self.slow)] + [
            self.index(0, q) for q in range(1, self.fast)
        ]

    def copy(self, source, target, sent, landed, peer):
        return pltpu.make_async_remote_copy(
            src_ref=source,
            dst_ref=target,
            send_sem=sent,
            recv_sem=landed,
            device_id={self.axis: peer},
            device_id_type=MESH,
        )


def part_of(ref, owner, start, rows, width, cols):
    if cols:
        return ref.at[pl.ds(start, rows), pl.ds(pl.multiple_of(owner * width, 128), width)]
    return ref.at[owner, pl.ds(start, rows), :]


class Gather:
    def __init__(self, grid, source, target, number, cols, sems, shape=None):
        self.grid, self.source, self.target, self.cols = grid, source, target, cols
        self.slow_sent, self.slow_landed, self.fast_sent, self.fast_landed, self.own_sem = sems
        self.rows, self.width = shape or source.shape
        self.step = self.rows // number
        self.number = number
        self.pending = []

    def piece(self, j):
        if self.source is None:
            return self.place(self.grid.me, j)
        return self.source.at[pl.ds(j * self.step, self.step), :]

    def place(self, owner, j):
        return part_of(self.target, owner, j * self.step, self.step, self.width, self.cols)

    def slow_copy(self, source, target, j, k, peer):
        return self.grid.copy(
            source, target, self.slow_sent.at[j, k - 1], self.slow_landed.at[j, k - 1], peer
        )

    def fast_copy(self, source, target, j, k, q, peer):
        return self.grid.copy(
            source, target, self.fast_sent.at[j, k, q - 1], self.fast_landed.at[j, k, q - 1], peer
        )

    def launch(self, copy):
        copy.start()
        self.pending.append(copy)

    def start_piece(self, j):
        grid = self.grid
        piece, spot = self.piece(j), self.place(grid.me, j)
        for k in range(1, grid.slow):
            self.launch(self.slow_copy(piece, spot, j, k, grid.index(k, 0)))
        for q in range(1, grid.fast):
            self.launch(self.fast_copy(piece, spot, j, 0, q, grid.index(0, q)))

    def start(self):
        for j in range(self.number):
            self.start_piece(j)
        if self.source is not None:
            self.own = pltpu.make_async_copy(
                self.source,
                part_of(self.target, self.grid.me, 0, self.rows, self.width, self.cols),
                self.own_sem,
            )
            self.own.start()

    def relay(self):
        grid = self.grid
        for j in range(self.number):
            for k in range(1, grid.slow):
                spot = self.place(grid.index(-k, 0), j)
                self.slow_copy(spot, spot, j, k, grid.index(-k, 0)).wait_recv()
                for q in range(1, grid.fast):
                    self.launch(self.fast_copy(spot, spot, j, k, q, grid.index(0, q)))

    def arrive(self):
        grid = self.grid
        for j in range(self.number):
            for k in range(grid.slow):
                for q in range(1, grid.fast):
                    spot = self.place(grid.index(-k, -q), j)
                    self.fast_copy(spot, spot, j, k, q, grid.index(0, -q)).wait_recv()
        if self.source is not None:
            self.own.wait()

    def finish(self):
        for copy in self.pending:
            copy.wait_send()


def gather_sems(grid_fast, grid_slow, number):
    return [
        pltpu.SemaphoreType.DMA((number, grid_slow - 1)),
        pltpu.SemaphoreType.DMA((number, grid_slow - 1)),
        pltpu.SemaphoreType.DMA((number, grid_slow, grid_fast - 1)),
        pltpu.SemaphoreType.DMA((number, grid_slow, grid_fast - 1)),
        pltpu.SemaphoreType.DMA,
    ]


class Reduce:
    def __init__(self, grid, source, number, cols, scratch):
        self.grid, self.source, self.cols, self.number = grid, source, cols, number
        self.got_fast, self.mid, self.got_slow, self.total = scratch[:4]
        self.fast_sent, self.fast_landed, self.slow_sent, self.slow_landed = scratch[4:]
        rows, self.width = self.total.shape
        self.step = rows // number
        self.pending = []

    def part(self, dest, j):
        return part_of(self.source, dest, j * self.step, self.step, self.width, self.cols)

    def span(self, j):
        return pl.ds(j * self.step, self.step)

    def fast_copy(self, source, k, j, q, peer):
        return self.grid.copy(
            source,
            self.got_fast.at[q - 1, k - 1, self.span(j), :],
            self.fast_sent.at[q - 1, k - 1, j],
            self.fast_landed.at[q - 1, k - 1, j],
            peer,
        )

    def slow_copy(self, k, j, peer):
        return self.grid.copy(
            self.mid.at[k - 1, self.span(j), :],
            self.got_slow.at[k - 1, self.span(j), :],
            self.slow_sent.at[k - 1, j],
            self.slow_landed.at[k - 1, j],
            peer,
        )

    def push_part(self, k, q):
        grid = self.grid
        for j in reversed(range(self.number)):
            copy = self.fast_copy(self.part(grid.index(k, q), j), k, j, q, grid.index(0, q))
            copy.start()
            self.pending.append(copy)

    def push(self):
        for k in range(1, self.grid.slow + 1):
            for q in range(1, self.grid.fast):
                self.push_part(k, q)

    def relay(self, pieces=None):
        grid = self.grid
        for k in range(1, grid.slow + 1):
            for j in reversed(range(self.number) if pieces is None else pieces):
                value = self.part(grid.index(k, 0), j)[...].astype(jnp.float32)
                for q in range(1, grid.fast):
                    block = self.got_fast.at[q - 1, k - 1, self.span(j), :]
                    self.fast_copy(block, k, j, q, grid.index(0, -q)).wait_recv()
                    value = value + block[...].astype(jnp.float32)
                if k == grid.slow:
                    self.total[self.span(j), :] = value
                else:
                    self.mid[k - 1, self.span(j), :] = value.astype(self.mid.dtype)
                    copy = self.slow_copy(k, j, grid.index(k, 0))
                    copy.start()
                    self.pending.append(copy)

    def collect_piece(self, j):
        value = self.total[self.span(j), :]
        for k in range(1, self.grid.slow):
            self.slow_copy(k, j, self.grid.index(-k, 0)).wait_recv()
            value = value + self.got_slow[k - 1, self.span(j), :].astype(jnp.float32)
        return value

    def collect(self, emit):
        for j in range(self.number):
            emit(self.span(j), self.collect_piece(j))

    def finish(self):
        for copy in self.pending:
            copy.wait_send()


def reduce_scratch(fast, slow, rows, width, number):
    return [
        pltpu.VMEM((fast - 1, slow, rows, width), jnp.bfloat16),
        pltpu.VMEM((slow - 1, rows, width), jnp.bfloat16),
        pltpu.VMEM((slow - 1, rows, width), jnp.bfloat16),
        pltpu.VMEM((rows, width), jnp.float32),
        pltpu.SemaphoreType.DMA((fast - 1, slow, number)),
        pltpu.SemaphoreType.DMA((fast - 1, slow, number)),
        pltpu.SemaphoreType.DMA((slow - 1, number)),
        pltpu.SemaphoreType.DMA((slow - 1, number)),
    ]


def tile_of(extent):
    for tile in (256, 128):
        if extent % tile == 0:
            return tile
    return extent


def mixer_kernel(
    *refs,
):
    far, partial, fresh_hbm = refs[:13], refs[13], refs[14]
    near, fresh, normed, sems = refs[15:28], refs[28], refs[29], refs[30]
    loads = []
    for item, (source, target) in enumerate(zip(far, near)):
        loads.append(pltpu.make_async_copy(source, target, sems.at[item]))
    for item in (3, 4, 5, 0, 1, 2, 6, 7, 11, 8, 9, 10, 12):
        loads[item].start()
    tokens, mix_gain, in_proj, decay_rate, frequency, log_step = near[:6]
    b_real, b_imag, c_real, c_imag, skip_gain, old, out_proj = near[6:]
    count, width = tokens.shape
    groups, entries = decay_rate.shape
    channels = skip_gain.shape[1]
    wide = groups * entries
    f32, bf16 = jnp.float32, jnp.bfloat16

    def iota(shape, dim):
        return lax.broadcasted_iota(jnp.int32, shape, dim)

    for item in range(3, 6):
        loads[item].wait()
    eye = iota((groups, groups), 0) == iota((groups, groups), 1)
    step_size = jnp.exp(jnp.sum(jnp.where(eye, log_step[...], 0.0), axis=1, keepdims=True))
    lam_re, lam_im = -decay_rate[...], frequency[...]
    magnitude = jnp.exp(lam_re * step_size)
    abar_re = magnitude * jnp.cos(lam_im * step_size)
    abar_im = magnitude * jnp.sin(lam_im * step_size)
    denom = lam_re * lam_re + lam_im * lam_im
    fac_re = ((abar_re - 1.0) * lam_re + abar_im * lam_im) / denom
    fac_im = (abar_im * lam_re - (abar_re - 1.0) * lam_im) / denom
    packed = jnp.concatenate([abar_re, abar_im, fac_re, fac_im], axis=0)
    repeat = (iota((entries, wide), 1) % entries == iota((entries, wide), 0)).astype(f32)
    spread = jnp.dot(packed, repeat, precision=lax.Precision.HIGHEST, preferred_element_type=f32)
    owner = iota((groups, wide), 1) // entries == iota((groups, wide), 0)

    def row_of(item):
        part = spread[item * groups : (item + 1) * groups]
        return jnp.sum(jnp.where(owner, part, 0.0), axis=0, keepdims=True)

    abar_re, abar_im, fac_re, fac_im = (row_of(item) for item in range(4))
    repeat = repeat.astype(bf16)
    inside = iota((channels, wide), 0) // GROUP == iota((channels, wide), 1) // entries

    def matrix(ref):
        flat = ref[...].reshape(channels, entries).astype(bf16)
        full = jnp.dot(flat, repeat, preferred_element_type=f32)
        return jnp.where(inside, full, 0.0).astype(bf16)

    def by_rows(left, right):
        return lax.dot_general(
            left, right, (((1,), (1,)), ((), ())), preferred_element_type=f32
        )

    loads[0].wait()
    loads[1].wait()
    step = 16
    for start in range(0, count, step):
        flt = tokens[start : start + step, :].astype(f32)
        scale = lax.rsqrt(jnp.mean(flt * flt, axis=-1, keepdims=True) + 1e-06)
        normed[start : start + step, :] = (flt * scale * mix_gain[...]).astype(bf16)
    loads[2].wait()
    drive = jnp.dot(normed[...], in_proj[...], preferred_element_type=f32).astype(bf16)
    for load in loads[6:12]:
        load.wait()
    push_a = jnp.dot(drive, matrix(b_real), preferred_element_type=f32)
    push_b = jnp.dot(drive, matrix(b_imag), preferred_element_type=f32)
    old_re, old_im = old[0], old[1]
    new_re = abar_re * old_re - abar_im * old_im + fac_re * push_a - fac_im * push_b
    fresh[0] = new_re
    new_im = abar_re * old_im + abar_im * old_re + fac_re * push_b + fac_im * push_a
    fresh[1] = new_im
    store = pltpu.make_async_copy(fresh, fresh_hbm, sems.at[13])
    store.start()
    readout = (
        by_rows(new_re.astype(bf16), matrix(c_real))
        - by_rows(new_im.astype(bf16), matrix(c_imag))
        + skip_gain[...] * drive.astype(f32)
    )
    reads = jax.nn.gelu(readout).astype(bf16)
    loads[12].wait()
    span = min(1024, partial.shape[1])
    for start in range(0, partial.shape[1], span):
        partial[:, start : start + span] = jnp.dot(
            reads, out_proj[:, start : start + span], preferred_element_type=f32
        ).astype(bf16)
    store.wait()


def mixer(*arrays):
    tokens, states = arrays[0], arrays[-2]
    far = pl.BlockSpec(memory_space=pl.ANY)
    return pl.pallas_call(
        mixer_kernel,
        out_shape=(
            jax.ShapeDtypeStruct(tokens.shape, jnp.bfloat16),
            jax.ShapeDtypeStruct(states.shape, jnp.float32),
        ),
        in_specs=[far] * len(arrays),
        out_specs=(pl.BlockSpec(memory_space=pltpu.VMEM), far),
        scratch_shapes=[pltpu.VMEM(array.shape, array.dtype) for array in arrays]
        + [
            pltpu.VMEM(states.shape, jnp.float32),
            pltpu.VMEM(tokens.shape, jnp.bfloat16),
            pltpu.SemaphoreType.DMA((14,)),
        ],
        compiler_params=pltpu.CompilerParams(vmem_limit_bytes=62 << 20),
    )(*arrays)


class Chain:
    def __init__(self, size):
        self.size = size
        self.x_size = fast_extent("ep", size)
        self.z_size = size // self.x_size
        self.me = lax.axis_index("ep")
        self.x = self.me % self.x_size
        self.z = self.me // self.x_size
        self.pending = []

    def at(self, j):
        left, right = self.z, self.z_size - 1 - self.z
        both = jnp.minimum(left, right)
        if j == 0:
            return self.z
        near = (j + 1) // 2
        paired = self.z - near if j % 2 else self.z + near
        single = jnp.where(left > right, self.z - (j - both), self.z + (j - both))
        return jnp.where(j <= 2 * both, paired, single)

    def traced_at(self, j):
        left, right = self.z, self.z_size - 1 - self.z
        both = jnp.minimum(left, right)
        near = (j + 1) // 2
        paired = jnp.where(j % 2 == 1, self.z - near, self.z + near)
        single = jnp.where(left > right, self.z - (j - both), self.z + (j - both))
        return jnp.where(j <= 2 * both, paired, single)

    def index(self, z, x_step):
        return z * self.x_size + (self.x + x_step + self.x_size) % self.x_size

    def copy(self, source, target, sent, landed, peer):
        return pltpu.make_async_remote_copy(
            src_ref=source,
            dst_ref=target,
            send_sem=sent,
            recv_sem=landed,
            device_id={"ep": peer},
            device_id_type=MESH,
        )

    def launch(self, copy, cond=None):
        if cond is None:
            copy.start()
        else:
            pl.when(cond)(copy.start)
        self.pending.append((copy, cond))

    def finish(self):
        for copy, cond in self.pending:
            if cond is None:
                copy.wait_send()
            else:
                pl.when(cond)(copy.wait_send)
        self.pending = []


def layer_kernel(ep_size, tp_size, top, cap, names, *refs):
    early_hbm = refs[:4]
    weights_hbm, branch_hbm, tokens_hbm = refs[4:10], refs[10], refs[11]
    out, refs = refs[12], refs[13:]
    r = dict(zip(names, refs))
    extra = list(refs[len(names) :])
    early = [r[name] for name in EARLY]
    partial, ffn_gain, route_ids, route_logits = early
    own_cols, resid_cols = r["own_cols"], r["resid_cols"]
    side, late = r["side"], r["late"]
    f32, bf16 = jnp.float32, jnp.bfloat16
    chain, grid = Chain(ep_size), Grid("tp", tp_size)
    z_size, x_size, z, x = chain.z_size, chain.x_size, chain.z, chain.x
    rounds = ep_size // tp_size
    pieces = min(tp_size, 4)
    count, width = own_cols.shape

    def take(number):
        taken = extra[:number]
        del extra[:number]
        return taken

    dense_sums, hidden_gathers, row_gathers, expert_sums = [], [], [], []
    both, every_hidden, own_hidden, full, part = [], [], [], [], []
    for g in range(rounds):
        stores = take(5)
        for target, store in zip((both, every_hidden, own_hidden, full, part), stores):
            target.append(store)
        dense_sums.append(Reduce(grid, both[g], 1, False, take(8)))
        hidden_gathers.append(Gather(grid, own_hidden[g], every_hidden[g], 1, False, take(5)))
        row_gathers.append(
            Gather(grid, None, full[g], pieces, True, take(5), (tp_size * cap, width))
        )
        expert_sums.append(Reduce(grid, part[g], pieces, True, take(8)))

    mix = Reduce(grid, partial, PIECES, True, take(8))
    mine = pl.ds(pl.multiple_of(grid.me * width, 128), width)
    barrier = pltpu.get_barrier_semaphore()
    for k in range(1, x_size):
        pl.semaphore_signal(
            barrier, inc=1, device_id={"ep": chain.index(z, k)}, device_id_type=MESH
        )
    ends = (z > 0, z - 1), (z < z_size - 1, z + 1)
    for cond, at in ends:

        @pl.when(cond)
        def _():
            pl.semaphore_signal(
                barrier, inc=1, device_id={"ep": at * x_size + x}, device_id_type=MESH
            )
    for k in range(1, tp_size):
        pl.semaphore_signal(
            barrier, inc=1, device_id={"tp": (grid.me + k) % tp_size}, device_id_type=MESH
        )
    near = [r[name] for name in WEIGHTS]
    loads = []
    transfers = list(zip(weights_hbm, near))
    transfers = list(zip(early_hbm, early)) + transfers
    transfers.insert(0, (tokens_hbm.at[:, mine], r["tokens"]))
    transfers.insert(1, (branch_hbm.at[mine], r["branch"]))
    for item, (source, target) in enumerate(transfers):
        load = pltpu.make_async_copy(source, target, r["load_sems"].at[item])
        load.start()
        loads.append(load)
    first_loads, loads = loads[:6], loads[6:]
    dense_gate, dense_up, gate, up, down, dense_down = near
    beside = (z + z_size - 1) // z_size + (2 * z_size - 2 - z) // z_size
    pl.semaphore_wait(barrier, x_size + tp_size - 2 + beside)
    for load in first_loads:
        load.wait()
    mix.push()
    logits = route_logits[...]
    raised = jnp.exp(logits - jnp.max(logits, axis=0, keepdims=True))
    side[...] = jnp.zeros((8, 128), f32)
    late[...] = jnp.zeros((8, 128), f32)
    side[0:top, 0:count] = route_ids[...].astype(f32)
    side[top : 2 * top, 0:count] = raised / jnp.sum(raised, axis=0, keepdims=True)
    mix.relay()

    cols, sides, lates = r["cols"], r["sides"], r["lates"]

    def chunk(j, q=0):
        return chain.index(chain.at(j), -q)

    step = count // PIECES

    def spot_of(source, p):
        if p >= PIECES:
            return (sides, lates)[p - PIECES].at[source]
        return cols.at[source, pl.ds(p * step, step), :]

    def chunk_of(j, q):
        return chain.index(chain.traced_at(j), -q)

    def send_chunk(j, p, cond=None, record=True, along=True, across=True):
        at = chain.at(j)
        spot = spot_of(chunk(j), p)
        if j:
            source = spot
        else:
            source = (side, late)[p - PIECES] if p >= PIECES else own_cols.at[pl.ds(p * step, step), :]
        copies = []
        for turn, move, go in (
            (0, 1, (at <= z) & (z < z_size - 1)),
            (1, -1, (at >= z) & (z > 0)),
        ) if along else ():
            copy = chain.copy(
                source,
                spot,
                r["z_sent"].at[turn, j, p],
                r["z_landed"].at[at, p],
                jnp.where(go, z + move, z) * x_size + x,
            )
            copies.append((copy, go))
        for q in range(1, x_size) if across else ():
            copy = chain.copy(
                source,
                spot,
                r["x_sent"].at[q - 1, j, p],
                r["x_landed"].at[q - 1, j, p],
                chain.index(z, q),
            )
            copies.append((copy, None))
        for copy, go in copies:
            if go is None:
                copy.start() if cond is None else pl.when(cond)(copy.start)
            else:
                pl.when(go if cond is None else go & cond)(copy.start)
            if record:
                chain.pending.append((copy, go))

    def wait_piece(j, q, p):
        spot = spot_of(chunk(j, q), p)
        if q:
            landed = r["x_landed"].at[q - 1, j, p]
        else:
            landed = r["z_landed"].at[chain.at(j), p]
        chain.copy(spot, spot, r["x_sent"].at[0, 0, 0], landed, chain.index(z, 1)).wait_recv()

    def wait_chunk(j, q):
        for p in PARTS:
            wait_piece(j, q, p)

    gain = ffn_gain[:, mine]
    gate_row = gain * r["branch"][...].astype(f32).reshape(1, width)
    lanes = lax.broadcasted_iota(jnp.int32, (count, 128), 1)
    tables = []
    send_chunk(0, PIECES)
    for p in reversed(range(PIECES)):
        span = mix.span(p)
        mixed = mix.collect_piece(p).astype(bf16).astype(f32)
        resid = (r["tokens"][span, :].astype(f32) + mixed).astype(bf16)
        resid_cols[span, :] = resid
        flt = resid.astype(f32)
        own_cols[span, :] = (flt * gain).astype(bf16)
        send_chunk(0, p)
        ssq = jnp.sum(flt * flt, axis=1, keepdims=True)
        dots = jnp.sum(flt * gate_row, axis=1, keepdims=True)
        tables.insert(0, jnp.where(lanes[:step] == 0, ssq, jnp.where(lanes[:step] == 1, dots, 0.0)))
    if count < 128:
        tables.append(jnp.zeros((128 - count, 128), f32))
    stat = jnp.concatenate(tables, axis=0).T[:8]
    r["stat"][...] = stat
    copies = []
    for k in range(1, tp_size):
        copy = grid.copy(
            r["stat"],
            r["stat_got"].at[k - 1],
            r["stat_sent"].at[k - 1],
            r["stat_landed"].at[k - 1],
            (grid.me + k) % tp_size,
        )
        copy.start()
        copies.append(copy)

    def finish_stat(stat=stat):
        for k, copy in enumerate(copies):
            copy.wait_recv()
            stat = stat + r["stat_got"][k]
        scale = lax.rsqrt(stat[0:1] / (width * tp_size) + 1e-06)
        late[0:1, :] = jax.nn.sigmoid(stat[1:2] * scale)
        late[1:2, :] = scale
        lates[chain.me] = late[...]
        send_chunk(0, PIECES + 1)
    hidden_width = dense_gate.shape[1]
    expert = chain.me.astype(f32)
    lane_ok = (lax.broadcasted_iota(jnp.int32, (1, 128), 1) < count).astype(f32)
    slots = lax.broadcasted_iota(jnp.int32, (128, 128), 0).astype(f32)
    before = (
        lax.broadcasted_iota(jnp.int32, (128, 128), 0)
        < lax.broadcasted_iota(jnp.int32, (128, 128), 1)
    ).astype(bf16)

    def process(j, q):
        i = j * x_size + q
        g, at = i // tp_size, i % tp_size
        if i == 0:
            block, info = own_cols[...], side[...]
        else:
            source = chunk(j, q)
            block, info = cols[source], sides[source]
        taken, weight = jnp.zeros((1, 128), f32), jnp.zeros((1, 128), f32)
        for item in range(top):
            hit = jnp.where(info[item : item + 1] == expert, lane_ok, 0.0)
            taken = taken + hit
            weight = weight + hit * info[top + item : top + item + 1]
        rank = jnp.dot(
            jnp.broadcast_to(taken, (8, 128)).astype(bf16), before, preferred_element_type=f32
        )[0:1]
        table = jnp.where(slots == rank, taken, 0.0)
        rows = jnp.dot(
            table[:cap, :count].astype(bf16), block, preferred_element_type=f32
        )
        full[g][at * cap : (at + 1) * cap, mine] = rows.astype(bf16)
        share = tp_size // pieces
        if at % share == share - 1:
            row_gathers[g].start_piece(at // share)
        r["table"][i] = table
        r["turned"][i] = (table * weight).T
        if i == 0:
            loads[0].wait()
            loads[1].wait()
        both[g][at, :, :hidden_width] = jnp.dot(
            block, dense_gate[...], preferred_element_type=f32
        ).astype(bf16)
        both[g][at, :, hidden_width:] = jnp.dot(
            block, dense_up[...], preferred_element_type=f32
        ).astype(bf16)
        if at == tp_size - 1:
            dense_sums[g].push()
        if at == 0 and g > 0:
            dense_sums[g - 1].relay()

    inner = gate.shape[1]
    tile = tile_of(inner)
    hidden = r["hidden"]

    def expert_hidden(g):
        row_gathers[g].relay()
        for at in range(tp_size):
            i = g * tp_size + at
            row = lates[chunk(i // x_size, i % x_size), 1:2, :]
            scales = jnp.sum(r["table"][i] * row, axis=1, keepdims=True)
            r["row_scale"][g, at * cap : (at + 1) * cap, :] = jnp.broadcast_to(
                scales[:cap], (cap, 128)
            )
        row_gathers[g].arrive()
        rows = full[g]

        @pl.loop(0, inner // tile)
        def _(step):
            span = pl.ds(pl.multiple_of(step * tile, 128), tile)
            scale = r["row_scale"][g, :, 0:1]
            gate_val = jnp.dot(rows[...], gate[:, span], preferred_element_type=f32) * scale
            up_val = jnp.dot(rows[...], up[:, span], preferred_element_type=f32) * scale
            hidden[g, :, span] = (jax.nn.silu(gate_val) * up_val).astype(bf16)

    wide = min(WIDE, width)

    def expert_part(g):
        target = part[g]

        def block(dest):
            @pl.loop(0, width // wide)
            def _(step):
                span = pl.ds(pl.multiple_of(dest * width + step * wide, 128), wide)
                target[:, span] = jnp.dot(
                    hidden[g], down[:, span], preferred_element_type=f32
                ).astype(bf16)

        for k in range(1, grid.slow + 1):
            for q in range(1, grid.fast):
                block(grid.index(k, q))
                expert_sums[g].push_part(k, q)
        for k in range(1, grid.slow + 1):
            block(grid.index(k, 0))

    def dense_hidden(g):
        i = g * tp_size + grid.me
        source = chunk_of(i // x_size, i % x_size)
        turned = jnp.concatenate([lates[source], jnp.zeros((120, 128), f32)], axis=0).T[:count]
        branch, scale = turned[:, 0:1], turned[:, 1:2]

        def emit(span, value):
            value = value * scale
            own_hidden[g][span, :] = (
                branch * jax.nn.silu(value[:, :hidden_width]) * value[:, hidden_width:]
            ).astype(bf16)

        dense_sums[g].collect(emit)
        hidden_gathers[g].start()

    fewer = jnp.minimum(z, z_size - 1 - z)

    def pass_on(j, p, cond=None, record=True, **kinds):
        def wait():
            wait_piece(j, 0, p)

        wait() if cond is None else pl.when(cond)(wait)
        send_chunk(j, p, cond, record, **kinds)

    last = rounds - 1
    end = z_size - 1
    process(0, 0)
    finish_stat()
    for j in range(1, end):
        if j % 2:
            two = j + 1 < end
            paired = j + 1 <= 2 * fewer
            for p in PARTS:
                pass_on(j, p)
                if two:
                    pass_on(j + 1, p, paired, across=False)
            if two:
                for p in PARTS:
                    send_chunk(j + 1, p, paired, along=False)
        else:
            for p in PARTS:
                pass_on(j, p, j > 2 * fewer, False)
        if j == end - 1:
            for p in PARTS:
                pass_on(end, p, fewer > 0)
        for q in range(1, x_size):
            wait_chunk(j - 1, q)
            process(j - 1, q)
        process(j, 0)
    for q in range(1, x_size):
        wait_chunk(end - 1, q)
        process(end - 1, q)
    for p in PARTS:
        pass_on(end, p, fewer == 0, False)
    for load in loads[2:5]:
        load.wait()
    for g in range(last):
        expert_hidden(g)
    process(end, 0)
    for q in range(1, x_size):
        wait_chunk(end, q)
        process(end, q)
    dense_sums[last].relay()
    for g in range(last):
        dense_hidden(g)
        expert_part(g)
    expert_hidden(last)
    expert_part(last)
    dense_hidden(last)
    expert_sums[last].relay()
    for g in reversed(range(last)):
        expert_sums[g].relay()
    for copy in copies:
        copy.wait_send()
    for phase in [mix] + row_gathers + dense_sums:
        phase.finish()
    chain.finish()
    loads[5].wait()

    collected, own_share = set(), r["own_share"]

    def share_of(j, q):
        i = j * x_size + q
        g, at = i // tp_size, i % tp_size
        chunks = tp_size // pieces
        piece = at // chunks
        if g not in collected:
            collected.add(g)
            hidden_gathers[g].relay()
            hidden_gathers[g].arrive()
        if (g, piece) not in collected:
            collected.add((g, piece))
            rows = chunks * cap
            r["expert_out"][g, piece * rows : (piece + 1) * rows, :] = (
                expert_sums[g].collect_piece(piece).astype(bf16)
            )
        turned = r["turned"][i]
        routed = jnp.dot(
            turned[:count, :cap].astype(bf16),
            r["expert_out"][g, at * cap : (at + 1) * cap, :],
            preferred_element_type=f32,
        )
        dense = jnp.dot(every_hidden[g][at], dense_down[...], preferred_element_type=f32)
        return routed + dense

    def send_share(j):
        own_share[j] = share_of(j, 0)

    def send_twins(j):
        for q in range(1, x_size):
            i = j * x_size + q
            r["x_share"][i] = share_of(j, q).astype(bf16)
            for p in range(PIECES):
                span = pl.ds(p * step, step)
                copy = chain.copy(
                    r["x_share"].at[i, span, :],
                    r["x_got"].at[j, q - 1, span, :],
                    r["xs_sent"].at[i, p],
                    r["xs_landed"].at[j, q - 1, p],
                    chain.index(z, -q),
                )
                chain.launch(copy)

    def finish_share(j):
        at = chain.at(j)
        for p in range(PIECES):
            finish_piece(j, at, pl.ds(p * step, step), p)

    def finish_piece(j, at, span, p):
        for q in range(1, x_size):
            spot = r["x_got"].at[j, q - 1, span, :]
            chain.copy(
                spot,
                spot,
                r["xs_sent"].at[0, 0],
                r["xs_landed"].at[j, q - 1, p],
                chain.index(z, q),
            ).wait_recv()
            own_share[j, span, :] = own_share[j, span, :] + r["x_got"][j, q - 1, span, :].astype(f32)
        for turn, cond in (
            (0, (at <= z) & (z < z_size - 1)),
            (1, (at >= z) & (z > 0)),
        ):

            @pl.when(cond)
            def _():
                spot = r["z_got"].at[turn, at, span, :]
                chain.copy(
                    spot,
                    spot,
                    r["zs_sent"].at[0, 0],
                    r["zs_landed"].at[turn, at, p],
                    chain.index(z, 1),
                ).wait_recv()
                own_share[j, span, :] = own_share[j, span, :] + r["z_got"][
                    turn, at, span, :
                ].astype(f32)

        if j == 0:
            total = own_share[0, span, :].astype(bf16).astype(f32)
            out[span, :] = (resid_cols[span, :].astype(f32) + total).astype(bf16)
        else:
            r["z_share"][j, span, :] = own_share[j, span, :].astype(bf16)
            share_copy(j, p).start()

    def share_copy(j, p):
        at, span = chain.at(j), pl.ds(p * step, step)
        turn = jnp.where(at < z, 0, 1)
        return chain.copy(
            r["z_share"].at[j, span, :],
            r["z_got"].at[turn, at, span, :],
            r["zs_sent"].at[j, p],
            r["zs_landed"].at[turn, at, p],
            jnp.where(at < z, z - 1, z + 1) * x_size + x,
        )

    def finish_if(cond, j):
        if 0 < j < z_size:
            pl.when(cond)(functools.partial(finish_share, j))

    for j in reversed(range(z_size)):
        send_twins(j)
        finish_if(fewer == 0, j + 1)
        finish_if(fewer > 0, j + 2)
        send_share(j)
    finish_if(fewer > 0, 1)
    finish_share(0)
    for j in range(1, z_size):
        for p in range(PIECES):
            share_copy(j, p).wait_send()
    chain.finish()
    for phase in hidden_gathers + expert_sums:
        phase.finish()


PIECES = 2
PARTS = (2, 1, 0, 3)
WIDE = 512
EARLY = ("partial", "ffn_gain", "route_ids", "route_logits")
WEIGHTS = ("dense_gate", "dense_up", "gate", "up", "down", "dense_down")


def layer(partial, ffn_gain, route_ids, route_logits, weights, branch_gate, tokens, ep_size, tp_size):
    count, width = tokens.shape[0], tokens.shape[1] // tp_size
    top = route_ids.shape[0]
    bf16, f32 = jnp.bfloat16, jnp.float32
    vmem, dma = pltpu.VMEM, pltpu.SemaphoreType.DMA
    x_size = fast_extent("ep", ep_size)
    z_size = ep_size // x_size
    cap = max(2, 2 * count * top // ep_size)
    cap = -(-cap // 16) * 16
    hidden_width, inner = weights[0].shape[1], weights[2].shape[1]
    rounds, rows = ep_size // tp_size, tp_size * cap
    pieces = min(tp_size, 4)
    fast = fast_extent("tp", tp_size)
    slow = tp_size // fast
    named = {name: vmem(array.shape, bf16) for name, array in zip(WEIGHTS, weights)}
    firsts = (partial, ffn_gain, route_ids, route_logits)
    named.update({name: vmem(array.shape, array.dtype) for name, array in zip(EARLY, firsts)})
    named.update(
        load_sems=dma((len(weights) + 6,)),
        tokens=vmem((count, width), bf16),
        branch=vmem((width,), bf16),
        own_cols=vmem((count, width), bf16),
        resid_cols=vmem((count, width), bf16),
        side=vmem((8, 128), f32),
        late=vmem((8, 128), f32),
        stat=vmem((8, 128), f32),
        stat_got=vmem((tp_size - 1, 8, 128), f32),
        stat_sent=dma((tp_size - 1,)),
        stat_landed=dma((tp_size - 1,)),
        cols=vmem((ep_size, count, width), bf16),
        sides=vmem((ep_size, 8, 128), f32),
        lates=vmem((ep_size, 8, 128), f32),
        table=vmem((ep_size, 128, 128), f32),
        row_scale=vmem((rounds, rows, 128), f32),
        turned=vmem((ep_size, 128, 128), f32),
        hidden=vmem((rounds, rows, inner), bf16),
        expert_out=vmem((rounds, rows, width), bf16),
        own_share=vmem((z_size, count, width), f32),
        x_share=vmem((ep_size, count, width), bf16),
        x_got=vmem((z_size, x_size - 1, count, width), bf16),
        z_share=vmem((z_size, count, width), bf16),
        z_got=vmem((2, z_size, count, width), bf16),
        z_sent=dma((2, z_size, PIECES + 2)),
        z_landed=dma((z_size, PIECES + 2)),
        x_sent=dma((x_size - 1, z_size, PIECES + 2)),
        x_landed=dma((x_size - 1, z_size, PIECES + 2)),
        xs_sent=dma((ep_size, PIECES)),
        xs_landed=dma((z_size, x_size - 1, PIECES)),
        zs_sent=dma((z_size, PIECES)),
        zs_landed=dma((2, z_size, PIECES)),
    )
    extra = []
    for _ in range(rounds):
        extra += [
            vmem((tp_size, count, 2 * hidden_width), bf16),
            vmem((tp_size, count, hidden_width), bf16),
            vmem((count, hidden_width), bf16),
            vmem((rows, tp_size * width), bf16),
            vmem((rows, tp_size * width), bf16),
        ]
        extra += reduce_scratch(fast, slow, count, 2 * hidden_width, 1)
        extra += gather_sems(fast, slow, 1) + gather_sems(fast, slow, pieces)
        extra += reduce_scratch(fast, slow, rows, width, pieces)
    extra += reduce_scratch(fast, slow, count, width, PIECES)
    whole = pl.BlockSpec(memory_space=pltpu.VMEM)
    far = pl.BlockSpec(memory_space=pl.ANY)
    return pl.pallas_call(
        functools.partial(layer_kernel, ep_size, tp_size, top, cap, tuple(named)),
        out_shape=jax.ShapeDtypeStruct((count, width), bf16),
        in_specs=[far] * (len(weights) + 6),
        out_specs=whole,
        scratch_shapes=list(named.values()) + extra,
        compiler_params=pltpu.CompilerParams(
            collective_id=0, has_side_effects=True, vmem_limit_bytes=62 << 20
        ),
    )(partial, ffn_gain, route_ids, route_logits, *weights, branch_gate, tokens)


def shards(
    tokens,
    mix_gain,
    ffn_gain,
    in_proj,
    decay_rate,
    frequency,
    log_step,
    b_real,
    b_imag,
    c_real,
    c_imag,
    skip_gain,
    states,
    out_proj,
    route_ids,
    route_logits,
    expert_gate,
    expert_up,
    expert_down,
    dense_gate,
    dense_up,
    dense_down,
    branch_gate,
):
    tp_count = lax.axis_size("tp")
    ep_count = lax.axis_size("ep")
    partial, new_states = mixer(
        tokens,
        mix_gain.reshape(1, -1),
        in_proj,
        decay_rate,
        frequency,
        log_step.reshape(1, -1),
        jnp.swapaxes(b_real, 1, 2),
        jnp.swapaxes(b_imag, 1, 2),
        c_real,
        c_imag,
        skip_gain.reshape(1, -1),
        states,
        out_proj,
    )
    weights = (
        dense_gate,
        dense_up,
        expert_gate[0],
        expert_up[0],
        expert_down[0],
        dense_down,
    )
    output = layer(
        partial,
        ffn_gain.reshape(1, -1),
        route_ids.T,
        route_logits.T,
        weights,
        branch_gate,
        tokens,
        ep_count,
        tp_count,
    )
    return (output, new_states)


def solution(mesh):
    return jax.shard_map(
        shards,
        mesh=mesh,
        in_specs=(
            P("ep", None),
            P(),
            P(),
            P(None, "tp"),
            P("tp", None),
            P("tp", None),
            P("tp"),
            P("tp", None, None),
            P("tp", None, None),
            P("tp", None, None),
            P("tp", None, None),
            P("tp"),
            P(None, "ep", "tp"),
            P("tp", None),
            P("ep", None),
            P("ep", None),
            P("ep", None, "tp"),
            P("ep", None, "tp"),
            P("ep", "tp", None),
            P("tp", "ep"),
            P("tp", "ep"),
            P("ep", "tp"),
            P(),
        ),
        out_specs=(P("ep", "tp"), P(None, "ep", "tp")),
        check_vma=False,
    )
```
